32 devices in a mesh: sp: 4 (over y, x), tp: 8 (over z, core).
Axes of the slice: x: 2, y: 2, z: 4, core: 2. Of those that a mesh axis runs over, the one named last changes fastest.
Arguments:
- query_rows: bfloat16 [8192, 1024], P('sp', 'tp'), may hold values from -6 to 6
- key_rows: bfloat16 [8192, 1024], P('sp', 'tp'), may hold values from -6 to 6
- value_rows: bfloat16 [8192, 1024], P('sp', 'tp'), may hold values from -6 to 6
- gate_rows: bfloat16 [8192, 1024], P('sp', 'tp'), may hold values from -6 to 6
- log_decay: float32 [16, 8192], P('tp', 'sp'), may hold values from -1 to 0
- residual: bfloat16 [8192, 2048], P(('sp', 'tp')), may hold values from -6 to 6
- head_gain: float32 [1024], P('tp'), may hold values from 0.1 to 1.9
- out_weight: bfloat16 [1024, 2048], P(None, 'tp'), may hold values from -0.1875 to 0.1875
- norm_gain: float32 [2048], replicated, may hold values from 0.1 to 1.9
- expert_ids: int32 [8192, 2], P(('sp', 'tp')), may hold values from 0 to 3, all different within a row; in each aligned block of 256 rows (0 to 255, 256 to 511, ...) at most 192 rows name the same one
- route_weights: float32 [8192, 2], P(('sp', 'tp')), may hold values from 0.2 to 1
- expert_gate: bfloat16 [2048, 4096], P(None, ('sp', 'tp')), may hold values from -0.125 to 0.125
- expert_up: bfloat16 [2048, 4096], P(None, ('sp', 'tp')), may hold values from -0.125 to 0.125
- expert_down: bfloat16 [2048, 4096], P(None, ('sp', 'tp')), may hold values from -0.1875 to 0.1875
- shared_gate: bfloat16 [2048, 512], replicated, may hold values from -0.125 to 0.125
- shared_up: bfloat16 [2048, 512], replicated, may hold values from -0.125 to 0.125
- shared_down: bfloat16 [2048, 512], replicated, may hold values from -0.25 to 0.25
Outputs:
- result: bfloat16 [8192, 2048], P(('sp', 'tp'))
The draws below stay inside these ranges and needn't reach their ends.
Inputs may be any that keep to these rules, and one draw needn't show every extreme that they name: `expert_ids`: each row names 2 different experts. Within the rows of one device (aligned blocks of 256 rows) no expert is named by more than 192 rows, and in some block an expert is named by exactly 192 rows.
All inputs are finite; a program needn't handle non-finite values.
Results may differ from the reference program's by a relative error of at most 0.0075.
Values may be sent and summed in bfloat16 or wider, within the bound.
A program may use at most 128 MiB of HBM per device.

```python
import math
import jax
import jax.numpy as jnp
import numpy as np
from jax import lax

D = 2048
HEADS = 16
HEAD = 64
HW = 1024
FF = 1024
SH = 512
TOPK = 2
SPAN = 512
TOK_DEV = 256
TOKENS = 8192
SPECIALISTS = 4
CAP = 192


def draw_log_decay(key, part):
    streams = jax.random.split(key, 6)
    slow_share = 0.5
    sequence_ordinals = jnp.arange(TOKENS, dtype=jnp.int32)
    chance = jax.random.uniform(streams[0], (HEADS,))
    slow = chance < slow_share
    fast_rate = jnp.exp(jax.random.uniform(streams[1], (HEADS,), minval=jnp.log(1.0 / 100.0), maxval=jnp.log(1.0 / 30.0)))
    slow_rate = jnp.exp(jax.random.uniform(streams[2], (HEADS,), minval=jnp.log(0.1), maxval=jnp.log(0.8))) / TOKENS
    rate = jnp.where(slow, slow_rate, fast_rate)
    factor = jnp.exp(jax.random.uniform(streams[3], (16,), minval=jnp.log(0.25), maxval=0.0))
    individual_slot_factor = factor[sequence_ordinals * 16 // TOKENS]
    constant_shrinkage = -rate[:, None] * individual_slot_factor[None, :]
    shifted_locations = jax.random.randint(streams[4], (HEADS, 2), 0, TOKENS)
    stack_level = jax.random.uniform(streams[5], (HEADS, 2), minval=jnp.log(0.5), maxval=jnp.log(0.8))
    segment_bundles = jnp.sum(jnp.where(sequence_ordinals[None, None, :] == shifted_locations[:, :, None], stack_level[:, :, None], 0.0), axis=1)
    return (constant_shrinkage + segment_bundles).astype(jnp.float32)


def block_levels(stream_key, dims, cuts, low, largest):
    gain = 1.0
    for dim, parts in cuts:
        heights = jax.random.uniform(jax.random.fold_in(jax.random.fold_in(stream_key, 6), dim), (parts,), jnp.float32, low / len(cuts), largest / len(cuts))
        gain = gain * jnp.repeat(jnp.exp(heights), dims[dim] // parts).reshape((-1,) + (1,) * (len(dims) - 1 - dim))
    return gain


def deal_out(rng, own, number, rows, count, top, reach, lean):
    sequence = jax.random.permutation(rng, count)
    crowded, common = load_shares(count, rows * top, reach, lean, True), load_shares(count, rows * top, reach, lean, False)
    places = jnp.arange(count)

    def named(lengths, offset_by):
        used = int((lengths > 0).sum())
        fixed = max(1, used // 4)
        moved = fixed + (places - fixed + offset_by * (used - fixed)) % max(1, count - fixed)
        return jnp.zeros((count,), jnp.int32).at[sequence[jnp.where(places < fixed, places, moved)]].set(jnp.asarray(lengths, jnp.int32))

    lengths = jnp.where(number % 4 == 0, named(crowded, number // 4), named(common, number - number // 4 - 1))
    mixed = jax.random.permutation(jax.random.fold_in(own, 3), count)
    giver, sink = mixed[0:count // 2 * 2:2], mixed[1:count // 2 * 2:2]
    slack = jnp.minimum(lengths[giver] - 1, reach - lengths[sink]) // 2
    slack = jnp.where((giver == sequence[0]) | (sink == sequence[0]) | (lengths[sink] == 0), 0, jnp.maximum(slack, 0))
    moved = jax.random.randint(jax.random.fold_in(own, 4), (count // 2,), 0, 1 << 20) % (slack + 1)
    lengths = lengths.at[giver].add(-moved).at[sink].add(moved)
    labels = jnp.searchsorted(jnp.cumsum(lengths), jnp.arange(rows * top), side="right").astype(jnp.int32)
    table = labels.reshape(top, rows).T
    table = table[jax.random.permutation(jax.random.fold_in(own, 1), rows)]
    offset_by = jax.random.randint(jax.random.fold_in(own, 2), (rows, 1), 0, top)
    return jnp.take_along_axis(table, (jnp.arange(top)[None, :] + offset_by) % top, axis=1)


def load_shares(number_of, total, reach, slope, full):
    portions = [(1 << 20) // math.isqrt(standing ** slope) + 1 for standing in range(1, number_of + 1)]
    largest = reach if full else min(reach, max(-(-total // number_of), total * portions[0] // sum(portions)))
    least = 1 if total - largest >= number_of - 1 else 0
    counts, rest = [largest] + [least] * (number_of - 1), total - largest - least * (number_of - 1)
    while rest > 0:
        candidates = [i for i in range(1, number_of) if counts[i] < largest] or [i for i in range(1, number_of) if counts[i] < reach]
        whole, budget = sum([portions[i] for i in candidates]), rest
        for i in candidates:
            addition = min(reach - counts[i], max(1, budget * portions[i] // whole), rest)
            counts[i] = counts[i] + addition
            rest = rest - addition
    return np.array(counts)


def centred(key, dims, scale, limit, pieces=(), kind=jnp.bfloat16):
    loudness = block_levels(key, dims, pieces, -0.22, 0.18) if pieces else 1.0
    array = jax.random.normal(key, dims, jnp.float32) * scale * loudness
    return jnp.minimum(jnp.maximum(array, -limit), limit).astype(kind)


def setup_inputs(seed: int = 0) -> dict:
    streams_of = jax.random.split(jax.random.key(seed), 18)
    query_rows = centred(streams_of[0], (TOKENS, HW), 1.0, 6.0, ((0, 4), (1, 8)))
    key_rows = centred(streams_of[1], (TOKENS, HW), 1.0, 6.0, ((0, 4), (1, 8)))
    value_rows = centred(streams_of[2], (TOKENS, HW), 1.0, 6.0, ((0, 4), (1, 8)))
    gate_rows = centred(streams_of[3], (TOKENS, HW), 1.0, 6.0, ((0, 4), (1, 8)))
    log_decay = draw_log_decay(jax.random.fold_in(streams_of[17], 71), 0)
    residual = centred(streams_of[5], (TOKENS, D), 1.0, 6.0, ((0, 32),))
    head_gain = jnp.clip(1.0 + 0.18 * jax.random.normal(streams_of[6], (HW,), jnp.float32), 0.1, 1.9)
    out_weight = centred(streams_of[7], (HW, D), HW ** -0.5, 0.1875, ((1, 8),))
    norm_gain = jnp.clip(1.0 + 0.18 * jax.random.normal(streams_of[8], (D,), jnp.float32), 0.1, 1.9)
    expert_ids_keys = jax.random.split(jax.random.fold_in(streams_of[9], 1), TOKENS // TOK_DEV)
    expert_ids_turns = jax.random.permutation(jax.random.fold_in(streams_of[9], 3), TOKENS // TOK_DEV)
    expert_ids = jax.vmap(lambda own, number: deal_out(jax.random.fold_in(streams_of[9], 2), own, number, TOK_DEV, SPECIALISTS, TOPK, CAP, 2))(expert_ids_keys, expert_ids_turns).reshape((TOKENS, TOPK))
    route_weights = jnp.clip(jnp.exp(math.log(1.0) - 1.609438 * jax.random.uniform(streams_of[10], (TOKENS, TOPK), jnp.float32) ** block_levels(streams_of[10], (TOKENS, TOPK), ((0, 32),), -0.2, 0.2)), 0.2, 1.0)
    expert_gate = centred(streams_of[11], (D, SPECIALISTS * FF), D ** -0.5, 0.125, ((1, 32),))
    expert_up = centred(streams_of[12], (D, SPECIALISTS * FF), D ** -0.5, 0.125, ((1, 32),))
    expert_down = centred(streams_of[13], (D, SPECIALISTS * FF), FF ** -0.5, 0.1875, ((1, 32),))
    shared_gate = centred(streams_of[14], (D, SH), D ** -0.5, 0.125)
    shared_up = centred(streams_of[15], (D, SH), D ** -0.5, 0.125)
    shared_down = centred(streams_of[16], (D, SH), SH ** -0.5, 0.25)
    return dict(query_rows=query_rows, key_rows=key_rows, value_rows=value_rows, gate_rows=gate_rows, log_decay=log_decay, residual=residual, head_gain=head_gain, out_weight=out_weight, norm_gain=norm_gain, expert_ids=expert_ids, route_weights=route_weights, expert_gate=expert_gate, expert_up=expert_up, expert_down=expert_down, shared_gate=shared_gate, shared_up=shared_up, shared_down=shared_down)


eps = 1e-05

def retain(queries, key_heads, values, log_decay):
    rows, heads, width = queries.shape
    count = rows // SPAN
    scale = width ** (-0.5)
    query_blocks = queries.reshape(count, SPAN, heads, width)
    key_blocks = key_heads.reshape(count, SPAN, heads, width)
    value_blocks = values.reshape(count, SPAN, heads, width)
    decay_blocks = log_decay.reshape(heads, count, SPAN).transpose(1, 0, 2)
    offsets = jnp.arange(SPAN, dtype=jnp.int32)
    causal = offsets[:, None] >= offsets[None, :]

    def advance(carry, inputs):
        block_queries, block_keys, block_values, decay_block = inputs
        query_matrix_full = block_queries.astype(jnp.float32)
        key_matrix_full = block_keys.astype(jnp.float32)
        value_matrix_full = block_values.astype(jnp.float32)
        running = jnp.cumsum(decay_block, axis=1)
        spread = running[:, :, None] - running[:, None, :]
        damping = jnp.exp(jnp.where(causal[None], spread, -jnp.inf))
        attention_scores = jnp.einsum('xru,jru->rxj', query_matrix_full, key_matrix_full)
        decay_weighted = lax.optimization_barrier((attention_scores * scale * damping).astype(jnp.bfloat16)).astype(jnp.float32)
        inner_block_term = jnp.einsum('svc,csj->vsj', decay_weighted, value_matrix_full)
        carried = jnp.einsum('nhd,hde->nhe', query_matrix_full, carry, precision=lax.Precision.HIGHEST)
        carried = carried * jnp.exp(running).T[:, :, None]
        decay_to_block_end = jnp.exp(running[:, -1:] - running).T[:, :, None] * scale
        state_update = jnp.einsum('jok,jow->okw', key_matrix_full * decay_to_block_end, value_matrix_full, precision=lax.Precision.HIGHEST)
        carry = carry * jnp.exp(running[:, -1])[:, None, None] + state_update
        return (carry, inner_block_term + carried)
    start = jnp.zeros((heads, width, width), jnp.float32)
    _, outputs = lax.scan(advance, start, (query_blocks, key_blocks, value_blocks, decay_blocks))
    return outputs.reshape(rows, heads, width)

def reference(query_rows, key_rows, value_rows, gate_rows, log_decay, residual, head_gain, out_weight, norm_gain, expert_ids, route_weights, expert_gate, expert_up, expert_down, shared_gate, shared_up, shared_down):
    retained = retain(query_rows.reshape(TOKENS, HEADS, HEAD), key_rows.reshape(TOKENS, HEADS, HEAD), value_rows.reshape(TOKENS, HEADS, HEAD), log_decay)
    centered = retained - lax.optimization_barrier(jnp.mean(retained, axis=2, keepdims=True))
    normed = centered * lax.rsqrt(lax.optimization_barrier(jnp.mean(centered * centered, axis=2, keepdims=True)) + eps)
    ret_rows = (normed.reshape(TOKENS, HW) * head_gain * jax.nn.silu(gate_rows.astype(jnp.float32))).astype(jnp.bfloat16)
    mixer = jnp.dot(ret_rows, out_weight, preferred_element_type=jnp.float32)
    hidden = (residual.astype(jnp.float32) + mixer).astype(jnp.bfloat16)
    hidden_wide = hidden.astype(jnp.float32)
    normed_rows = (hidden_wide * lax.rsqrt(lax.optimization_barrier(jnp.mean(hidden_wide * hidden_wide, axis=1, keepdims=True)) + eps) * norm_gain).astype(jnp.bfloat16)
    shared_mid = (jax.nn.silu(jnp.dot(normed_rows, shared_gate, preferred_element_type=jnp.float32)) * jnp.dot(normed_rows, shared_up, preferred_element_type=jnp.float32)).astype(jnp.bfloat16)
    shared_out = lax.dot_general(shared_mid, shared_down, (((1,), (1,)), ((), ())), preferred_element_type=jnp.float32)
    block_count = TOKENS // TOK_DEV
    slots = block_count * CAP
    block_index = jnp.arange(block_count, dtype=jnp.int32)[:, None]
    token_index = jnp.arange(TOKENS, dtype=jnp.int32)

    def expert_step(total, index):
        chosen = expert_ids == index
        picked = jnp.any(chosen, axis=1)
        weight = lax.optimization_barrier(jnp.sum(jnp.where(chosen, route_weights, 0.0), axis=1))
        blocked = picked.reshape(block_count, TOK_DEV).astype(jnp.int32)
        position = jnp.cumsum(blocked, axis=1) - 1
        target = jnp.where(blocked > 0, block_index * CAP + position, slots).reshape(-1).astype(jnp.int32)
        table = jnp.zeros((slots + 1,), jnp.int32).at[target].set(token_index)[:slots]
        live = jnp.zeros((slots + 1,), jnp.float32).at[target].set(1.0)[:slots]
        rows = normed_rows[table]
        gate_cols = lax.dynamic_slice_in_dim(expert_gate, index * FF, FF, 1)
        up_cols = lax.dynamic_slice_in_dim(expert_up, index * FF, FF, 1)
        down_cols = lax.dynamic_slice_in_dim(expert_down, index * FF, FF, 1)
        middle = (jax.nn.silu(jnp.dot(rows, gate_cols, preferred_element_type=jnp.float32)) * jnp.dot(rows, up_cols, preferred_element_type=jnp.float32)).astype(jnp.bfloat16)
        outcome = lax.dot_general(middle, down_cols, (((1,), (1,)), ((), ())), preferred_element_type=jnp.float32).astype(jnp.bfloat16)
        contrib = outcome.astype(jnp.float32) * (weight[table] * live)[:, None]
        return (total.at[table].add(contrib), None)
    routed, _ = lax.scan(expert_step, jnp.zeros((TOKENS, D), jnp.float32), jnp.arange(SPECIALISTS, dtype=jnp.int32))
    return (hidden_wide + routed + shared_out).astype(jnp.bfloat16)
```

```python
import functools

import jax
import jax.numpy as jnp
from jax import lax
from jax.experimental import pallas as pl
from jax.experimental.pallas import tpu as pltpu
from jax.sharding import PartitionSpec as P


HEAD = 64
BLOCK = 256
EXTRA = 8


eps = 1e-05
F32 = jnp.float32
BF16 = jnp.bfloat16


def split(value):
    high = value.astype(BF16)
    return high, (value - high.astype(F32)).astype(BF16)


def per_head(columns, lanes):
    heads = columns.shape[1]
    out = jnp.broadcast_to(columns[:, 0:1], lanes.shape)
    for head in range(1, heads):
        out = jnp.where(lanes // HEAD == head, columns[:, head : head + 1], out)
    return out


def gathered_update(keys, values, column, lanes, end):
    scale = HEAD ** (-0.5)
    weighted = keys.astype(F32) * (jnp.exp(per_head(end - column, lanes)) * scale)
    high, low = split(weighted)
    dims = (((0,), (0,)), ((), ()))
    return lax.dot_general(high, values, dims, preferred_element_type=F32) + lax.dot_general(
        low, values, dims, preferred_element_type=F32
    )


def state_kernel(key_ref, value_ref, column_ref, out_ref):
    width = key_ref.shape[1]
    step = pl.program_id(0)

    @pl.when(step == 0)
    def _():
        out_ref[0:width, :] = jnp.zeros((width, width), F32)
        out_ref[width:, :] = jnp.zeros((EXTRA, width), F32)

    lanes = lax.broadcasted_iota(jnp.int32, key_ref.shape, 1)
    column = column_ref[...]
    end = column[BLOCK - 1 : BLOCK, :]
    end_lanes = per_head(end, lanes[0:1, :])
    fresh = gathered_update(key_ref[...], value_ref[...], column, lanes, end)
    out_ref[0:width, :] = out_ref[0:width, :] * jnp.exp(end_lanes) + fresh
    out_ref[width:, :] = out_ref[width:, :] + end_lanes


def retention_kernel(
    mine_ref, query_ref, key_ref, value_ref, gate_ref, column_ref, row_ref, gain_ref, states_ref,
    out_ref, state
):
    rows, width = query_ref.shape
    heads = width // HEAD
    step = pl.program_id(0)
    count = states_ref.shape[0]
    row_ids = lax.broadcasted_iota(jnp.int32, (width, width), 0) // HEAD
    column_ids = lax.broadcasted_iota(jnp.int32, (width, width), 1) // HEAD

    @pl.when(step == 0)
    def _():
        total = jnp.zeros((width, width), F32)
        for position in range(count - 1):
            decay = jnp.exp(states_ref[position, width : width + 1, :])
            longer = total * decay + states_ref[position, 0:width, :]
            total = jnp.where(position < mine_ref[0], longer, total)
        state[...] = jnp.where(row_ids == column_ids, total, 0.0)

    lanes = lax.broadcasted_iota(jnp.int32, (rows, width), 1)
    queries, keys, values = query_ref[...], key_ref[...], value_ref[...]
    column = column_ref[...]
    end = column[rows - 1 : rows, :]
    causal = lax.broadcasted_iota(jnp.int32, (rows, rows), 0) >= lax.broadcasted_iota(
        jnp.int32, (rows, rows), 1
    )
    scale = HEAD ** (-0.5)
    high, low = split(state[...])
    carried = jnp.dot(queries, high, preferred_element_type=F32) + jnp.dot(
        queries, low, preferred_element_type=F32
    )
    retained = carried * jnp.exp(per_head(column, lanes))
    inner = None
    for head in range(heads):
        own = jnp.where(lanes // HEAD == head, queries.astype(F32), 0.0).astype(BF16)
        scores = lax.dot_general(
            own, keys, (((1,), (1,)), ((), ())), preferred_element_type=F32
        )
        spread = column[:, head : head + 1] - row_ref[0, head : head + 1, :]
        damping = jnp.exp(jnp.where(causal, spread, -jnp.inf))
        factor = (scores * scale * damping).astype(BF16)
        term = jnp.dot(factor, values, preferred_element_type=F32)
        inner = term if inner is None else jnp.where(lanes // HEAD == head, term, inner)
    retained = retained + inner
    fresh = gathered_update(keys, values, column, lanes, end)
    end_lanes = per_head(end, lanes[0:1, :])
    state[...] = state[...] * jnp.exp(end_lanes) + jnp.where(row_ids == column_ids, fresh, 0.0)

    def head_mean(array):
        out = None
        for head in range(heads):
            inside = lanes // HEAD == head
            mean = jnp.sum(jnp.where(inside, array, 0.0), axis=1, keepdims=True) * (1.0 / HEAD)
            out = jnp.broadcast_to(mean, array.shape) if out is None else jnp.where(inside, mean, out)
        return out

    centered = retained - head_mean(retained)
    normed = centered * lax.rsqrt(head_mean(centered * centered) + eps)
    gates = gate_ref[...].astype(F32)
    out_ref[...] = (normed * gain_ref[...] * (gates * jax.nn.sigmoid(gates))).astype(BF16)


def retention(query_rows, key_rows, value_rows, gate_rows, log_decay, head_gain):
    rows, width = query_rows.shape
    heads = width // HEAD
    count = rows // BLOCK
    running = jnp.cumsum(log_decay.reshape(heads, count, BLOCK), axis=2)
    row = running.transpose(1, 0, 2)
    column = running.reshape(heads, rows).T
    block = pl.BlockSpec((BLOCK, width), lambda i: (i, 0))
    column_block = pl.BlockSpec((BLOCK, heads), lambda i: (i, 0))
    state_call = pl.pallas_call(
        state_kernel,
        grid=(count,),
        in_specs=[block, block, column_block],
        out_specs=pl.BlockSpec((width + EXTRA, width), lambda i: (0, 0)),
        out_shape=jax.ShapeDtypeStruct((width + EXTRA, width), F32),
        compiler_params=pltpu.CompilerParams(dimension_semantics=("arbitrary",)),
        cost_estimate=pl.CostEstimate(
            flops=4 * rows * width * width, bytes_accessed=4 * rows * width, transcendentals=rows * width
        ),
    )
    own = state_call(key_rows, value_rows, column)
    states = lax.all_gather(own, "sp")
    mine = lax.axis_index("sp").astype(jnp.int32).reshape(1)
    return pl.pallas_call(
        retention_kernel,
        grid=(count,),
        in_specs=[
            pl.BlockSpec(memory_space=pltpu.SMEM),
            block,
            block,
            block,
            block,
            column_block,
            pl.BlockSpec((1, heads, BLOCK), lambda i: (i, 0, 0)),
            pl.BlockSpec((1, width), lambda i: (0, 0)),
            pl.BlockSpec(states.shape, lambda i: (0, 0, 0)),
        ],
        out_specs=block,
        out_shape=jax.ShapeDtypeStruct((rows, width), BF16),
        scratch_shapes=[pltpu.VMEM((width, width), F32)],
        compiler_params=pltpu.CompilerParams(dimension_semantics=("arbitrary",)),
        cost_estimate=pl.CostEstimate(
            flops=8 * rows * width * BLOCK,
            bytes_accessed=10 * rows * width,
            transcendentals=rows * BLOCK * heads,
        ),
    )(mine, query_rows, key_rows, value_rows, gate_rows, column, row, head_gain[None, :], states)


def send(piece, pairs):
    return lax.ppermute(piece, "tp", pairs)


def ring_start(own):
    size = lax.axis_size("tp")
    right = [(i, (i + 2) % size) for i in range(size)]
    left = [(i, (i - 2) % size) for i in range(size)]
    swap = [(i, i ^ 1) for i in range(size)]
    return send(own, right), send(own, left), send(own, swap)


def ring_finish(own, from_left, from_right, other):
    size = lax.axis_size("tp")
    chips = size // 2
    right = [(i, (i + 2) % size) for i in range(size)]
    left = [(i, (i - 2) % size) for i in range(size)]
    swap = [(i, i ^ 1) for i in range(size)]
    half = own.shape[1] // 2
    last = chips // 2
    pieces = [[own], [other]]
    for hop in range(1, (chips - 1) // 2 + 1):
        if hop > 1:
            from_left = send(from_left, right)
            from_right = send(from_right, left)
        for piece in (from_left, from_right):
            pieces += [[piece], [send(piece, swap)]]
    if chips % 2 == 0 and last > 1:
        first = send(from_left[:, :half], right)
        second = send(from_right[:, half:], left)
        pieces += [[first, second], [send(first, swap), send(second, swap)]]
    elif chips == 2:
        pieces += [[from_left], [send(from_left, swap)]]
    return pieces


def expert_kernel(layout, row_ref, *refs):
    count = len(layout)
    piece_refs, out_ref = refs[:count], refs[count]
    weights, middle, sems = refs[count + 1 :]
    slots, _, width, ff = weights.shape
    rows = row_ref.shape[0]
    copies = []
    for index, (slot, start, length) in enumerate(layout):
        copy = pltpu.make_async_copy(
            piece_refs[index], weights.at[slot, :, pl.ds(start, length), :], sems.at[index]
        )
        copy.start()
        copies.append(copy)
    tile = rows // 2
    for pair in range(slots // 2):
        for index, (slot, _, _) in enumerate(layout):
            if slot // 2 == pair:
                copies[index].wait()

        @pl.loop(0, 2)
        def _(step):
            span = pl.ds(pl.multiple_of(step * tile, tile), tile)
            block = row_ref[span, :]
            gate = jnp.concatenate([weights[2 * pair, 0], weights[2 * pair + 1, 0]], axis=1)
            up = jnp.concatenate([weights[2 * pair, 1], weights[2 * pair + 1, 1]], axis=1)
            gated = jnp.dot(block, gate, preferred_element_type=F32)
            raised = jnp.dot(block, up, preferred_element_type=F32)
            value = gated * jax.nn.sigmoid(gated) * raised
            middle[span, 2 * pair * ff : 2 * (pair + 1) * ff] = value.astype(BF16)

    part = 512

    @pl.loop(0, width // part)
    def _(step):
        span = pl.ds(pl.multiple_of(step * part, part), part)
        down = jnp.concatenate([weights[slot, 2, span, :] for slot in range(slots)], axis=1)
        out_ref[:, span] = lax.dot_general(
            middle[...], down, (((1,), (1,)), ((), ())), preferred_element_type=F32
        ).astype(BF16)


def experts(rows, shards):
    _, width, ff = shards[0][0].shape
    count = len(shards)
    if ff % 128 or count % 2:
        whole = jnp.concatenate([jnp.concatenate(shard, axis=1) for shard in shards], axis=2)
        middle = (
            jax.nn.silu(jnp.dot(rows, whole[0], preferred_element_type=F32))
            * jnp.dot(rows, whole[1], preferred_element_type=F32)
        ).astype(BF16)
        return lax.dot_general(
            middle, whole[2], (((1,), (1,)), ((), ())), preferred_element_type=F32
        ).astype(BF16)
    layout, pieces = [], []
    for slot, shard in enumerate(shards):
        start = 0
        for piece in shard:
            layout.append((slot, start, piece.shape[1]))
            pieces.append(piece)
            start += piece.shape[1]
    return pl.pallas_call(
        functools.partial(expert_kernel, layout),
        in_specs=[pl.BlockSpec(memory_space=pltpu.VMEM)]
        + [pl.BlockSpec(memory_space=pl.ANY)] * len(pieces),
        out_specs=pl.BlockSpec(memory_space=pltpu.VMEM),
        out_shape=jax.ShapeDtypeStruct(rows.shape, BF16),
        scratch_shapes=[
            pltpu.VMEM((count, 3, width, ff), BF16),
            pltpu.VMEM((rows.shape[0], count * ff), BF16),
            pltpu.SemaphoreType.DMA((len(pieces),)),
        ],
        compiler_params=pltpu.CompilerParams(vmem_limit_bytes=60 * 1024 * 1024),
        cost_estimate=pl.CostEstimate(
            flops=6 * rows.shape[0] * width * count * ff,
            bytes_accessed=6 * width * count * ff + 4 * rows.size,
            transcendentals=rows.shape[0] * count * ff,
        ),
    )(rows, *pieces)


def on_device(
    query_rows,
    key_rows,
    value_rows,
    gate_rows,
    log_decay,
    residual,
    head_gain,
    out_weight,
    norm_gain,
    expert_ids,
    route_weights,
    expert_gate,
    expert_up,
    expert_down,
    shared_gate,
    shared_up,
    shared_down,
):
    part = out_weight.shape[0] // lax.axis_size("sp")
    own_part = lax.dynamic_slice_in_dim(out_weight, lax.axis_index("sp") * part, part, 0)
    out_part = lax.all_gather(own_part, "tp", axis=1, tiled=True)
    out_full = lax.all_gather(out_part, "sp", axis=0, tiled=True)
    shard = jnp.stack([expert_gate, expert_up, expert_down])
    shard, log_decay = lax.optimization_barrier((shard, log_decay))
    from_left, from_right, other = ring_start(shard)

    specialists = lax.axis_size("sp")
    tokens, chosen = expert_ids.shape
    width = residual.shape[1]
    capacity = 3 * tokens * chosen // (2 * specialists)
    names = jnp.arange(specialists, dtype=jnp.int32)[:, None]
    named = [expert_ids[:, j][None, :] == names for j in range(chosen)]
    match = functools.reduce(jnp.logical_or, named)
    weight = sum(jnp.where(named[j], route_weights[:, j][None, :], 0.0) for j in range(chosen))
    earlier = jnp.arange(tokens)[:, None] < jnp.arange(tokens)[None, :]
    position = jnp.dot(match.astype(BF16), earlier.astype(BF16), preferred_element_type=F32)
    place = jnp.where(match, position.astype(jnp.int32), -1)
    sits = place[:, None, :] == jnp.arange(capacity, dtype=jnp.int32)[None, :, None]
    pick = sits.astype(BF16).reshape(specialists * capacity, tokens)
    weight_high = lax.reduce_precision(weight, 8, 7)
    weight_low = weight - weight_high
    back_high = jnp.where(sits, weight_high[:, None, :], 0.0).astype(BF16)
    back_low = jnp.where(sits, weight_low[:, None, :], 0.0).astype(BF16)

    ret_rows = retention(query_rows, key_rows, value_rows, gate_rows, log_decay, head_gain)
    token_rows = lax.all_to_all(ret_rows, "tp", split_axis=0, concat_axis=1, tiled=True)
    token_rows, from_left, from_right = lax.optimization_barrier((token_rows, from_left, from_right))
    shards = ring_finish(shard, from_left, from_right, other)
    mixer = jnp.dot(token_rows, out_full, preferred_element_type=F32)
    hidden = (residual.astype(F32) + mixer).astype(BF16)
    hidden_wide = hidden.astype(F32)
    normed_rows = (
        hidden_wide
        * lax.rsqrt(jnp.mean(hidden_wide * hidden_wide, axis=1, keepdims=True) + eps)
        * norm_gain
    ).astype(BF16)
    outgoing = jnp.dot(pick, normed_rows, preferred_element_type=F32).astype(BF16)
    outgoing = outgoing.reshape(specialists, capacity, width)
    arrived = lax.all_to_all(outgoing, "sp", split_axis=0, concat_axis=0, tiled=True)
    shared_mid = (
        jax.nn.silu(jnp.dot(normed_rows, shared_gate, preferred_element_type=F32))
        * jnp.dot(normed_rows, shared_up, preferred_element_type=F32)
    ).astype(BF16)
    shared_out = lax.dot_general(
        shared_mid, shared_down, (((1,), (1,)), ((), ())), preferred_element_type=F32
    )
    flat_rows = arrived.reshape(-1, width)
    processed = experts(flat_rows, shards).reshape(arrived.shape)
    returned = lax.all_to_all(processed, "sp", split_axis=0, concat_axis=0, tiled=True)
    dims = (((0, 1), (0, 1)), ((), ()))
    routed = lax.dot_general(back_high, returned, dims, preferred_element_type=F32)
    routed += lax.dot_general(back_low, returned, dims, preferred_element_type=F32)
    return (hidden_wide + routed + shared_out).astype(BF16)


MESH = pl.DeviceIdType.MESH
NT = (((1,), (1,)), ((), ()))
TN = (((0,), (0,)), ((), ()))


def thirds(value):
    first = value.astype(BF16)
    rest = value - first.astype(F32)
    second = rest.astype(BF16)
    return first, second, (rest - second.astype(F32)).astype(BF16)


def layer_kernel(
    query_hbm, key_hbm, value_hbm, gate_hbm, decay_ref, residual_hbm, head_gain_ref, out_weight_hbm,
    norm_gain_ref, ids_ref, route_ref, expert_gate_hbm, expert_up_hbm, expert_down_hbm,
    shared_gate_hbm, shared_up_hbm, shared_down_hbm,
    result_ref,
    query, key, value, gates, residual, shared_gate, shared_up, shared_down,
    weights, out_full, running, row_running, updates, states, state, inner, ret_rows, token_rows,
    hidden, normed, squares, places, outgoing, arrived, middle, processed, returned, base,
    shared_middle, back,
    local_sem, state_send, state_recv, mix_send, mix_recv, out_z_send, out_xy_send, out_recv,
    out_pair_send, out_pair_recv, right_send, left_send, pair_send, weight_recv,
    go_send, go_recv, back_send, back_recv,
):
    places_count = states.shape[0]
    size = token_rows.shape[0]
    chips = size // 2
    sp = lax.axis_index("sp")
    tp = lax.axis_index("tp")
    z, core = tp // 2, tp % 2
    blocks, rows, width = ret_rows.shape
    heads = width // HEAD
    depth = residual.shape[1]
    capacity = arrived.shape[1]
    specialists = arrived.shape[0]
    ff = weights.shape[3]
    quarter = out_full.shape[1] // places_count
    out_columns = out_full.shape[2]
    pieces = returned.shape[0]
    piece = depth // pieces
    scale = HEAD ** (-0.5)
    inputs = (expert_gate_hbm, expert_up_hbm, expert_down_hbm)
    units = [(0, 0, depth), (1, 0, depth)] + [(2, index * piece, piece) for index in range(pieces)]

    def remote(src, dst, send, recv, device):
        return pltpu.make_async_remote_copy(
            src_ref=src, dst_ref=dst, send_sem=send, recv_sem=recv, device_id=device, device_id_type=MESH
        )

    partner = (sp, z * 2 + 1 - core)
    right = (sp, tp + 2)
    left = (sp, tp - 2)

    local = [
        pltpu.make_async_copy(src, dst, local_sem.at[index])
        for index, (src, dst) in enumerate(
            [
                (key_hbm, key),
                (value_hbm, value),
                (query_hbm, query),
                (gate_hbm, gates),
                (out_weight_hbm, out_full.at[tp]),
                (residual_hbm, residual),
                (shared_gate_hbm, shared_gate),
                (shared_up_hbm, shared_up),
                (shared_down_hbm, shared_down),
                (expert_gate_hbm, weights.at[tp, 0]),
                (expert_up_hbm, weights.at[tp, 1]),
                (expert_down_hbm, weights.at[tp, 2]),
            ]
        )
    ]
    for copy in local[:4]:
        copy.start()

    barrier = pltpu.get_barrier_semaphore()
    for step in range(1, size):
        pl.semaphore_signal(barrier, inc=1, device_id=(sp, (tp + step) % size), device_id_type=MESH)
    for step in range(1, places_count):
        pl.semaphore_signal(barrier, inc=1, device_id=(sp ^ step, tp), device_id_type=MESH)
    pl.semaphore_wait(barrier, size - 1 + places_count - 1)

    def weight_copy(slot, unit, send, device, own=False):
        which, start, length = units[unit]
        span = pl.ds(start, length)
        there = weights.at[slot, which, span, :]
        here = inputs[which].at[span, :] if own else there
        return remote(here, there, send, weight_recv.at[slot, unit], device)

    def own_send(unit):
        @pl.when(z < chips - 1)
        def _():
            weight_copy(tp, unit, right_send.at[z, unit], right, True).start()

        @pl.when(z > 0)
        def _():
            weight_copy(tp, unit, left_send.at[z, unit], left, True).start()

        weight_copy(tp, unit, pair_send.at[z, unit], partner, True).start()

    def relay(unit, distance):
        @pl.when(z - distance >= 0)
        def _():
            origin = z - distance
            slot = origin * 2 + core
            weight_copy(slot, unit, right_send.at[origin, unit], right).wait_recv()

            @pl.when(z < chips - 1)
            def _():
                weight_copy(slot, unit, right_send.at[origin, unit], right).start()

            weight_copy(slot, unit, pair_send.at[origin, unit], partner).start()

        @pl.when(z + distance < chips)
        def _():
            origin = z + distance
            slot = origin * 2 + core
            weight_copy(slot, unit, left_send.at[origin, unit], left).wait_recv()

            @pl.when(z > 0)
            def _():
                weight_copy(slot, unit, left_send.at[origin, unit], left).start()

            weight_copy(slot, unit, pair_send.at[origin, unit], partner).start()

    def from_partner(unit, chip):
        weight_copy(chip * 2 + 1 - core, unit, pair_send.at[chip, unit], partner).wait_recv()

    def out_z(step):
        target = (z + step) % chips
        span = pl.ds(pl.multiple_of(sp * quarter, quarter), quarter)
        return remote(
            out_weight_hbm.at[span, :], out_full.at[tp, span, :], out_z_send.at[step - 1],
            out_recv.at[tp, sp], (sp, target * 2 + core),
        )

    def out_piece(step, part, send, device):
        slot = ((z + step) % chips) * 2 + core
        span = pl.ds(pl.multiple_of(part * quarter, quarter), quarter)
        there = out_full.at[slot, span, :]
        return remote(there, there, send, out_recv.at[slot, part], device)

    def out_pair(slot, index, own=False):
        return remote(
            out_weight_hbm if own else out_full.at[slot], out_full.at[slot], out_pair_send.at[index],
            out_pair_recv.at[slot], partner,
        )

    for step in range(1, chips):
        out_z(step).start()
    own_send(0)
    out_pair(tp, 0, True).start()
    for copy in local[4:]:
        copy.start()

    row_ids = lax.broadcasted_iota(jnp.int32, (width, width), 0) // HEAD
    column_ids = lax.broadcasted_iota(jnp.int32, (width, width), 1) // HEAD
    same_head = row_ids == column_ids
    lanes = lax.broadcasted_iota(jnp.int32, (rows, width), 1)
    later = lax.broadcasted_iota(jnp.int32, (rows, rows), 0)
    sooner = lax.broadcasted_iota(jnp.int32, (rows, rows), 1)
    lower = jnp.where(later >= sooner, 1.0, 0.0).astype(BF16)
    upper = jnp.where(later <= sooner, 1.0, 0.0).astype(BF16)

    listed = jnp.concatenate(
        [
            decay_ref[head : head + 1, block * rows : (block + 1) * rows]
            for head in range(heads)
            for block in range(blocks)
        ],
        axis=0,
    )
    row_running[...] = functools.reduce(
        jnp.add, [jnp.dot(part, upper, preferred_element_type=F32) for part in thirds(listed)]
    )
    head_rows = lax.broadcasted_iota(jnp.int32, (width, rows), 0) // HEAD
    for block in range(blocks):
        spread = jnp.broadcast_to(listed[block : block + 1, :], (width, rows))
        for head in range(1, heads):
            spread = jnp.where(
                head_rows == head, listed[head * blocks + block : head * blocks + block + 1, :], spread
            )
        running[block] = functools.reduce(
            jnp.add,
            [
                lax.dot_general(lower, part, NT, preferred_element_type=F32)
                for part in thirds(spread)
            ],
        )

    for copy in local[:2]:
        copy.wait()
    state[...] = jnp.zeros((width + EXTRA, width), F32)

    @pl.loop(0, blocks)
    def _(block):
        span = pl.ds(pl.multiple_of(block * rows, rows), rows)
        column = running[block]
        end = column[rows - 1 : rows, :]
        weighted = key[span, :].astype(F32) * (jnp.exp(end - column) * scale)
        high, low = split(weighted)
        fresh = lax.dot_general(high, value[span, :], TN, preferred_element_type=F32)
        fresh += lax.dot_general(low, value[span, :], TN, preferred_element_type=F32)
        fresh = jnp.where(same_head, fresh, 0.0)
        updates[block] = fresh
        state[0:width, :] = state[0:width, :] * jnp.exp(end) + fresh
        state[width:, :] = state[width:, :] + end

    states[sp] = state[...]

    def state_copy(step):
        return remote(
            state, states.at[sp], state_send.at[step - 1], state_recv.at[sp], (sp ^ step, tp)
        )

    def state_arrival(step):
        return remote(
            state, states.at[sp ^ step], state_send.at[step - 1], state_recv.at[sp ^ step], (sp ^ step, tp)
        )

    local[2].wait()
    for step in range(1, places_count):
        state_copy(step).start()

    for step in range(1, chips):
        out_piece(step, sp, out_xy_send.at[step - 1, 0], partner).wait_recv()
        for other in range(1, places_count):
            out_piece(step, sp, out_xy_send.at[step - 1, other - 1], (sp ^ other, tp)).start()

    @pl.loop(0, blocks)
    def _(block):
        span = pl.ds(pl.multiple_of(block * rows, rows), rows)
        queries, keys, values = query[span, :], key[span, :], value[span, :]
        column = running[block]
        causal = later >= sooner
        total = None
        for head in range(heads):
            own = jnp.where(lanes // HEAD == head, queries.astype(F32), 0.0).astype(BF16)
            scores = lax.dot_general(own, keys, NT, preferred_element_type=F32)
            spread = column[:, head * HEAD : head * HEAD + 1] - row_running[pl.ds(head * blocks + block, 1), :]
            damping = jnp.exp(jnp.where(causal, spread, -jnp.inf))
            factor = (scores * scale * damping).astype(BF16)
            term = jnp.dot(factor, values, preferred_element_type=F32)
            total = term if total is None else jnp.where(lanes // HEAD == head, term, total)
        inner[block] = total

    for step in range(1, places_count):
        state_copy(step).wait_send()
        state_arrival(step).wait_recv()
    total = jnp.zeros((width, width), F32)
    for position in range(places_count - 1):
        longer = total * jnp.exp(states[position, width : width + 1, :]) + states[position, 0:width, :]
        total = jnp.where(position < sp, longer, total)
    state[0:width, :] = total
    local[3].wait()

    def head_mean(array):
        out = None
        for head in range(heads):
            inside = lanes // HEAD == head
            mean = jnp.sum(jnp.where(inside, array, 0.0), axis=1, keepdims=True) * (1.0 / HEAD)
            out = jnp.broadcast_to(mean, array.shape) if out is None else jnp.where(inside, mean, out)
        return out

    def mix_copy(block):
        return remote(
            ret_rows.at[block], token_rows.at[tp], mix_send.at[block], mix_recv.at[tp], (sp, block)
        )

    def mix_start(block):
        @pl.when(block != tp)
        def _():
            mix_copy(block).start()

    @pl.loop(0, blocks)
    def _(block):
        span = pl.ds(pl.multiple_of(block * rows, rows), rows)
        column = running[block]
        end = column[rows - 1 : rows, :]
        before = state[0:width, :]
        high, low = split(before)
        queries = query[span, :]
        carried = jnp.dot(queries, high, preferred_element_type=F32) + jnp.dot(
            queries, low, preferred_element_type=F32
        )
        state[0:width, :] = before * jnp.exp(end) + updates[block]
        retained = carried * jnp.exp(column) + inner[block]
        centered = retained - head_mean(retained)
        norm = centered * lax.rsqrt(head_mean(centered * centered) + eps)
        gate = gates[span, :].astype(F32)
        mixed = (norm * head_gain_ref[...] * (gate * jax.nn.sigmoid(gate))).astype(BF16)
        ret_rows[block] = mixed

        @pl.when(block == tp)
        def _():
            token_rows[tp] = mixed

        @pl.when(block > 0)
        def _():
            mix_start(block - 1)

    mix_start(blocks - 1)

    relay(0, 1)
    own_send(1)

    tokens = ids_ref.shape[0]
    chosen = ids_ref.shape[1]
    names = lax.broadcasted_iota(jnp.int32, (tokens, width), 1)
    ids = ids_ref[...]
    route = route_ref[...]
    match = names < 0
    weight = jnp.zeros((tokens, width), F32)
    for j in range(chosen):
        named = ids[:, j : j + 1] == names
        match = jnp.logical_or(match, named)
        weight = weight + jnp.where(named, route[:, j : j + 1], 0.0)
    strict = jnp.where(later > sooner, 1.0, 0.0).astype(BF16)
    position = jnp.dot(strict, jnp.where(match, 1.0, 0.0).astype(BF16), preferred_element_type=F32)
    place = jnp.where(match, position, -4096.0)
    places[...] = place.T[0 : places.shape[0], :]
    slots = lax.broadcasted_iota(jnp.int32, (tokens, specialists * capacity), 1).astype(F32)
    placed = jnp.zeros((tokens, specialists * capacity), F32)
    for index in range(specialists):
        spot = place[:, index : index + 1] + float(index * capacity)
        placed = jnp.where(slots == spot, weight[:, index : index + 1], placed)
    high, low = split(placed)
    back[0] = high
    back[1] = low

    for copy in local[4:6]:
        copy.wait()
    out_pair(tp, 0, True).wait_send()
    for step in range(1, chips):
        for other in range(1, places_count):
            out_piece(step, sp ^ other, out_xy_send.at[step - 1, other - 1], (sp ^ other, tp)).wait_recv()
        out_pair(((z + step) % chips) * 2 + core, step).start()
    for chip in range(chips):
        out_pair(chip * 2 + 1 - core, 0).wait_recv()
    for step in range(1, size):
        source = (tp + step) % size
        remote(
            ret_rows.at[0], token_rows.at[source], mix_send.at[0], mix_recv.at[source], (sp, source)
        ).wait_recv()

    squares[...] = jnp.zeros(squares.shape, F32)

    @pl.loop(0, size)
    def _(slot):
        span = pl.ds(pl.multiple_of(slot * out_columns, out_columns), out_columns)
        token = jnp.concatenate([token_rows[index] for index in range(size)], axis=1)
        mixer = jnp.dot(token, out_full[slot], preferred_element_type=F32)
        total = (residual[:, span].astype(F32) + mixer).astype(BF16)
        hidden[:, span] = total
        wide = total.astype(F32)
        wide = wide * wide
        squares[...] += functools.reduce(
            jnp.add, [wide[:, start : start + 128] for start in range(0, out_columns, 128)]
        )

    factor = lax.rsqrt(jnp.sum(squares[...], axis=1, keepdims=True) * (1.0 / depth) + eps)

    @pl.loop(0, depth // 256)
    def _(index):
        span = pl.ds(pl.multiple_of(index * 256, 256), 256)
        normed[:, span] = (hidden[:, span].astype(F32) * factor * norm_gain_ref[:, span]).astype(BF16)

    slot_rows = lax.broadcasted_iota(jnp.int32, (capacity, tokens), 0).astype(F32)

    def go(step):
        return remote(
            outgoing.at[step - 1], arrived.at[sp], go_send.at[step - 1], go_recv.at[sp], (sp ^ step, tp)
        )

    for step in list(range(places_count - 1, -1, -1)):
        sits = jnp.where(places[pl.ds(sp ^ step, 1), :] == slot_rows, 1.0, 0.0).astype(BF16)

        @pl.loop(0, depth // 512)
        def _(index):
            span = pl.ds(pl.multiple_of(index * 512, 512), 512)
            picked = jnp.dot(sits, normed[:, span], preferred_element_type=F32).astype(BF16)
            if step:
                outgoing[step - 1, :, span] = picked
            else:
                arrived[sp, :, span] = picked

        if step:
            go(step).start()

    relay(0, 2)
    relay(1, 1)

    for copy in local[6:9]:
        copy.wait()
    shared = shared_gate.shape[1]

    @pl.loop(0, shared // 256)
    def _(index):
        span = pl.ds(pl.multiple_of(index * 256, 256), 256)
        gated = jnp.dot(normed[...], shared_gate[:, span], preferred_element_type=F32)
        raised = jnp.dot(normed[...], shared_up[:, span], preferred_element_type=F32)
        shared_middle[:, span] = (gated * jax.nn.sigmoid(gated) * raised).astype(BF16)

    @pl.loop(0, depth // 512)
    def _(index):
        span = pl.ds(pl.multiple_of(index * 512, 512), 512)
        base[:, span] = hidden[:, span].astype(F32) + lax.dot_general(
            shared_middle[...], shared_down[span, :], NT, preferred_element_type=F32
        )

    relay(0, 3)
    relay(1, 2)
    for unit in range(2, len(units)):
        own_send(unit)

    for copy in local[9:]:
        copy.wait()
    for step in range(1, places_count):
        remote(
            outgoing.at[0], arrived.at[sp ^ step], go_send.at[0], go_recv.at[sp ^ step], (sp ^ step, tp)
        ).wait_recv()

    def pair_middle(chip):
        @pl.loop(0, specialists // 2)
        def _(index):
            rows_here = jnp.concatenate([arrived[2 * index], arrived[2 * index + 1]], axis=0)
            gate_pair = jnp.concatenate([weights[2 * chip, 0], weights[2 * chip + 1, 0]], axis=1)
            up_pair = jnp.concatenate([weights[2 * chip, 1], weights[2 * chip + 1, 1]], axis=1)
            gated = jnp.dot(rows_here, gate_pair, preferred_element_type=F32)
            raised = jnp.dot(rows_here, up_pair, preferred_element_type=F32)
            found = (gated * jax.nn.sigmoid(gated) * raised).astype(BF16)
            span = pl.ds(pl.multiple_of(index * 2 * capacity, 2 * capacity), 2 * capacity)
            middle[span, pl.ds(pl.multiple_of(chip * 2 * ff, 2 * ff), 2 * ff)] = found

    last_chip = jnp.where(z * 2 < chips, chips - 1, 0)

    def chip_at(index):
        if index == 0:
            return z
        if index == chips - 1:
            return last_chip
        toward = jnp.where(last_chip == 0, chips - 1 - index, index)
        shifted = jnp.where(last_chip == 0, chips - index, index - 1)
        passed = jnp.where(last_chip == 0, z <= chips - 1 - index, z >= index)
        return jnp.where(passed, shifted, toward)

    for index in range(chips):
        chip = chip_at(index)
        if index == chips - 1:
            relay(1, 3)
        for unit in (0, 1):
            from_partner(unit, chip)
        pair_middle(chip)

    def home(index, step, source):
        return remote(
            processed.at[index, source], returned.at[index, sp], back_send.at[index, step - 1],
            back_recv.at[index, sp], (source, tp),
        )

    for index in range(pieces):
        unit = 2 + index
        for distance in range(1, chips):
            relay(unit, distance)
        for chip in range(chips):
            from_partner(unit, chip)

        @pl.loop(0, piece // 256)
        def _(part):
            span = pl.ds(pl.multiple_of(index * piece + part * 256, 256), 256)
            down = jnp.concatenate([weights[slot, 2, span, :] for slot in range(size)], axis=1)
            columns = pl.ds(pl.multiple_of(part * 256, 256), 256)
            found = lax.dot_general(middle[...], down, NT, preferred_element_type=F32).astype(BF16)
            for source in range(specialists):
                own = found[source * capacity : (source + 1) * capacity, :]
                processed[index, source, :, columns] = own

                @pl.when(source == sp)
                def _():
                    returned[index, sp, :, columns] = own

        for step in range(1, places_count):
            home(index, step, sp ^ step).start()

    for index in range(pieces):
        for step in range(1, places_count):
            source = sp ^ step
            remote(
                processed.at[index, source], returned.at[index, source], back_send.at[index, step - 1],
                back_recv.at[index, source], (source, tp),
            ).wait_recv()

        rows_back = jnp.concatenate([returned[index, source] for source in range(specialists)], axis=0)
        routed = jnp.dot(back[0], rows_back, preferred_element_type=F32)
        routed += jnp.dot(back[1], rows_back, preferred_element_type=F32)
        span = slice(index * piece, (index + 1) * piece)
        result_ref[:, span] = (base[:, span] + routed).astype(BF16)

    for step in range(1, chips):
        out_z(step).wait_send()
        for other in range(1, places_count):
            out_piece(step, sp, out_xy_send.at[step - 1, other - 1], (sp ^ other, tp)).wait_send()
        out_pair(((z + step) % chips) * 2 + core, step).wait_send()

    @pl.loop(0, blocks)
    def _(block):
        @pl.when(block != tp)
        def _():
            mix_copy(block).wait_send()

    for step in range(1, places_count):
        go(step).wait_send()
        for index in range(pieces):
            home(index, step, sp ^ step).wait_send()
    for unit in range(len(units)):
        for origin in range(chips):
            slot = origin * 2 + core

            @pl.when(jnp.logical_and(origin <= z, z < chips - 1))
            def _():
                weight_copy(slot, unit, right_send.at[origin, unit], right).wait_send()

            @pl.when(jnp.logical_and(origin >= z, z > 0))
            def _():
                weight_copy(slot, unit, left_send.at[origin, unit], left).wait_send()

            weight_copy(slot, unit, pair_send.at[origin, unit], partner).wait_send()


def whole_layer(*arrays):
    (query, _, _, _, _, residual, head_gain, out_weight, norm_gain, ids, _, expert_gate) = arrays[:12]
    shared_gate = arrays[14]
    places_count, size = lax.axis_size("sp"), lax.axis_size("tp")
    rows_all, width = query.shape
    tokens, depth = residual.shape
    blocks = rows_all // tokens
    chosen = ids.shape[1]
    capacity = 3 * tokens * chosen // (2 * places_count)
    ff = expert_gate.shape[1]
    shared = shared_gate.shape[1]
    chips = size // 2
    pieces = 4
    units = 2 + pieces
    heads = width // HEAD
    dma = pltpu.SemaphoreType.DMA
    arrays = list(arrays)
    arrays[6] = head_gain[None, :]
    arrays[8] = norm_gain[None, :]
    small = (4, 6, 8, 9, 10)
    vmem, anywhere = pl.BlockSpec(memory_space=pltpu.VMEM), pl.BlockSpec(memory_space=pl.ANY)
    block = lambda *shape: pltpu.VMEM(shape, BF16)
    wide = lambda *shape: pltpu.VMEM(shape, F32)
    return pl.pallas_call(
        layer_kernel,
        in_specs=[vmem if index in small else anywhere for index in range(len(arrays))],
        out_specs=vmem,
        out_shape=jax.ShapeDtypeStruct((tokens, depth), BF16),
        scratch_shapes=[
            block(rows_all, width), block(rows_all, width), block(rows_all, width), block(rows_all, width),
            block(tokens, depth), block(depth, shared), block(depth, shared), block(depth, shared),
            block(size, 3, depth, ff),
            block(size, out_weight.shape[0], out_weight.shape[1]),
            wide(blocks, tokens, width),
            wide(heads * blocks, tokens),
            wide(blocks, width, width),
            wide(places_count, width + EXTRA, width),
            wide(width + EXTRA, width),
            wide(blocks, tokens, width),
            block(blocks, tokens, width),
            block(size, tokens, width),
            block(tokens, depth), block(tokens, depth),
            wide(tokens, 128),
            wide(8, tokens),
            block(places_count - 1, capacity, depth),
            block(places_count, capacity, depth),
            block(places_count * capacity, size * ff),
            block(pieces, places_count, capacity, depth // pieces),
            block(pieces, places_count, capacity, depth // pieces),
            wide(tokens, depth),
            block(tokens, shared),
            block(2, tokens, places_count * capacity),
            dma((12,)),
            dma((places_count - 1,)), dma((places_count,)),
            dma((blocks,)), dma((size,)),
            dma((chips - 1,)), dma((chips - 1, places_count - 1)), dma((size, places_count)),
            dma((chips,)), dma((size,)),
            dma((chips, units)), dma((chips, units)), dma((chips, units)), dma((size, units)),
            dma((places_count - 1,)), dma((places_count,)),
            dma((pieces, places_count - 1)), dma((pieces, places_count)),
        ],
        compiler_params=pltpu.CompilerParams(
            collective_id=0, has_side_effects=True, vmem_limit_bytes=66 * 1000 * 1000
        ),
        cost_estimate=pl.CostEstimate(
            flops=20 * 10**9, bytes_accessed=40 * 10**6, transcendentals=4 * 10**6
        ),
    )(*arrays)


def kernel_fits(mesh, shapes):
    places_count, size = mesh.shape["sp"], mesh.shape["tp"]
    if places_count != 4 or size % 2 or size < 4:
        return False
    width = shapes[0][1] // size
    tokens = shapes[5][0] // (places_count * size)
    rows_all = shapes[0][0] // places_count
    ff = shapes[11][1] // (places_count * size)
    return width == 128 and ff % 128 == 0 and tokens % 128 == 0 and rows_all == tokens * size


def solution(mesh):
    placed = (
        P("sp", "tp"),
        P("sp", "tp"),
        P("sp", "tp"),
        P("sp", "tp"),
        P("tp", "sp"),
        P(("sp", "tp"), None),
        P("tp"),
        P(None, "tp"),
        P(),
        P(("sp", "tp"), None),
        P(("sp", "tp"), None),
        P(None, ("sp", "tp")),
        P(None, ("sp", "tp")),
        P(None, ("sp", "tp")),
        P(),
        P(),
        P(),
    )

    placement = dict(mesh=mesh, in_specs=placed, out_specs=P(("sp", "tp"), None), check_vma=False)
    step = jax.shard_map(on_device, **placement)
    fused = jax.shard_map(whole_layer, **placement)

    def run(*arrays):
        fits = kernel_fits(mesh, [array.shape for array in arrays])
        return fused(*arrays) if fits else step(*arrays)

    return run
```

```python
import functools

import jax
import jax.numpy as jnp
from jax import lax
from jax.experimental import pallas as pl
from jax.experimental.pallas import tpu as pltpu
from jax.sharding import PartitionSpec as P


HEAD = 64
BLOCK = 256
EXTRA = 8


eps = 1e-05
F32 = jnp.float32
BF16 = jnp.bfloat16


def split(value):
    high = value.astype(BF16)
    return high, (value - high.astype(F32)).astype(BF16)


def per_head(columns, lanes):
    heads = columns.shape[1]
    out = jnp.broadcast_to(columns[:, 0:1], lanes.shape)
    for head in range(1, heads):
        out = jnp.where(lanes // HEAD == head, columns[:, head : head + 1], out)
    return out


def gathered_update(keys, values, column, lanes, end):
    scale = HEAD ** (-0.5)
    weighted = keys.astype(F32) * (jnp.exp(per_head(end - column, lanes)) * scale)
    high, low = split(weighted)
    dims = (((0,), (0,)), ((), ()))
    return lax.dot_general(high, values, dims, preferred_element_type=F32) + lax.dot_general(
        low, values, dims, preferred_element_type=F32
    )


def state_kernel(key_ref, value_ref, column_ref, out_ref):
    width = key_ref.shape[1]
    step = pl.program_id(0)

    @pl.when(step == 0)
    def _():
        out_ref[0:width, :] = jnp.zeros((width, width), F32)
        out_ref[width:, :] = jnp.zeros((EXTRA, width), F32)

    lanes = lax.broadcasted_iota(jnp.int32, key_ref.shape, 1)
    column = column_ref[...]
    end = column[BLOCK - 1 : BLOCK, :]
    end_lanes = per_head(end, lanes[0:1, :])
    fresh = gathered_update(key_ref[...], value_ref[...], column, lanes, end)
    out_ref[0:width, :] = out_ref[0:width, :] * jnp.exp(end_lanes) + fresh
    out_ref[width:, :] = out_ref[width:, :] + end_lanes


def retention_kernel(
    mine_ref, query_ref, key_ref, value_ref, gate_ref, column_ref, row_ref, gain_ref, states_ref,
    out_ref, state
):
    rows, width = query_ref.shape
    heads = width // HEAD
    step = pl.program_id(0)
    count = states_ref.shape[0]
    row_ids = lax.broadcasted_iota(jnp.int32, (width, width), 0) // HEAD
    column_ids = lax.broadcasted_iota(jnp.int32, (width, width), 1) // HEAD

    @pl.when(step == 0)
    def _():
        total = jnp.zeros((width, width), F32)
        for position in range(count - 1):
            decay = jnp.exp(states_ref[position, width : width + 1, :])
            longer = total * decay + states_ref[position, 0:width, :]
            total = jnp.where(position < mine_ref[0], longer, total)
        state[...] = jnp.where(row_ids == column_ids, total, 0.0)

    lanes = lax.broadcasted_iota(jnp.int32, (rows, width), 1)
    queries, keys, values = query_ref[...], key_ref[...], value_ref[...]
    column = column_ref[...]
    end = column[rows - 1 : rows, :]
    causal = lax.broadcasted_iota(jnp.int32, (rows, rows), 0) >= lax.broadcasted_iota(
        jnp.int32, (rows, rows), 1
    )
    scale = HEAD ** (-0.5)
    high, low = split(state[...])
    carried = jnp.dot(queries, high, preferred_element_type=F32) + jnp.dot(
        queries, low, preferred_element_type=F32
    )
    retained = carried * jnp.exp(per_head(column, lanes))
    inner = None
    for head in range(heads):
        own = jnp.where(lanes // HEAD == head, queries.astype(F32), 0.0).astype(BF16)
        scores = lax.dot_general(
            own, keys, (((1,), (1,)), ((), ())), preferred_element_type=F32
        )
        spread = column[:, head : head + 1] - row_ref[0, head : head + 1, :]
        damping = jnp.exp(jnp.where(causal, spread, -jnp.inf))
        factor = (scores * scale * damping).astype(BF16)
        term = jnp.dot(factor, values, preferred_element_type=F32)
        inner = term if inner is None else jnp.where(lanes // HEAD == head, term, inner)
    retained = retained + inner
    fresh = gathered_update(keys, values, column, lanes, end)
    end_lanes = per_head(end, lanes[0:1, :])
    state[...] = state[...] * jnp.exp(end_lanes) + jnp.where(row_ids == column_ids, fresh, 0.0)

    def head_mean(array):
        out = None
        for head in range(heads):
            inside = lanes // HEAD == head
            mean = jnp.sum(jnp.where(inside, array, 0.0), axis=1, keepdims=True) * (1.0 / HEAD)
            out = jnp.broadcast_to(mean, array.shape) if out is None else jnp.where(inside, mean, out)
        return out

    centered = retained - head_mean(retained)
    normed = centered * lax.rsqrt(head_mean(centered * centered) + eps)
    gates = gate_ref[...].astype(F32)
    out_ref[...] = (normed * gain_ref[...] * (gates * jax.nn.sigmoid(gates))).astype(BF16)


def retention(query_rows, key_rows, value_rows, gate_rows, log_decay, head_gain):
    rows, width = query_rows.shape
    heads = width // HEAD
    count = rows // BLOCK
    running = jnp.cumsum(log_decay.reshape(heads, count, BLOCK), axis=2)
    row = running.transpose(1, 0, 2)
    column = running.reshape(heads, rows).T
    block = pl.BlockSpec((BLOCK, width), lambda i: (i, 0))
    column_block = pl.BlockSpec((BLOCK, heads), lambda i: (i, 0))
    state_call = pl.pallas_call(
        state_kernel,
        grid=(count,),
        in_specs=[block, block, column_block],
        out_specs=pl.BlockSpec((width + EXTRA, width), lambda i: (0, 0)),
        out_shape=jax.ShapeDtypeStruct((width + EXTRA, width), F32),
        compiler_params=pltpu.CompilerParams(dimension_semantics=("arbitrary",)),
        cost_estimate=pl.CostEstimate(
            flops=4 * rows * width * width, bytes_accessed=4 * rows * width, transcendentals=rows * width
        ),
    )
    own = state_call(key_rows, value_rows, column)
    states = lax.all_gather(own, "sp")
    mine = lax.axis_index("sp").astype(jnp.int32).reshape(1)
    return pl.pallas_call(
        retention_kernel,
        grid=(count,),
        in_specs=[
            pl.BlockSpec(memory_space=pltpu.SMEM),
            block,
            block,
            block,
            block,
            column_block,
            pl.BlockSpec((1, heads, BLOCK), lambda i: (i, 0, 0)),
            pl.BlockSpec((1, width), lambda i: (0, 0)),
            pl.BlockSpec(states.shape, lambda i: (0, 0, 0)),
        ],
        out_specs=block,
        out_shape=jax.ShapeDtypeStruct((rows, width), BF16),
        scratch_shapes=[pltpu.VMEM((width, width), F32)],
        compiler_params=pltpu.CompilerParams(dimension_semantics=("arbitrary",)),
        cost_estimate=pl.CostEstimate(
            flops=8 * rows * width * BLOCK,
            bytes_accessed=10 * rows * width,
            transcendentals=rows * BLOCK * heads,
        ),
    )(mine, query_rows, key_rows, value_rows, gate_rows, column, row, head_gain[None, :], states)


def send(piece, pairs):
    return lax.ppermute(piece, "tp", pairs)


def ring_start(own):
    size = lax.axis_size("tp")
    right = [(i, (i + 2) % size) for i in range(size)]
    left = [(i, (i - 2) % size) for i in range(size)]
    swap = [(i, i ^ 1) for i in range(size)]
    return send(own, right), send(own, left), send(own, swap)


def ring_finish(own, from_left, from_right, other):
    size = lax.axis_size("tp")
    chips = size // 2
    right = [(i, (i + 2) % size) for i in range(size)]
    left = [(i, (i - 2) % size) for i in range(size)]
    swap = [(i, i ^ 1) for i in range(size)]
    half = own.shape[1] // 2
    last = chips // 2
    pieces = [[own], [other]]
    for hop in range(1, (chips - 1) // 2 + 1):
        if hop > 1:
            from_left = send(from_left, right)
            from_right = send(from_right, left)
        for piece in (from_left, from_right):
            pieces += [[piece], [send(piece, swap)]]
    if chips % 2 == 0 and last > 1:
        first = send(from_left[:, :half], right)
        second = send(from_right[:, half:], left)
        pieces += [[first, second], [send(first, swap), send(second, swap)]]
    elif chips == 2:
        pieces += [[from_left], [send(from_left, swap)]]
    return pieces


def expert_kernel(layout, row_ref, *refs):
    count = len(layout)
    piece_refs, out_ref = refs[:count], refs[count]
    weights, middle, sems = refs[count + 1 :]
    slots, _, width, ff = weights.shape
    rows = row_ref.shape[0]
    copies = []
    for index, (slot, start, length) in enumerate(layout):
        copy = pltpu.make_async_copy(
            piece_refs[index], weights.at[slot, :, pl.ds(start, length), :], sems.at[index]
        )
        copy.start()
        copies.append(copy)
    tile = rows // 2
    for pair in range(slots // 2):
        for index, (slot, _, _) in enumerate(layout):
            if slot // 2 == pair:
                copies[index].wait()

        @pl.loop(0, 2)
        def _(step):
            span = pl.ds(pl.multiple_of(step * tile, tile), tile)
            block = row_ref[span, :]
            gate = jnp.concatenate([weights[2 * pair, 0], weights[2 * pair + 1, 0]], axis=1)
            up = jnp.concatenate([weights[2 * pair, 1], weights[2 * pair + 1, 1]], axis=1)
            gated = jnp.dot(block, gate, preferred_element_type=F32)
            raised = jnp.dot(block, up, preferred_element_type=F32)
            value = gated * jax.nn.sigmoid(gated) * raised
            middle[span, 2 * pair * ff : 2 * (pair + 1) * ff] = value.astype(BF16)

    part = 512

    @pl.loop(0, width // part)
    def _(step):
        span = pl.ds(pl.multiple_of(step * part, part), part)
        down = jnp.concatenate([weights[slot, 2, span, :] for slot in range(slots)], axis=1)
        out_ref[:, span] = lax.dot_general(
            middle[...], down, (((1,), (1,)), ((), ())), preferred_element_type=F32
        ).astype(BF16)


def experts(rows, shards):
    _, width, ff = shards[0][0].shape
    count = len(shards)
    if ff % 128 or count % 2:
        whole = jnp.concatenate([jnp.concatenate(shard, axis=1) for shard in shards], axis=2)
        middle = (
            jax.nn.silu(jnp.dot(rows, whole[0], preferred_element_type=F32))
            * jnp.dot(rows, whole[1], preferred_element_type=F32)
        ).astype(BF16)
        return lax.dot_general(
            middle, whole[2], (((1,), (1,)), ((), ())), preferred_element_type=F32
        ).astype(BF16)
    layout, pieces = [], []
    for slot, shard in enumerate(shards):
        start = 0
        for piece in shard:
            layout.append((slot, start, piece.shape[1]))
            pieces.append(piece)
            start += piece.shape[1]
    return pl.pallas_call(
        functools.partial(expert_kernel, layout),
        in_specs=[pl.BlockSpec(memory_space=pltpu.VMEM)]
        + [pl.BlockSpec(memory_space=pl.ANY)] * len(pieces),
        out_specs=pl.BlockSpec(memory_space=pltpu.VMEM),
        out_shape=jax.ShapeDtypeStruct(rows.shape, BF16),
        scratch_shapes=[
            pltpu.VMEM((count, 3, width, ff), BF16),
            pltpu.VMEM((rows.shape[0], count * ff), BF16),
            pltpu.SemaphoreType.DMA((len(pieces),)),
        ],
        compiler_params=pltpu.CompilerParams(vmem_limit_bytes=60 * 1024 * 1024),
        cost_estimate=pl.CostEstimate(
            flops=6 * rows.shape[0] * width * count * ff,
            bytes_accessed=6 * width * count * ff + 4 * rows.size,
            transcendentals=rows.shape[0] * count * ff,
        ),
    )(rows, *pieces)


def on_device(
    query_rows,
    key_rows,
    value_rows,
    gate_rows,
    log_decay,
    residual,
    head_gain,
    out_weight,
    norm_gain,
    expert_ids,
    route_weights,
    expert_gate,
    expert_up,
    expert_down,
    shared_gate,
    shared_up,
    shared_down,
):
    part = out_weight.shape[0] // lax.axis_size("sp")
    own_part = lax.dynamic_slice_in_dim(out_weight, lax.axis_index("sp") * part, part, 0)
    out_part = lax.all_gather(own_part, "tp", axis=1, tiled=True)
    out_full = lax.all_gather(out_part, "sp", axis=0, tiled=True)
    shard = jnp.stack([expert_gate, expert_up, expert_down])
    shard, log_decay = lax.optimization_barrier((shard, log_decay))
    from_left, from_right, other = ring_start(shard)

    specialists = lax.axis_size("sp")
    tokens, chosen = expert_ids.shape
    width = residual.shape[1]
    capacity = 3 * tokens * chosen // (2 * specialists)
    names = jnp.arange(specialists, dtype=jnp.int32)[:, None]
    named = [expert_ids[:, j][None, :] == names for j in range(chosen)]
    match = functools.reduce(jnp.logical_or, named)
    weight = sum(jnp.where(named[j], route_weights[:, j][None, :], 0.0) for j in range(chosen))
    earlier = jnp.arange(tokens)[:, None] < jnp.arange(tokens)[None, :]
    position = jnp.dot(match.astype(BF16), earlier.astype(BF16), preferred_element_type=F32)
    place = jnp.where(match, position.astype(jnp.int32), -1)
    sits = place[:, None, :] == jnp.arange(capacity, dtype=jnp.int32)[None, :, None]
    pick = sits.astype(BF16).reshape(specialists * capacity, tokens)
    weight_high = lax.reduce_precision(weight, 8, 7)
    weight_low = weight - weight_high
    back_high = jnp.where(sits, weight_high[:, None, :], 0.0).astype(BF16)
    back_low = jnp.where(sits, weight_low[:, None, :], 0.0).astype(BF16)

    ret_rows = retention(query_rows, key_rows, value_rows, gate_rows, log_decay, head_gain)
    token_rows = lax.all_to_all(ret_rows, "tp", split_axis=0, concat_axis=1, tiled=True)
    token_rows, from_left, from_right = lax.optimization_barrier((token_rows, from_left, from_right))
    shards = ring_finish(shard, from_left, from_right, other)
    mixer = jnp.dot(token_rows, out_full, preferred_element_type=F32)
    hidden = (residual.astype(F32) + mixer).astype(BF16)
    hidden_wide = hidden.astype(F32)
    normed_rows = (
        hidden_wide
        * lax.rsqrt(jnp.mean(hidden_wide * hidden_wide, axis=1, keepdims=True) + eps)
        * norm_gain
    ).astype(BF16)
    outgoing = jnp.dot(pick, normed_rows, preferred_element_type=F32).astype(BF16)
    outgoing = outgoing.reshape(specialists, capacity, width)
    arrived = lax.all_to_all(outgoing, "sp", split_axis=0, concat_axis=0, tiled=True)
    shared_mid = (
        jax.nn.silu(jnp.dot(normed_rows, shared_gate, preferred_element_type=F32))
        * jnp.dot(normed_rows, shared_up, preferred_element_type=F32)
    ).astype(BF16)
    shared_out = lax.dot_general(
        shared_mid, shared_down, (((1,), (1,)), ((), ())), preferred_element_type=F32
    )
    flat_rows = arrived.reshape(-1, width)
    processed = experts(flat_rows, shards).reshape(arrived.shape)
    returned = lax.all_to_all(processed, "sp", split_axis=0, concat_axis=0, tiled=True)
    dims = (((0, 1), (0, 1)), ((), ()))
    routed = lax.dot_general(back_high, returned, dims, preferred_element_type=F32)
    routed += lax.dot_general(back_low, returned, dims, preferred_element_type=F32)
    return (hidden_wide + routed + shared_out).astype(BF16)


MESH = pl.DeviceIdType.MESH
NT = (((1,), (1,)), ((), ()))
TN = (((0,), (0,)), ((), ()))


def thirds(value):
    first = value.astype(BF16)
    rest = value - first.astype(F32)
    second = rest.astype(BF16)
    return first, second, (rest - second.astype(F32)).astype(BF16)


def piece_widths(depth):
    return [128] + [256] * ((depth - 256) // 256) + [128]


def layer_kernel(
    query_hbm, key_hbm, value_hbm, gate_hbm, decay_hbm, residual_hbm, head_gain_hbm, out_weight_hbm,
    norm_gain_hbm, ids_hbm, route_hbm, expert_gate_hbm, expert_up_hbm, expert_down_hbm,
    shared_gate_hbm, shared_up_hbm, shared_down_hbm,
    result_ref,
    decay_ref, head_gain_ref, norm_gain_ref, ids_ref, route_ref,
    query, key, value, gates, residual, shared_gate, shared_up, shared_down,
    weights, out_full, running, row_running, updates, states, state, inner, ret_rows, token_rows,
    hidden, normed, squares, tables, outgoing, arrived, middle, processed, direct, passing, merged,
    combined, final, base, shared_middle, back,
    local_sem, state_send, state_recv, mix_send, mix_recv, out_z_send, out_xy_send, out_z_recv, out_xy_recv,
    out_pair_send, out_pair_recv, right_send, left_send, pair_send, line_recv, pair_recv, pair_down_recv,
    go_send, go_recv, table_send, table_recv, direct_send, direct_recv, passing_send, passing_recv,
    merged_send, merged_recv, final_send, final_recv,
):
    places_count = states.shape[0]
    size = token_rows.shape[0]
    chips = size // 2
    sp = lax.axis_index("sp")
    tp = lax.axis_index("tp")
    z, core = tp // 2, tp % 2
    blocks, rows, width = ret_rows.shape
    heads = width // HEAD
    depth = residual.shape[1]
    capacity = arrived.shape[1]
    specialists = arrived.shape[0]
    ff = weights.shape[3]
    quarter = out_full.shape[1] // places_count
    out_columns = out_full.shape[2]
    widths = piece_widths(depth)
    pieces = len(widths)
    starts = [sum(widths[:index]) for index in range(pieces)]
    half = depth // 2
    scale = HEAD ** (-0.5)
    inputs = (expert_gate_hbm, expert_up_hbm, expert_down_hbm)
    units = [(which, start, half) for which in (0, 1) for start in (0, half)]
    first_down = len(units)
    units += [(2, start, length) for start, length in zip(starts, widths)]

    def remote(src, dst, send, recv, device):
        return pltpu.make_async_remote_copy(
            src_ref=src, dst_ref=dst, send_sem=send, recv_sem=recv, device_id=device, device_id_type=MESH
        )

    partner = (sp, z * 2 + 1 - core)
    right = (sp, tp + 2)
    left = (sp, tp - 2)

    local = [
        pltpu.make_async_copy(src, dst, local_sem.at[index])
        for index, (src, dst) in enumerate(
            [
                (decay_hbm, decay_ref),
                (ids_hbm, ids_ref),
                (route_hbm, route_ref),
                (key_hbm, key),
                (value_hbm, value),
                (query_hbm, query),
                (gate_hbm, gates),
                (head_gain_hbm, head_gain_ref),
                (norm_gain_hbm, norm_gain_ref),
                (out_weight_hbm, out_full.at[tp]),
                (residual_hbm, residual),
                (shared_gate_hbm, shared_gate),
                (shared_up_hbm, shared_up),
                (shared_down_hbm, shared_down),
                (expert_gate_hbm, weights.at[tp, 0]),
                (expert_up_hbm, weights.at[tp, 1]),
                (expert_down_hbm, weights.at[tp, 2]),
            ]
        )
    ]
    for copy in local[:9]:
        copy.start()

    barrier = pltpu.get_barrier_semaphore()
    for step in range(1, size):
        pl.semaphore_signal(barrier, inc=1, device_id=(sp, (tp + step) % size), device_id_type=MESH)
    for step in range(1, places_count):
        pl.semaphore_signal(barrier, inc=1, device_id=(sp ^ step, tp), device_id_type=MESH)
    pl.semaphore_wait(barrier, size - 1 + places_count - 1)

    def weight_copy(origin, unit, send, device, own=False, pair=False):
        which, start, length = units[unit]
        span = pl.ds(start, length)
        there = weights.at[origin * 2 + core, which, span, :]
        here = inputs[which].at[span, :] if own else there
        if not pair:
            received = line_recv.at[origin, unit]
        elif unit < first_down:
            received = pair_recv.at[origin]
        else:
            received = pair_down_recv.at[unit - first_down]
        return remote(here, there, send, received, device)

    def to_partner(origin, unit, own=False):
        return weight_copy(origin, unit, pair_send.at[origin], partner, own, True)

    def own_send(unit):
        @pl.when(z < chips - 1)
        def _():
            weight_copy(z, unit, right_send.at[z], right, True).start()

        @pl.when(z > 0)
        def _():
            weight_copy(z, unit, left_send.at[z], left, True).start()

        to_partner(z, unit, True).start()

    def relay(unit, distance):
        @pl.when(z - distance >= 0)
        def _():
            origin = z - distance
            copy = weight_copy(origin, unit, right_send.at[origin], right)
            copy.wait_recv()

            @pl.when(z < chips - 1)
            def _():
                copy.start()

            to_partner(origin, unit).start()

        @pl.when(z + distance < chips)
        def _():
            origin = z + distance
            copy = weight_copy(origin, unit, left_send.at[origin], left)
            copy.wait_recv()

            @pl.when(z > 0)
            def _():
                copy.start()

            to_partner(origin, unit).start()

    def from_partner(origin):
        there = weights.at[0, 0:2]
        remote(there, there, pair_send.at[origin], pair_recv.at[origin], partner).wait_recv()

    def downs_from_partner(index):
        there = weights.at[0, 2, pl.ds(0, chips * widths[index]), :]
        remote(there, there, pair_send.at[0], pair_down_recv.at[index], partner).wait_recv()

    def out_z(step):
        target = (z + step) % chips
        span = pl.ds(pl.multiple_of(sp * quarter, quarter), quarter)
        return remote(
            out_weight_hbm.at[span, :], out_full.at[tp, span, :], out_z_send, out_z_recv.at[z],
            (sp, target * 2 + core),
        )

    def out_z_arrival(step):
        origin = (z + step) % chips
        there = out_full.at[0, pl.ds(0, quarter), :]
        return remote(there, there, out_z_send, out_z_recv.at[origin], partner)

    def out_piece(step, device):
        origin = (z + step) % chips
        span = pl.ds(pl.multiple_of(sp * quarter, quarter), quarter)
        there = out_full.at[origin * 2 + core, span, :]
        return remote(there, there, out_xy_send.at[step - 1], out_xy_recv.at[origin], device)

    def out_pieces(step):
        origin = (z + step) % chips
        there = out_full.at[0, pl.ds(0, (places_count - 1) * quarter), :]
        return remote(there, there, out_xy_send.at[step - 1], out_xy_recv.at[origin], partner)

    def out_pair(slot, own=False):
        return remote(
            out_weight_hbm if own else out_full.at[slot], out_full.at[slot], out_pair_send,
            out_pair_recv, partner,
        )

    def out_pairs():
        there = out_full.at[0:chips]
        return remote(there, there, out_pair_send, out_pair_recv, partner)

    for step in range(1, chips):
        out_z(step).start()
    own_send(0)
    own_send(1)
    out_pair(tp, True).start()
    for copy in local[9:]:
        copy.start()

    for copy in local[:3]:
        copy.wait()

    row_ids = lax.broadcasted_iota(jnp.int32, (width, width), 0) // HEAD
    column_ids = lax.broadcasted_iota(jnp.int32, (width, width), 1) // HEAD
    same_head = row_ids == column_ids
    lanes = lax.broadcasted_iota(jnp.int32, (rows, width), 1)
    later = lax.broadcasted_iota(jnp.int32, (rows, rows), 0)
    sooner = lax.broadcasted_iota(jnp.int32, (rows, rows), 1)
    lower = jnp.where(later >= sooner, 1.0, 0.0).astype(BF16)
    upper = jnp.where(later <= sooner, 1.0, 0.0).astype(BF16)

    chosen, tokens = ids_ref.shape
    names = lax.broadcasted_iota(jnp.int32, (8, tokens), 0)
    match = names < 0
    weight = jnp.zeros((8, tokens), F32)
    for j in range(chosen):
        named = ids_ref[j : j + 1, :] == names
        match = jnp.logical_or(match, named)
        weight = weight + jnp.where(named, route_ref[j : j + 1, :], 0.0)
    strict = jnp.where(later < sooner, 1.0, 0.0).astype(BF16)
    position = jnp.dot(jnp.where(match, 1.0, 0.0).astype(BF16), strict, preferred_element_type=F32)
    tables[0, 0:8, :] = jnp.where(match, position, -1.0)
    tables[0, 8:16, :] = weight

    def table_copy(step):
        return remote(
            tables.at[0], tables.at[step], table_send, table_recv.at[step - 1], (sp ^ step, tp)
        )

    listed = jnp.concatenate(
        [
            decay_ref[head : head + 1, block * rows : (block + 1) * rows]
            for head in range(heads)
            for block in range(blocks)
        ],
        axis=0,
    )
    row_running[...] = functools.reduce(
        jnp.add, [jnp.dot(part, upper, preferred_element_type=F32) for part in thirds(listed)]
    )
    head_rows = lax.broadcasted_iota(jnp.int32, (width, rows), 0) // HEAD
    for block in range(blocks):
        spread = jnp.broadcast_to(listed[block : block + 1, :], (width, rows))
        for head in range(1, heads):
            spread = jnp.where(
                head_rows == head, listed[head * blocks + block : head * blocks + block + 1, :], spread
            )
        running[block] = functools.reduce(
            jnp.add,
            [
                lax.dot_general(lower, part, NT, preferred_element_type=F32)
                for part in thirds(spread)
            ],
        )

    for copy in local[3:5]:
        copy.wait()
    state[...] = jnp.zeros((width + EXTRA, width), F32)

    @pl.loop(0, blocks)
    def _(block):
        span = pl.ds(pl.multiple_of(block * rows, rows), rows)
        column = running[block]
        end = column[rows - 1 : rows, :]
        weighted = key[span, :].astype(F32) * (jnp.exp(end - column) * scale)
        high, low = split(weighted)
        fresh = lax.dot_general(high, value[span, :], TN, preferred_element_type=F32)
        fresh += lax.dot_general(low, value[span, :], TN, preferred_element_type=F32)
        fresh = jnp.where(same_head, fresh, 0.0)
        updates[block] = fresh
        state[0:width, :] = state[0:width, :] * jnp.exp(end) + fresh
        state[width:, :] = state[width:, :] + end

    states[sp] = state[...]

    def state_copy(step):
        return remote(
            state, states.at[sp], state_send, state_recv.at[sp], (sp ^ step, tp)
        )

    def state_arrival(step):
        return remote(
            state, states.at[sp ^ step], state_send, state_recv.at[sp ^ step], (sp ^ step, tp)
        )

    local[5].wait()
    for step in range(1, places_count):
        state_copy(step).start()
    for step in (1, 2):
        table_copy(step).start()

    @pl.loop(0, blocks)
    def _(block):
        span = pl.ds(pl.multiple_of(block * rows, rows), rows)
        queries, keys, values = query[span, :], key[span, :], value[span, :]
        column = running[block]
        causal = later >= sooner
        total = None
        for head in range(heads):
            own = jnp.where(lanes // HEAD == head, queries.astype(F32), 0.0).astype(BF16)
            scores = lax.dot_general(own, keys, NT, preferred_element_type=F32)
            spread = column[:, head * HEAD : head * HEAD + 1] - row_running[pl.ds(head * blocks + block, 1), :]
            damping = jnp.exp(jnp.where(causal, spread, -jnp.inf))
            factor = (scores * scale * damping).astype(BF16)
            term = jnp.dot(factor, values, preferred_element_type=F32)
            total = term if total is None else jnp.where(lanes // HEAD == head, term, total)
        inner[block] = total

    for step in range(1, chips):
        out_z_arrival(step).wait_recv()
        for other in range(1, places_count):
            out_piece(step, (sp ^ other, tp)).start()

    for step in range(1, places_count):
        state_arrival(step).wait_recv()
    there = states.at[pl.ds(0, places_count - 1)]
    remote(there, there, state_send, state_recv.at[0], partner).wait_send()
    total = jnp.zeros((width, width), F32)
    for position in range(places_count - 1):
        longer = total * jnp.exp(states[position, width : width + 1, :]) + states[position, 0:width, :]
        total = jnp.where(position < sp, longer, total)
    state[0:width, :] = total
    local[6].wait()
    local[7].wait()

    def head_mean(array):
        out = None
        for head in range(heads):
            inside = lanes // HEAD == head
            mean = jnp.sum(jnp.where(inside, array, 0.0), axis=1, keepdims=True) * (1.0 / HEAD)
            out = jnp.broadcast_to(mean, array.shape) if out is None else jnp.where(inside, mean, out)
        return out

    def mix_copy(block):
        return remote(
            ret_rows.at[block], token_rows.at[tp], mix_send, mix_recv.at[tp], (sp, block)
        )

    def mix_start(block):
        @pl.when(block != tp)
        def _():
            mix_copy(block).start()

    @pl.loop(0, blocks)
    def _(block):
        span = pl.ds(pl.multiple_of(block * rows, rows), rows)
        column = running[block]
        end = column[rows - 1 : rows, :]
        before = state[0:width, :]
        high, low = split(before)
        queries = query[span, :]
        carried = jnp.dot(queries, high, preferred_element_type=F32) + jnp.dot(
            queries, low, preferred_element_type=F32
        )
        state[0:width, :] = before * jnp.exp(end) + updates[block]
        retained = carried * jnp.exp(column) + inner[block]
        centered = retained - head_mean(retained)
        norm = centered * lax.rsqrt(head_mean(centered * centered) + eps)
        gate = gates[span, :].astype(F32)
        mixed = (norm * head_gain_ref[...] * (gate * jax.nn.sigmoid(gate))).astype(BF16)
        ret_rows[block] = mixed

        @pl.when(block == tp)
        def _():
            token_rows[tp] = mixed

        @pl.when(block > 0)
        def _():
            mix_start(block - 1)

    mix_start(blocks - 1)

    relay(0, 1)
    own_send(2)
    relay(1, 1)
    own_send(3)

    slot_rows = lax.broadcasted_iota(jnp.int32, (capacity, tokens), 0).astype(F32)
    for step in (1, 2):
        table_copy(step).wait_recv()
    for turn, (table, pair) in enumerate(
        ((0, (0, 2)), (0, (0, 1)), (1, (0, 2)), (2, (0, 1)), (0, (2, 3)))
    ):
        parts = []
        for other in pair:
            name = sp ^ other
            place = tables[table, pl.ds(name, 1), :]
            parts.append(jnp.where(place == slot_rows, tables[table, pl.ds(8 + name, 1), :], 0.0))
        high, low = split(jnp.concatenate(parts, axis=0).T)
        back[turn, 0] = high
        back[turn, 1] = low

    for copy in local[8:11]:
        copy.wait()
    for step in range(1, chips):
        out_pieces(step).wait_recv()
        out_pair(((z + step) % chips) * 2 + core).start()
    out_pairs().wait_recv()
    for step in range(1, size):
        source = (tp + step) % size
        remote(
            ret_rows.at[0], token_rows.at[source], mix_send, mix_recv.at[source], (sp, source)
        ).wait_recv()

    squares[...] = jnp.zeros(squares.shape, F32)

    @pl.loop(0, size)
    def _(slot):
        span = pl.ds(pl.multiple_of(slot * out_columns, out_columns), out_columns)
        token = jnp.concatenate([token_rows[index] for index in range(size)], axis=1)
        mixer = jnp.dot(token, out_full[slot], preferred_element_type=F32)
        total = (residual[:, span].astype(F32) + mixer).astype(BF16)
        hidden[:, span] = total
        wide = total.astype(F32)
        wide = wide * wide
        squares[...] += functools.reduce(
            jnp.add, [wide[:, start : start + 128] for start in range(0, out_columns, 128)]
        )

    factor = lax.rsqrt(jnp.sum(squares[...], axis=1, keepdims=True) * (1.0 / depth) + eps)

    @pl.loop(0, depth // 256)
    def _(index):
        span = pl.ds(pl.multiple_of(index * 256, 256), 256)
        normed[:, span] = (hidden[:, span].astype(F32) * factor * norm_gain_ref[:, span]).astype(BF16)

    relay(0, 2)

    def go(step):
        return remote(
            outgoing.at[step - 1], arrived.at[sp], go_send, go_recv.at[sp], (sp ^ step, tp)
        )

    for step in list(range(places_count - 1, -1, -1)):
        sits = jnp.where(tables[0, pl.ds(sp ^ step, 1), :] == slot_rows, 1.0, 0.0).astype(BF16)

        @pl.loop(0, depth // 512)
        def _(index):
            span = pl.ds(pl.multiple_of(index * 512, 512), 512)
            picked = jnp.dot(sits, normed[:, span], preferred_element_type=F32).astype(BF16)
            if step:
                outgoing[step - 1, :, span] = picked
            else:
                arrived[sp, :, span] = picked

        if step:
            go(step).start()

    relay(1, 2)
    relay(2, 1)

    for copy in local[11:14]:
        copy.wait()
    shared = shared_gate.shape[1]

    @pl.loop(0, shared // 256)
    def _(index):
        span = pl.ds(pl.multiple_of(index * 256, 256), 256)
        gated = jnp.dot(normed[...], shared_gate[:, span], preferred_element_type=F32)
        raised = jnp.dot(normed[...], shared_up[:, span], preferred_element_type=F32)
        shared_middle[:, span] = (gated * jax.nn.sigmoid(gated) * raised).astype(BF16)

    @pl.loop(0, depth // 512)
    def _(index):
        span = pl.ds(pl.multiple_of(index * 512, 512), 512)
        base[:, span] = hidden[:, span].astype(F32) + lax.dot_general(
            shared_middle[...], shared_down[span, :], NT, preferred_element_type=F32
        )

    relay(0, 3)
    relay(3, 1)
    relay(2, 2)
    relay(1, 3)
    relay(3, 2)
    own_send(first_down)
    own_send(first_down + 1)
    own_send(first_down + 2)

    for copy in local[14:]:
        copy.wait()
    for step in range(1, places_count):
        remote(
            outgoing.at[0], arrived.at[sp ^ step], go_send, go_recv.at[sp ^ step], (sp ^ step, tp)
        ).wait_recv()

    def pair_middle(chip):
        @pl.loop(0, specialists // 2)
        def _(index):
            rows_here = jnp.concatenate([arrived[2 * index], arrived[2 * index + 1]], axis=0)
            gate_pair = jnp.concatenate([weights[2 * chip, 0], weights[2 * chip + 1, 0]], axis=1)
            up_pair = jnp.concatenate([weights[2 * chip, 1], weights[2 * chip + 1, 1]], axis=1)
            gated = jnp.dot(rows_here, gate_pair, preferred_element_type=F32)
            raised = jnp.dot(rows_here, up_pair, preferred_element_type=F32)
            found = (gated * jax.nn.sigmoid(gated) * raised).astype(BF16)
            span = pl.ds(pl.multiple_of(index * 2 * capacity, 2 * capacity), 2 * capacity)
            middle[span, pl.ds(pl.multiple_of(chip * 2 * ff, 2 * ff), 2 * ff)] = found

    last_chip = jnp.where(z * 2 < chips, chips - 1, 0)

    def chip_at(index):
        if index == 0:
            return z
        if index == chips - 1:
            return last_chip
        toward = jnp.where(last_chip == 0, chips - 1 - index, index)
        shifted = jnp.where(last_chip == 0, chips - index, index - 1)
        passed = jnp.where(last_chip == 0, z <= chips - 1 - index, z >= index)
        return jnp.where(passed, shifted, toward)

    for index in range(chips):
        chip = chip_at(index)
        if index == chips - 1:
            relay(2, 3)
            relay(3, 3)
        from_partner(chip)
        pair_middle(chip)

    tile = processed.shape[3]

    def tiles(index):
        return range(starts[index] // tile, (starts[index] + widths[index]) // tile)

    def piece_of(number):
        return next(index for index in range(pieces) if number in tiles(index))

    def arrivals(buffer, send, received, index):
        there = buffer.at[pl.ds(starts[index] // tile, widths[index] // tile)]
        remote(there, there, send, received.at[index], partner).wait_recv()

    def near(number):
        return sp ^ (2, 1)[number % 2]

    def far(number):
        return sp ^ (1, 2)[number % 2]

    def direct_copy(number):
        return remote(
            processed.at[number, near(number)], direct.at[number], direct_send,
            direct_recv.at[piece_of(number)], (near(number), tp),
        )

    def passing_copy(number):
        return remote(
            processed.at[number, sp ^ 3], passing.at[number], passing_send,
            passing_recv.at[piece_of(number)], (near(number), tp),
        )

    def merged_copy(number):
        return remote(
            merged.at[number], combined.at[number], merged_send,
            merged_recv.at[piece_of(number)], (far(number), tp),
        )

    def weighted(turn, first, second):
        rows_back = jnp.concatenate([first, second], axis=0)
        return jnp.dot(back[turn, 0], rows_back, preferred_element_type=F32) + jnp.dot(
            back[turn, 1], rows_back, preferred_element_type=F32
        )

    def merge(index):
        arrivals(passing, passing_send, passing_recv, index)
        for number in tiles(index):
            found = weighted(2 + number % 2, processed[number, far(number)], passing[number])
            merged[number] = found.astype(BF16)
        for number in tiles(index):
            merged_copy(number).start()

    last_tile = depth // tile - 1

    def final_copy(step):
        return remote(
            processed.at[last_tile, sp ^ step], final.at[step - 1], final_send, final_recv, (sp ^ step, tp)
        )

    def store(number, routed):
        span = slice(number * tile, (number + 1) * tile)
        result_ref[:, span] = (base[:, span] + routed).astype(BF16)

    def combine(index):
        arrivals(direct, direct_send, direct_recv, index)
        arrivals(merged, merged_send, merged_recv, index)
        for number in tiles(index):
            routed = weighted(number % 2, processed[number, sp], direct[number])
            store(number, routed + combined[number].astype(F32))

    lead = 3
    lag = 3
    for turn in range(pieces + chips - 2):
        if turn + lead < pieces:
            own_send(first_down + turn + lead)
        for distance in range(1, chips):
            if 0 <= turn - (distance - 1) < pieces:
                relay(first_down + turn - (distance - 1), distance)
        index = turn - (chips - 2)
        if index < 0:
            continue
        downs_from_partner(index)
        down = jnp.concatenate(
            [weights[slot, 2, starts[index] : starts[index] + widths[index], :] for slot in range(size)], axis=1
        )

        found = lax.dot_general(middle[...], down, NT, preferred_element_type=F32).astype(BF16)
        for part, number in enumerate(tiles(index)):
            for source in range(specialists):
                processed[number, source] = found[
                    source * capacity : (source + 1) * capacity, part * tile : (part + 1) * tile
                ]

        if index == pieces - 1:
            for step in range(places_count - 1, 0, -1):
                final_copy(step).start()
        else:
            for number in tiles(index):
                passing_copy(number).start()
            for number in tiles(index):
                direct_copy(number).start()
        if index:
            merge(index - 1)
        if index >= lag:
            combine(index - lag)

    for index in range(pieces - lag, pieces - 1):
        combine(index)
    remote(final, final, final_send, final_recv, partner).wait_recv()
    routed = weighted(1, processed[last_tile, sp], final[0]) + weighted(4, final[1], final[2])
    store(last_tile, routed)

    there = out_full.at[0, pl.ds(0, (chips - 1) * quarter), :]
    remote(there, there, out_z_send, out_z_recv.at[0], partner).wait_send()
    for step in range(1, chips):
        out_pieces(step).wait_send()
    out_pairs().wait_send()
    there = ret_rows.at[pl.ds(0, blocks - 1)]
    remote(there, there, mix_send, mix_recv.at[0], partner).wait_send()
    remote(outgoing, outgoing, go_send, go_recv.at[0], partner).wait_send()
    for buffer, sent, received in (
        (direct, direct_send, direct_recv), (passing, passing_send, passing_recv),
        (merged, merged_send, merged_recv),
    ):
        there = buffer.at[pl.ds(0, last_tile)]
        remote(there, there, sent, received.at[0], partner).wait_send()
    remote(final, final, final_send, final_recv, partner).wait_send()
    there = tables.at[0:2]
    remote(there, there, table_send, table_recv.at[0], partner).wait_send()
    for origin in range(chips):
        there = weights.at[origin]

        @pl.when(jnp.logical_and(origin <= z, z < chips - 1))
        def _():
            remote(there, there, right_send.at[origin], line_recv.at[0, 0], right).wait_send()

        @pl.when(jnp.logical_and(origin >= z, z > 0))
        def _():
            remote(there, there, left_send.at[origin], line_recv.at[0, 0], left).wait_send()

        remote(there, there, pair_send.at[origin], line_recv.at[0, 0], partner).wait_send()


def whole_layer(*arrays):
    (query, _, _, _, _, residual, head_gain, out_weight, norm_gain, ids, _, expert_gate) = arrays[:12]
    shared_gate = arrays[14]
    places_count, size = lax.axis_size("sp"), lax.axis_size("tp")
    rows_all, width = query.shape
    tokens, depth = residual.shape
    blocks = rows_all // tokens
    chosen = ids.shape[1]
    capacity = 3 * tokens * chosen // (2 * places_count)
    ff = expert_gate.shape[1]
    shared = shared_gate.shape[1]
    chips = size // 2
    pieces = len(piece_widths(depth))
    units = 4 + pieces
    heads = width // HEAD
    dma = pltpu.SemaphoreType.DMA
    arrays = list(arrays)
    arrays[6] = head_gain[None, :]
    arrays[8] = norm_gain[None, :]
    arrays[9], arrays[10] = arrays[9].T, arrays[10].T
    vmem, anywhere = pl.BlockSpec(memory_space=pltpu.VMEM), pl.BlockSpec(memory_space=pl.ANY)
    block = lambda *shape: pltpu.VMEM(shape, BF16)
    wide = lambda *shape: pltpu.VMEM(shape, F32)
    return pl.pallas_call(
        layer_kernel,
        in_specs=[anywhere] * len(arrays),
        out_specs=vmem,
        out_shape=pltpu.VMEM((tokens, depth), BF16),
        scratch_shapes=[
            wide(*arrays[4].shape), wide(1, width), wide(1, depth),
            pltpu.VMEM(arrays[9].shape, jnp.int32), wide(*arrays[10].shape),
            block(rows_all, width), block(rows_all, width), block(rows_all, width), block(rows_all, width),
            block(tokens, depth), block(depth, shared), block(depth, shared), block(depth, shared),
            block(size, 3, depth, ff),
            block(size, out_weight.shape[0], out_weight.shape[1]),
            wide(blocks, tokens, width),
            wide(heads * blocks, tokens),
            wide(blocks, width, width),
            wide(places_count, width + EXTRA, width),
            wide(width + EXTRA, width),
            wide(blocks, tokens, width),
            block(blocks, tokens, width),
            block(size, tokens, width),
            block(tokens, depth), block(tokens, depth),
            wide(tokens, 128),
            wide(3, 16, tokens),
            block(places_count - 1, capacity, depth),
            block(places_count, capacity, depth),
            block(places_count * capacity, size * ff),
            block(depth // 128, places_count, capacity, 128),
            block(depth // 128, capacity, 128), block(depth // 128, capacity, 128),
            block(depth // 128, tokens, 128), block(depth // 128, tokens, 128),
            block(places_count - 1, capacity, 128),
            wide(tokens, depth),
            block(tokens, shared),
            block(5, 2, tokens, 2 * capacity),
            dma((17,)),
            dma, dma((places_count,)),
            dma, dma((size,)),
            dma, dma((chips - 1,)), dma((chips,)), dma((chips,)),
            dma, dma,
            dma((chips,)), dma((chips,)), dma((chips,)), dma((chips, units)), dma((chips,)), dma((pieces,)),
            dma, dma((places_count,)),
            dma, dma((2,)),
            dma, dma((pieces,)), dma, dma((pieces,)), dma, dma((pieces,)), dma, dma,
        ],
        compiler_params=pltpu.CompilerParams(
            collective_id=0, has_side_effects=True, vmem_limit_bytes=58 * 1000 * 1000
        ),
        cost_estimate=pl.CostEstimate(
            flops=20 * 10**9, bytes_accessed=40 * 10**6, transcendentals=4 * 10**6
        ),
    )(*arrays)


def kernel_fits(mesh, shapes):
    places_count, size = mesh.shape["sp"], mesh.shape["tp"]
    if places_count != 4 or size % 2 or size < 4:
        return False
    width = shapes[0][1] // size
    tokens = shapes[5][0] // (places_count * size)
    rows_all = shapes[0][0] // places_count
    ff = shapes[11][1] // (places_count * size)
    return width == 128 and ff % 128 == 0 and tokens % 128 == 0 and rows_all == tokens * size


def solution(mesh):
    placed = (
        P("sp", "tp"),
        P("sp", "tp"),
        P("sp", "tp"),
        P("sp", "tp"),
        P("tp", "sp"),
        P(("sp", "tp"), None),
        P("tp"),
        P(None, "tp"),
        P(),
        P(("sp", "tp"), None),
        P(("sp", "tp"), None),
        P(None, ("sp", "tp")),
        P(None, ("sp", "tp")),
        P(None, ("sp", "tp")),
        P(),
        P(),
        P(),
    )

    placement = dict(mesh=mesh, in_specs=placed, out_specs=P(("sp", "tp"), None), check_vma=False)
    step = jax.shard_map(on_device, **placement)
    fused = jax.shard_map(whole_layer, **placement)

    def run(*arrays):
        fits = kernel_fits(mesh, [array.shape for array in arrays])
        return fused(*arrays) if fits else step(*arrays)

    return run
```

```python
import functools

import jax
import jax.numpy as jnp
from jax import lax
from jax.experimental import pallas as pl
from jax.experimental.pallas import tpu as pltpu
from jax.sharding import PartitionSpec as P


HEAD = 64
BLOCK = 256
EXTRA = 8


eps = 1e-05
F32 = jnp.float32
BF16 = jnp.bfloat16


def split(value):
    high = value.astype(BF16)
    return high, (value - high.astype(F32)).astype(BF16)


def per_head(columns, lanes):
    heads = columns.shape[1]
    out = jnp.broadcast_to(columns[:, 0:1], lanes.shape)
    for head in range(1, heads):
        out = jnp.where(lanes // HEAD == head, columns[:, head : head + 1], out)
    return out


def gathered_update(keys, values, column, lanes, end):
    scale = HEAD ** (-0.5)
    weighted = keys.astype(F32) * (jnp.exp(per_head(end - column, lanes)) * scale)
    high, low = split(weighted)
    dims = (((0,), (0,)), ((), ()))
    return lax.dot_general(high, values, dims, preferred_element_type=F32) + lax.dot_general(
        low, values, dims, preferred_element_type=F32
    )


def state_kernel(key_ref, value_ref, column_ref, out_ref):
    width = key_ref.shape[1]
    step = pl.program_id(0)

    @pl.when(step == 0)
    def _():
        out_ref[0:width, :] = jnp.zeros((width, width), F32)
        out_ref[width:, :] = jnp.zeros((EXTRA, width), F32)

    lanes = lax.broadcasted_iota(jnp.int32, key_ref.shape, 1)
    column = column_ref[...]
    end = column[BLOCK - 1 : BLOCK, :]
    end_lanes = per_head(end, lanes[0:1, :])
    fresh = gathered_update(key_ref[...], value_ref[...], column, lanes, end)
    out_ref[0:width, :] = out_ref[0:width, :] * jnp.exp(end_lanes) + fresh
    out_ref[width:, :] = out_ref[width:, :] + end_lanes


def retention_kernel(
    mine_ref, query_ref, key_ref, value_ref, gate_ref, column_ref, row_ref, gain_ref, states_ref,
    out_ref, state
):
    rows, width = query_ref.shape
    heads = width // HEAD
    step = pl.program_id(0)
    count = states_ref.shape[0]
    row_ids = lax.broadcasted_iota(jnp.int32, (width, width), 0) // HEAD
    column_ids = lax.broadcasted_iota(jnp.int32, (width, width), 1) // HEAD

    @pl.when(step == 0)
    def _():
        total = jnp.zeros((width, width), F32)
        for position in range(count - 1):
            decay = jnp.exp(states_ref[position, width : width + 1, :])
            longer = total * decay + states_ref[position, 0:width, :]
            total = jnp.where(position < mine_ref[0], longer, total)
        state[...] = jnp.where(row_ids == column_ids, total, 0.0)

    lanes = lax.broadcasted_iota(jnp.int32, (rows, width), 1)
    queries, keys, values = query_ref[...], key_ref[...], value_ref[...]
    column = column_ref[...]
    end = column[rows - 1 : rows, :]
    causal = lax.broadcasted_iota(jnp.int32, (rows, rows), 0) >= lax.broadcasted_iota(
        jnp.int32, (rows, rows), 1
    )
    scale = HEAD ** (-0.5)
    high, low = split(state[...])
    carried = jnp.dot(queries, high, preferred_element_type=F32) + jnp.dot(
        queries, low, preferred_element_type=F32
    )
    retained = carried * jnp.exp(per_head(column, lanes))
    inner = None
    for head in range(heads):
        own = jnp.where(lanes // HEAD == head, queries.astype(F32), 0.0).astype(BF16)
        scores = lax.dot_general(
            own, keys, (((1,), (1,)), ((), ())), preferred_element_type=F32
        )
        spread = column[:, head : head + 1] - row_ref[0, head : head + 1, :]
        damping = jnp.exp(jnp.where(causal, spread, -jnp.inf))
        factor = (scores * scale * damping).astype(BF16)
        term = jnp.dot(factor, values, preferred_element_type=F32)
        inner = term if inner is None else jnp.where(lanes // HEAD == head, term, inner)
    retained = retained + inner
    fresh = gathered_update(keys, values, column, lanes, end)
    end_lanes = per_head(end, lanes[0:1, :])
    state[...] = state[...] * jnp.exp(end_lanes) + jnp.where(row_ids == column_ids, fresh, 0.0)

    def head_mean(array):
        out = None
        for head in range(heads):
            inside = lanes // HEAD == head
            mean = jnp.sum(jnp.where(inside, array, 0.0), axis=1, keepdims=True) * (1.0 / HEAD)
            out = jnp.broadcast_to(mean, array.shape) if out is None else jnp.where(inside, mean, out)
        return out

    centered = retained - head_mean(retained)
    normed = centered * lax.rsqrt(head_mean(centered * centered) + eps)
    gates = gate_ref[...].astype(F32)
    out_ref[...] = (normed * gain_ref[...] * (gates * jax.nn.sigmoid(gates))).astype(BF16)


def retention(query_rows, key_rows, value_rows, gate_rows, log_decay, head_gain):
    rows, width = query_rows.shape
    heads = width // HEAD
    count = rows // BLOCK
    running = jnp.cumsum(log_decay.reshape(heads, count, BLOCK), axis=2)
    row = running.transpose(1, 0, 2)
    column = running.reshape(heads, rows).T
    block = pl.BlockSpec((BLOCK, width), lambda i: (i, 0))
    column_block = pl.BlockSpec((BLOCK, heads), lambda i: (i, 0))
    state_call = pl.pallas_call(
        state_kernel,
        grid=(count,),
        in_specs=[block, block, column_block],
        out_specs=pl.BlockSpec((width + EXTRA, width), lambda i: (0, 0)),
        out_shape=jax.ShapeDtypeStruct((width + EXTRA, width), F32),
        compiler_params=pltpu.CompilerParams(dimension_semantics=("arbitrary",)),
        cost_estimate=pl.CostEstimate(
            flops=4 * rows * width * width, bytes_accessed=4 * rows * width, transcendentals=rows * width
        ),
    )
    own = state_call(key_rows, value_rows, column)
    states = lax.all_gather(own, "sp")
    mine = lax.axis_index("sp").astype(jnp.int32).reshape(1)
    return pl.pallas_call(
        retention_kernel,
        grid=(count,),
        in_specs=[
            pl.BlockSpec(memory_space=pltpu.SMEM),
            block,
            block,
            block,
            block,
            column_block,
            pl.BlockSpec((1, heads, BLOCK), lambda i: (i, 0, 0)),
            pl.BlockSpec((1, width), lambda i: (0, 0)),
            pl.BlockSpec(states.shape, lambda i: (0, 0, 0)),
        ],
        out_specs=block,
        out_shape=jax.ShapeDtypeStruct((rows, width), BF16),
        scratch_shapes=[pltpu.VMEM((width, width), F32)],
        compiler_params=pltpu.CompilerParams(dimension_semantics=("arbitrary",)),
        cost_estimate=pl.CostEstimate(
            flops=8 * rows * width * BLOCK,
            bytes_accessed=10 * rows * width,
            transcendentals=rows * BLOCK * heads,
        ),
    )(mine, query_rows, key_rows, value_rows, gate_rows, column, row, head_gain[None, :], states)


def send(piece, pairs):
    return lax.ppermute(piece, "tp", pairs)


def ring_start(own):
    size = lax.axis_size("tp")
    right = [(i, (i + 2) % size) for i in range(size)]
    left = [(i, (i - 2) % size) for i in range(size)]
    swap = [(i, i ^ 1) for i in range(size)]
    return send(own, right), send(own, left), send(own, swap)


def ring_finish(own, from_left, from_right, other):
    size = lax.axis_size("tp")
    chips = size // 2
    right = [(i, (i + 2) % size) for i in range(size)]
    left = [(i, (i - 2) % size) for i in range(size)]
    swap = [(i, i ^ 1) for i in range(size)]
    half = own.shape[1] // 2
    last = chips // 2
    pieces = [[own], [other]]
    for hop in range(1, (chips - 1) // 2 + 1):
        if hop > 1:
            from_left = send(from_left, right)
            from_right = send(from_right, left)
        for piece in (from_left, from_right):
            pieces += [[piece], [send(piece, swap)]]
    if chips % 2 == 0 and last > 1:
        first = send(from_left[:, :half], right)
        second = send(from_right[:, half:], left)
        pieces += [[first, second], [send(first, swap), send(second, swap)]]
    elif chips == 2:
        pieces += [[from_left], [send(from_left, swap)]]
    return pieces


def expert_kernel(layout, row_ref, *refs):
    count = len(layout)
    piece_refs, out_ref = refs[:count], refs[count]
    weights, middle, sems = refs[count + 1 :]
    slots, _, width, ff = weights.shape
    rows = row_ref.shape[0]
    copies = []
    for index, (slot, start, length) in enumerate(layout):
        copy = pltpu.make_async_copy(
            piece_refs[index], weights.at[slot, :, pl.ds(start, length), :], sems.at[index]
        )
        copy.start()
        copies.append(copy)
    tile = rows // 2
    for pair in range(slots // 2):
        for index, (slot, _, _) in enumerate(layout):
            if slot // 2 == pair:
                copies[index].wait()

        @pl.loop(0, 2)
        def _(step):
            span = pl.ds(pl.multiple_of(step * tile, tile), tile)
            block = row_ref[span, :]
            gate = jnp.concatenate([weights[2 * pair, 0], weights[2 * pair + 1, 0]], axis=1)
            up = jnp.concatenate([weights[2 * pair, 1], weights[2 * pair + 1, 1]], axis=1)
            gated = jnp.dot(block, gate, preferred_element_type=F32)
            raised = jnp.dot(block, up, preferred_element_type=F32)
            value = gated * jax.nn.sigmoid(gated) * raised
            middle[span, 2 * pair * ff : 2 * (pair + 1) * ff] = value.astype(BF16)

    part = 512

    @pl.loop(0, width // part)
    def _(step):
        span = pl.ds(pl.multiple_of(step * part, part), part)
        down = jnp.concatenate([weights[slot, 2, span, :] for slot in range(slots)], axis=1)
        out_ref[:, span] = lax.dot_general(
            middle[...], down, (((1,), (1,)), ((), ())), preferred_element_type=F32
        ).astype(BF16)


def experts(rows, shards):
    _, width, ff = shards[0][0].shape
    count = len(shards)
    if ff % 128 or count % 2:
        whole = jnp.concatenate([jnp.concatenate(shard, axis=1) for shard in shards], axis=2)
        middle = (
            jax.nn.silu(jnp.dot(rows, whole[0], preferred_element_type=F32))
            * jnp.dot(rows, whole[1], preferred_element_type=F32)
        ).astype(BF16)
        return lax.dot_general(
            middle, whole[2], (((1,), (1,)), ((), ())), preferred_element_type=F32
        ).astype(BF16)
    layout, pieces = [], []
    for slot, shard in enumerate(shards):
        start = 0
        for piece in shard:
            layout.append((slot, start, piece.shape[1]))
            pieces.append(piece)
            start += piece.shape[1]
    return pl.pallas_call(
        functools.partial(expert_kernel, layout),
        in_specs=[pl.BlockSpec(memory_space=pltpu.VMEM)]
        + [pl.BlockSpec(memory_space=pl.ANY)] * len(pieces),
        out_specs=pl.BlockSpec(memory_space=pltpu.VMEM),
        out_shape=jax.ShapeDtypeStruct(rows.shape, BF16),
        scratch_shapes=[
            pltpu.VMEM((count, 3, width, ff), BF16),
            pltpu.VMEM((rows.shape[0], count * ff), BF16),
            pltpu.SemaphoreType.DMA((len(pieces),)),
        ],
        compiler_params=pltpu.CompilerParams(vmem_limit_bytes=60 * 1024 * 1024),
        cost_estimate=pl.CostEstimate(
            flops=6 * rows.shape[0] * width * count * ff,
            bytes_accessed=6 * width * count * ff + 4 * rows.size,
            transcendentals=rows.shape[0] * count * ff,
        ),
    )(rows, *pieces)


def on_device(
    query_rows,
    key_rows,
    value_rows,
    gate_rows,
    log_decay,
    residual,
    head_gain,
    out_weight,
    norm_gain,
    expert_ids,
    route_weights,
    expert_gate,
    expert_up,
    expert_down,
    shared_gate,
    shared_up,
    shared_down,
):
    part = out_weight.shape[0] // lax.axis_size("sp")
    own_part = lax.dynamic_slice_in_dim(out_weight, lax.axis_index("sp") * part, part, 0)
    out_part = lax.all_gather(own_part, "tp", axis=1, tiled=True)
    out_full = lax.all_gather(out_part, "sp", axis=0, tiled=True)
    shard = jnp.stack([expert_gate, expert_up, expert_down])
    shard, log_decay = lax.optimization_barrier((shard, log_decay))
    from_left, from_right, other = ring_start(shard)

    specialists = lax.axis_size("sp")
    tokens, chosen = expert_ids.shape
    width = residual.shape[1]
    capacity = 3 * tokens * chosen // (2 * specialists)
    names = jnp.arange(specialists, dtype=jnp.int32)[:, None]
    named = [expert_ids[:, j][None, :] == names for j in range(chosen)]
    match = functools.reduce(jnp.logical_or, named)
    weight = sum(jnp.where(named[j], route_weights[:, j][None, :], 0.0) for j in range(chosen))
    earlier = jnp.arange(tokens)[:, None] < jnp.arange(tokens)[None, :]
    position = jnp.dot(match.astype(BF16), earlier.astype(BF16), preferred_element_type=F32)
    place = jnp.where(match, position.astype(jnp.int32), -1)
    sits = place[:, None, :] == jnp.arange(capacity, dtype=jnp.int32)[None, :, None]
    pick = sits.astype(BF16).reshape(specialists * capacity, tokens)
    weight_high = lax.reduce_precision(weight, 8, 7)
    weight_low = weight - weight_high
    back_high = jnp.where(sits, weight_high[:, None, :], 0.0).astype(BF16)
    back_low = jnp.where(sits, weight_low[:, None, :], 0.0).astype(BF16)

    ret_rows = retention(query_rows, key_rows, value_rows, gate_rows, log_decay, head_gain)
    token_rows = lax.all_to_all(ret_rows, "tp", split_axis=0, concat_axis=1, tiled=True)
    token_rows, from_left, from_right = lax.optimization_barrier((token_rows, from_left, from_right))
    shards = ring_finish(shard, from_left, from_right, other)
    mixer = jnp.dot(token_rows, out_full, preferred_element_type=F32)
    hidden = (residual.astype(F32) + mixer).astype(BF16)
    hidden_wide = hidden.astype(F32)
    normed_rows = (
        hidden_wide
        * lax.rsqrt(jnp.mean(hidden_wide * hidden_wide, axis=1, keepdims=True) + eps)
        * norm_gain
    ).astype(BF16)
    outgoing = jnp.dot(pick, normed_rows, preferred_element_type=F32).astype(BF16)
    outgoing = outgoing.reshape(specialists, capacity, width)
    arrived = lax.all_to_all(outgoing, "sp", split_axis=0, concat_axis=0, tiled=True)
    shared_mid = (
        jax.nn.silu(jnp.dot(normed_rows, shared_gate, preferred_element_type=F32))
        * jnp.dot(normed_rows, shared_up, preferred_element_type=F32)
    ).astype(BF16)
    shared_out = lax.dot_general(
        shared_mid, shared_down, (((1,), (1,)), ((), ())), preferred_element_type=F32
    )
    flat_rows = arrived.reshape(-1, width)
    processed = experts(flat_rows, shards).reshape(arrived.shape)
    returned = lax.all_to_all(processed, "sp", split_axis=0, concat_axis=0, tiled=True)
    dims = (((0, 1), (0, 1)), ((), ()))
    routed = lax.dot_general(back_high, returned, dims, preferred_element_type=F32)
    routed += lax.dot_general(back_low, returned, dims, preferred_element_type=F32)
    return (hidden_wide + routed + shared_out).astype(BF16)


MESH = pl.DeviceIdType.MESH
NT = (((1,), (1,)), ((), ()))
TN = (((0,), (0,)), ((), ()))


def thirds(value):
    first = value.astype(BF16)
    rest = value - first.astype(F32)
    second = rest.astype(BF16)
    return first, second, (rest - second.astype(F32)).astype(BF16)


def piece_widths(depth):
    return [128] + [256] * ((depth - 256) // 256) + [128]


def layer_kernel(
    query_hbm, key_hbm, value_hbm, gate_hbm, decay_hbm, residual_hbm, head_gain_hbm, out_weight_hbm,
    norm_gain_hbm, ids_hbm, route_hbm, expert_gate_hbm, expert_up_hbm, expert_down_hbm,
    shared_gate_hbm, shared_up_hbm, shared_down_hbm,
    result_ref,
    decay_ref, head_gain_ref, norm_gain_ref, ids_ref, route_ref,
    query, key, value, gates, residual, shared_gate, shared_up, shared_down,
    weights, out_full, running, row_running, updates, states, state, inner, ret_rows, token_rows,
    hidden, normed, squares, tables, outgoing, arrived, middle, processed, direct, passing, merged,
    combined, final, base, shared_middle, back, shares,
    local_sem, state_send, state_recv, mix_send, mix_recv, out_z_send, out_xy_send, out_z_recv, out_xy_recv,
    out_pair_send, out_pair_recv, right_send, left_send, pair_send, line_recv, pair_recv, pair_down_recv,
    go_send, go_recv, table_send, table_recv, direct_send, direct_recv, passing_send, passing_recv,
    merged_send, merged_recv, final_send, final_recv,
):
    places_count = states.shape[0]
    size = token_rows.shape[0]
    chips = size // 2
    sp = lax.axis_index("sp")
    tp = lax.axis_index("tp")
    z, core = tp // 2, tp % 2
    blocks, rows, width = ret_rows.shape
    heads = width // HEAD
    depth = residual.shape[1]
    capacity = arrived.shape[1]
    specialists = arrived.shape[0]
    ff = weights.shape[3]
    quarter = out_full.shape[1] // places_count
    out_columns = out_full.shape[2]
    widths = piece_widths(depth)
    pieces = len(widths)
    starts = [sum(widths[:index]) for index in range(pieces)]
    half = depth // 2
    tile = processed.shape[3]
    scale = HEAD ** (-0.5)
    inputs = (expert_gate_hbm, expert_up_hbm, expert_down_hbm)
    units = [(which, start, half) for which in (0, 1) for start in (0, half)]
    first_down = len(units)
    units += [(2, start, length) for start, length in zip(starts, widths)]

    def remote(src, dst, send, recv, device):
        return pltpu.make_async_remote_copy(
            src_ref=src, dst_ref=dst, send_sem=send, recv_sem=recv, device_id=device, device_id_type=MESH
        )

    partner = (sp, z * 2 + 1 - core)
    right = (sp, tp + 2)
    left = (sp, tp - 2)

    local = [
        pltpu.make_async_copy(src, dst, local_sem.at[index])
        for index, (src, dst) in enumerate(
            [
                (decay_hbm, decay_ref),
                (ids_hbm, ids_ref),
                (route_hbm, route_ref),
                (key_hbm, key),
                (value_hbm, value),
                (query_hbm, query),
                (gate_hbm, gates),
                (head_gain_hbm, head_gain_ref),
                (norm_gain_hbm, norm_gain_ref),
                (out_weight_hbm, out_full.at[tp]),
                (residual_hbm, residual),
                (shared_gate_hbm, shared_gate),
                (shared_up_hbm, shared_up),
                (shared_down_hbm, shared_down),
                (expert_gate_hbm, weights.at[tp, 0]),
                (expert_up_hbm, weights.at[tp, 1]),
                (expert_down_hbm, weights.at[tp, 2]),
            ]
        )
    ]
    barrier = pltpu.get_barrier_semaphore()
    for step in range(1, size):
        pl.semaphore_signal(barrier, inc=1, device_id=(sp, (tp + step) % size), device_id_type=MESH)
    for step in range(1, places_count):
        pl.semaphore_signal(barrier, inc=1, device_id=(sp ^ step, tp), device_id_type=MESH)
    for copy in local[:9]:
        copy.start()
    pl.semaphore_wait(barrier, size - 1 + places_count - 1)

    def weight_copy(origin, unit, send, device, own=False, pair=False):
        which, start, length = units[unit]
        span = pl.ds(start, length)
        there = weights.at[origin * 2 + core, which, span, :]
        here = inputs[which].at[span, :] if own else there
        if not pair:
            received = line_recv.at[origin, unit]
        elif unit < first_down:
            received = pair_recv.at[origin]
        else:
            received = pair_down_recv.at[unit - first_down]
        return remote(here, there, send, received, device)

    def to_partner(origin, unit, own=False):
        return weight_copy(origin, unit, pair_send.at[origin], partner, own, True)

    def own_send(unit):
        @pl.when(z < chips - 1)
        def _():
            weight_copy(z, unit, right_send.at[z], right, True).start()

        @pl.when(z > 0)
        def _():
            weight_copy(z, unit, left_send.at[z], left, True).start()

        to_partner(z, unit, True).start()

    def relay(unit, distance):
        @pl.when(z - distance >= 0)
        def _():
            origin = z - distance
            copy = weight_copy(origin, unit, right_send.at[origin], right)
            copy.wait_recv()

            @pl.when(z < chips - 1)
            def _():
                copy.start()

            to_partner(origin, unit).start()

        @pl.when(z + distance < chips)
        def _():
            origin = z + distance
            copy = weight_copy(origin, unit, left_send.at[origin], left)
            copy.wait_recv()

            @pl.when(z > 0)
            def _():
                copy.start()

            to_partner(origin, unit).start()

    def from_partner(origin):
        there = weights.at[0, 0:2]
        remote(there, there, pair_send.at[origin], pair_recv.at[origin], partner).wait_recv()

    def downs_from_partner(index):
        there = weights.at[0, 2, pl.ds(0, chips * widths[index]), :]
        remote(there, there, pair_send.at[0], pair_down_recv.at[index], partner).wait_recv()

    def out_z(step):
        target = (z + step) % chips
        span = pl.ds(pl.multiple_of(sp * quarter, quarter), quarter)
        return remote(
            out_weight_hbm.at[span, :], out_full.at[tp, span, :], out_z_send, out_z_recv.at[z],
            (sp, target * 2 + core),
        )

    def out_z_arrival(step):
        origin = (z + step) % chips
        there = out_full.at[0, pl.ds(0, quarter), :]
        return remote(there, there, out_z_send, out_z_recv.at[origin], partner)

    def out_piece(step, device):
        origin = (z + step) % chips
        span = pl.ds(pl.multiple_of(sp * quarter, quarter), quarter)
        there = out_full.at[origin * 2 + core, span, :]
        return remote(there, there, out_xy_send.at[step - 1], out_xy_recv.at[origin], device)

    def out_pieces(step):
        origin = (z + step) % chips
        there = out_full.at[0, pl.ds(0, (places_count - 1) * quarter), :]
        return remote(there, there, out_xy_send.at[step - 1], out_xy_recv.at[origin], partner)

    def out_pair(slot, own=False):
        return remote(
            out_weight_hbm if own else out_full.at[slot], out_full.at[slot], out_pair_send,
            out_pair_recv, partner,
        )

    def out_pairs():
        there = out_full.at[0:chips]
        return remote(there, there, out_pair_send, out_pair_recv, partner)

    for step in range(1, chips):
        out_z(step).start()
    own_send(0)
    own_send(1)
    out_pair(tp, True).start()
    for copy in local[9:]:
        copy.start()

    for copy in local[:3]:
        copy.wait()

    row_ids = lax.broadcasted_iota(jnp.int32, (width, width), 0) // HEAD
    column_ids = lax.broadcasted_iota(jnp.int32, (width, width), 1) // HEAD
    same_head = row_ids == column_ids
    lanes = lax.broadcasted_iota(jnp.int32, (rows, width), 1)
    later = lax.broadcasted_iota(jnp.int32, (rows, rows), 0)
    sooner = lax.broadcasted_iota(jnp.int32, (rows, rows), 1)
    lower = jnp.where(later >= sooner, 1.0, 0.0).astype(BF16)
    upper = jnp.where(later <= sooner, 1.0, 0.0).astype(BF16)

    chosen, tokens = ids_ref.shape
    names = lax.broadcasted_iota(jnp.int32, (8, tokens), 0)
    match = names < 0
    weight = jnp.zeros((8, tokens), F32)
    for j in range(chosen):
        named = ids_ref[j : j + 1, :] == names
        match = jnp.logical_or(match, named)
        weight = weight + jnp.where(named, route_ref[j : j + 1, :], 0.0)
    strict = jnp.where(later < sooner, 1.0, 0.0).astype(BF16)
    position = jnp.dot(jnp.where(match, 1.0, 0.0).astype(BF16), strict, preferred_element_type=F32)
    tables[0, 0:8, :] = jnp.where(match, position, -1.0)
    tables[0, 8:16, :] = weight

    def table_copy(step):
        return remote(
            tables.at[0], tables.at[step], table_send, table_recv.at[step - 1], (sp ^ step, tp)
        )

    listed = jnp.concatenate(
        [
            decay_ref[head : head + 1, block * rows : (block + 1) * rows]
            for head in range(heads)
            for block in range(blocks)
        ],
        axis=0,
    )
    row_running[...] = functools.reduce(
        jnp.add, [jnp.dot(part, upper, preferred_element_type=F32) for part in thirds(listed)]
    )
    head_rows = lax.broadcasted_iota(jnp.int32, (width, rows), 0) // HEAD
    for block in range(blocks):
        spread = jnp.broadcast_to(listed[block : block + 1, :], (width, rows))
        for head in range(1, heads):
            spread = jnp.where(
                head_rows == head, listed[head * blocks + block : head * blocks + block + 1, :], spread
            )
        running[block] = functools.reduce(
            jnp.add,
            [
                lax.dot_general(lower, part, NT, preferred_element_type=F32)
                for part in thirds(spread)
            ],
        )

    for copy in local[3:5]:
        copy.wait()
    state[...] = jnp.zeros((width + EXTRA, width), F32)

    @pl.loop(0, blocks)
    def _(block):
        span = pl.ds(pl.multiple_of(block * rows, rows), rows)
        column = running[block]
        end = column[rows - 1 : rows, :]
        weighted = key[span, :].astype(F32) * (jnp.exp(end - column) * scale)
        high, low = split(weighted)
        fresh = lax.dot_general(high, value[span, :], TN, preferred_element_type=F32)
        fresh += lax.dot_general(low, value[span, :], TN, preferred_element_type=F32)
        fresh = jnp.where(same_head, fresh, 0.0)
        updates[block] = fresh
        state[0:width, :] = state[0:width, :] * jnp.exp(end) + fresh
        state[width:, :] = state[width:, :] + end

    states[sp] = state[...]

    def state_copy(step):
        return remote(
            state, states.at[sp], state_send, state_recv.at[sp], (sp ^ step, tp)
        )

    def state_arrival(step):
        return remote(
            state, states.at[sp ^ step], state_send, state_recv.at[sp ^ step], (sp ^ step, tp)
        )

    local[5].wait()
    for step in range(1, places_count):
        state_copy(step).start()
    for step in (1, 2):
        table_copy(step).start()

    @pl.loop(0, blocks)
    def _(block):
        span = pl.ds(pl.multiple_of(block * rows, rows), rows)
        queries, keys, values = query[span, :], key[span, :], value[span, :]
        column = running[block]
        causal = later >= sooner
        total = None
        for head in range(heads):
            own = jnp.where(lanes // HEAD == head, queries.astype(F32), 0.0).astype(BF16)
            scores = lax.dot_general(own, keys, NT, preferred_element_type=F32)
            spread = column[:, head * HEAD : head * HEAD + 1] - row_running[pl.ds(head * blocks + block, 1), :]
            damping = jnp.exp(jnp.where(causal, spread, -jnp.inf))
            factor = (scores * scale * damping).astype(BF16)
            term = jnp.dot(factor, values, preferred_element_type=F32)
            total = term if total is None else jnp.where(lanes // HEAD == head, term, total)
        inner[block] = total

    for step in range(1, chips):
        out_z_arrival(step).wait_recv()
        for other in range(1, places_count):
            out_piece(step, (sp ^ other, tp)).start()

    for step in range(1, places_count):
        state_arrival(step).wait_recv()
    there = states.at[pl.ds(0, places_count - 1)]
    remote(there, there, state_send, state_recv.at[0], partner).wait_send()
    total = jnp.zeros((width, width), F32)
    for position in range(places_count - 1):
        longer = total * jnp.exp(states[position, width : width + 1, :]) + states[position, 0:width, :]
        total = jnp.where(position < sp, longer, total)
    state[0:width, :] = total
    local[6].wait()
    local[7].wait()

    def head_mean(array):
        out = None
        for head in range(heads):
            inside = lanes // HEAD == head
            mean = jnp.sum(jnp.where(inside, array, 0.0), axis=1, keepdims=True) * (1.0 / HEAD)
            out = jnp.broadcast_to(mean, array.shape) if out is None else jnp.where(inside, mean, out)
        return out

    def mix_copy(block):
        return remote(
            ret_rows.at[block], token_rows.at[tp], mix_send, mix_recv.at[tp], (sp, block)
        )

    def mix_start(block):
        @pl.when(block != tp)
        def _():
            mix_copy(block).start()

    @pl.loop(0, blocks)
    def _(block):
        span = pl.ds(pl.multiple_of(block * rows, rows), rows)
        column = running[block]
        end = column[rows - 1 : rows, :]
        before = state[0:width, :]
        high, low = split(before)
        queries = query[span, :]
        carried = jnp.dot(queries, high, preferred_element_type=F32) + jnp.dot(
            queries, low, preferred_element_type=F32
        )
        state[0:width, :] = before * jnp.exp(end) + updates[block]
        retained = carried * jnp.exp(column) + inner[block]
        centered = retained - head_mean(retained)
        norm = centered * lax.rsqrt(head_mean(centered * centered) + eps)
        gate = gates[span, :].astype(F32)
        mixed = (norm * head_gain_ref[...] * (gate * jax.nn.sigmoid(gate))).astype(BF16)
        ret_rows[block] = mixed

        @pl.when(block == tp)
        def _():
            token_rows[tp] = mixed

        @pl.when(block > 0)
        def _():
            mix_start(block - 1)

    mix_start(blocks - 1)

    relay(0, 1)
    own_send(2)
    relay(1, 1)
    own_send(3)

    between = jnp.logical_and(z > 0, z < chips - 1)

    @pl.when(jnp.logical_not(between))
    def _():
        for unit in range(first_down, len(units)):
            own_send(unit)

    def pass_on(unit, distance, rightward):
        origin = z - distance if rightward else z + distance
        sent, device = (right_send, right) if rightward else (left_send, left)
        copy = weight_copy(origin, unit, sent.at[origin], device)
        copy.wait_recv()
        copy.start()
        to_partner(origin, unit).start()

    def inward(unit):
        for chip, rightward in ((1, True), (chips - 2, False)):

            @pl.when(z == chip)
            def _():
                sent, device = (right_send, right) if rightward else (left_send, left)
                weight_copy(z, unit, sent.at[z], device, True).start()
                to_partner(z, unit, True).start()
                pass_on(unit, 1, rightward)

    def outward(unit):
        for chip, rightward in ((1, False), (chips - 2, True)):

            @pl.when(z == chip)
            def _():
                sent, device = (right_send, right) if rightward else (left_send, left)
                weight_copy(z, unit, sent.at[z], device, True).start()
                for distance in (1, 2):
                    pass_on(unit, distance, rightward)


    slot_rows = lax.broadcasted_iota(jnp.int32, (capacity, tokens), 0).astype(F32)
    for step in (1, 2):
        table_copy(step).wait_recv()
    for turn, (table, pair) in enumerate(
        ((0, (0, 2)), (0, (0, 1)), (1, (0, 2)), (2, (0, 1)), (0, (2, 3)))
    ):
        for side, other in enumerate(pair):
            name = sp ^ other
            place = tables[table, pl.ds(name, 1), :]
            back[turn, side] = jnp.where(place == slot_rows, 1.0, 0.0).T.astype(BF16)
            share = tables[table, pl.ds(8 + name, 1), :]
            shares[turn, side] = jnp.broadcast_to(share, (tile, tokens)).T

    for copy in local[8:11]:
        copy.wait()
    for step in range(1, chips):
        out_pieces(step).wait_recv()
        out_pair(((z + step) % chips) * 2 + core).start()
    out_pairs().wait_recv()
    for step in range(1, size):
        source = (tp + step) % size
        remote(
            ret_rows.at[0], token_rows.at[source], mix_send, mix_recv.at[source], (sp, source)
        ).wait_recv()

    squares[...] = jnp.zeros(squares.shape, F32)

    @pl.loop(0, size)
    def _(slot):
        span = pl.ds(pl.multiple_of(slot * out_columns, out_columns), out_columns)
        token = jnp.concatenate([token_rows[index] for index in range(size)], axis=1)
        mixer = jnp.dot(token, out_full[slot], preferred_element_type=F32)
        total = (residual[:, span].astype(F32) + mixer).astype(BF16)
        hidden[:, span] = total
        wide = total.astype(F32)
        wide = wide * wide
        squares[...] += functools.reduce(
            jnp.add, [wide[:, start : start + 128] for start in range(0, out_columns, 128)]
        )

    factor = lax.rsqrt(jnp.sum(squares[...], axis=1, keepdims=True) * (1.0 / depth) + eps)

    @pl.loop(0, depth // 256)
    def _(index):
        span = pl.ds(pl.multiple_of(index * 256, 256), 256)
        normed[:, span] = (hidden[:, span].astype(F32) * factor * norm_gain_ref[:, span]).astype(BF16)

    relay(0, 2)

    def go(step):
        return remote(
            outgoing.at[step - 1], arrived.at[sp], go_send, go_recv.at[sp], (sp ^ step, tp)
        )

    for step in list(range(places_count - 1, -1, -1)):
        sits = jnp.where(tables[0, pl.ds(sp ^ step, 1), :] == slot_rows, 1.0, 0.0).astype(BF16)

        @pl.loop(0, depth // 512)
        def _(index):
            span = pl.ds(pl.multiple_of(index * 512, 512), 512)
            picked = jnp.dot(sits, normed[:, span], preferred_element_type=F32).astype(BF16)
            if step:
                outgoing[step - 1, :, span] = picked
            else:
                arrived[sp, :, span] = picked

        if step:
            go(step).start()

    relay(1, 2)
    relay(2, 1)

    for copy in local[11:14]:
        copy.wait()
    shared = shared_gate.shape[1]

    @pl.loop(0, shared // 256)
    def _(index):
        span = pl.ds(pl.multiple_of(index * 256, 256), 256)
        gated = jnp.dot(normed[...], shared_gate[:, span], preferred_element_type=F32)
        raised = jnp.dot(normed[...], shared_up[:, span], preferred_element_type=F32)
        shared_middle[:, span] = (gated * jax.nn.sigmoid(gated) * raised).astype(BF16)

    @pl.loop(0, depth // 512)
    def _(index):
        span = pl.ds(pl.multiple_of(index * 512, 512), 512)
        base[:, span] = hidden[:, span].astype(F32) + lax.dot_general(
            shared_middle[...], shared_down[span, :], NT, preferred_element_type=F32
        )

    relay(0, 3)
    relay(3, 1)
    relay(2, 2)
    relay(1, 3)
    relay(3, 2)
    inward(first_down)
    inward(first_down + 1)

    for copy in local[14:]:
        copy.wait()
    for step in range(1, places_count):
        remote(
            outgoing.at[0], arrived.at[sp ^ step], go_send, go_recv.at[sp ^ step], (sp ^ step, tp)
        ).wait_recv()

    outward(first_down)
    inward(first_down + 2)

    def pair_middle(chip):
        @pl.loop(0, specialists // 2)
        def _(index):
            rows_here = jnp.concatenate([arrived[2 * index], arrived[2 * index + 1]], axis=0)
            gate_pair = jnp.concatenate([weights[2 * chip, 0], weights[2 * chip + 1, 0]], axis=1)
            up_pair = jnp.concatenate([weights[2 * chip, 1], weights[2 * chip + 1, 1]], axis=1)
            gated = jnp.dot(rows_here, gate_pair, preferred_element_type=F32)
            raised = jnp.dot(rows_here, up_pair, preferred_element_type=F32)
            found = (gated * jax.nn.sigmoid(gated) * raised).astype(BF16)
            span = pl.ds(pl.multiple_of(index * 2 * capacity, 2 * capacity), 2 * capacity)
            middle[span, pl.ds(pl.multiple_of(chip * 2 * ff, 2 * ff), 2 * ff)] = found

    last_chip = jnp.where(z * 2 < chips, chips - 1, 0)

    def chip_at(index):
        if index == 0:
            return z
        if index == chips - 1:
            return last_chip
        toward = jnp.where(last_chip == 0, chips - 1 - index, index)
        shifted = jnp.where(last_chip == 0, chips - index, index - 1)
        passed = jnp.where(last_chip == 0, z <= chips - 1 - index, z >= index)
        return jnp.where(passed, shifted, toward)

    for index in range(chips):
        chip = chip_at(index)
        if index == chips - 1:
            relay(2, 3)
            relay(3, 3)
        from_partner(chip)
        pair_middle(chip)

    def tiles(index):
        return range(starts[index] // tile, (starts[index] + widths[index]) // tile)

    def piece_of(number):
        return next(index for index in range(pieces) if number in tiles(index))

    def arrivals(buffer, send, received, index):
        there = buffer.at[pl.ds(starts[index] // tile, widths[index] // tile)]
        remote(there, there, send, received.at[index], partner).wait_recv()

    def near(number):
        return sp ^ (2, 1)[number % 2]

    def far(number):
        return sp ^ (1, 2)[number % 2]

    def direct_copy(number):
        return remote(
            processed.at[number, near(number)], direct.at[number], direct_send,
            direct_recv.at[piece_of(number)], (near(number), tp),
        )

    def passing_copy(number):
        return remote(
            processed.at[number, sp ^ 3], passing.at[number], passing_send,
            passing_recv.at[piece_of(number)], (near(number), tp),
        )

    def merged_copy(number):
        return remote(
            merged.at[number], combined.at[number], merged_send,
            merged_recv.at[piece_of(number)], (far(number), tp),
        )

    def weighted(turn, first, second):
        first = jnp.dot(back[turn, 0], first, preferred_element_type=F32) * shares[turn, 0]
        return first + jnp.dot(back[turn, 1], second, preferred_element_type=F32) * shares[turn, 1]

    def merge(index):
        arrivals(passing, passing_send, passing_recv, index)
        for number in tiles(index):
            found = weighted(2 + number % 2, processed[number, far(number)], passing[number])
            merged[number] = found.astype(BF16)
        for number in tiles(index):
            merged_copy(number).start()

    last_tile = depth // tile - 1

    def final_copy(step):
        return remote(
            processed.at[last_tile, sp ^ step], final.at[step - 1], final_send, final_recv, (sp ^ step, tp)
        )

    def store(number, routed):
        span = slice(number * tile, (number + 1) * tile)
        result_ref[:, span] = (base[:, span] + routed).astype(BF16)

    def combine(index):
        arrivals(direct, direct_send, direct_recv, index)
        arrivals(merged, merged_send, merged_recv, index)
        for number in tiles(index):
            routed = weighted(number % 2, processed[number, sp], direct[number])
            store(number, routed + combined[number].astype(F32))

    lag = 3

    outward(first_down + 1)
    inward(first_down + 3)
    for index in range(pieces):
        unit = first_down + index

        if index + 2 < pieces:
            outward(unit + 2)
        if index + 4 < pieces:
            inward(unit + 4)

        @pl.when(jnp.logical_not(between))
        def _():
            for distance in range(1, chips):
                relay(unit, distance)

        downs_from_partner(index)
        down = jnp.concatenate(
            [weights[slot, 2, starts[index] : starts[index] + widths[index], :] for slot in range(size)], axis=1
        )

        found = lax.dot_general(middle[...], down, NT, preferred_element_type=F32).astype(BF16)
        for part, number in enumerate(tiles(index)):
            for source in range(specialists):
                processed[number, source] = found[
                    source * capacity : (source + 1) * capacity, part * tile : (part + 1) * tile
                ]

        if index == pieces - 1:
            for step in range(places_count - 1, 0, -1):
                final_copy(step).start()
        else:
            for number in tiles(index):
                passing_copy(number).start()
            for number in tiles(index):
                direct_copy(number).start()
        if index:
            merge(index - 1)
        if index >= lag:
            combine(index - lag)

    for index in range(pieces - lag, pieces - 1):
        combine(index)
    remote(final, final, final_send, final_recv, partner).wait_recv()
    routed = weighted(1, processed[last_tile, sp], final[0]) + weighted(4, final[1], final[2])
    store(last_tile, routed)

    there = out_full.at[0, pl.ds(0, (chips - 1) * quarter), :]
    remote(there, there, out_z_send, out_z_recv.at[0], partner).wait_send()
    for step in range(1, chips):
        out_pieces(step).wait_send()
    out_pairs().wait_send()
    there = ret_rows.at[pl.ds(0, blocks - 1)]
    remote(there, there, mix_send, mix_recv.at[0], partner).wait_send()
    remote(outgoing, outgoing, go_send, go_recv.at[0], partner).wait_send()
    for buffer, sent, received in (
        (direct, direct_send, direct_recv), (passing, passing_send, passing_recv),
        (merged, merged_send, merged_recv),
    ):
        there = buffer.at[pl.ds(0, last_tile)]
        remote(there, there, sent, received.at[0], partner).wait_send()
    remote(final, final, final_send, final_recv, partner).wait_send()
    there = tables.at[0:2]
    remote(there, there, table_send, table_recv.at[0], partner).wait_send()
    for origin in range(chips):
        there = weights.at[origin]

        @pl.when(jnp.logical_and(origin <= z, z < chips - 1))
        def _():
            remote(there, there, right_send.at[origin], line_recv.at[0, 0], right).wait_send()

        @pl.when(jnp.logical_and(origin >= z, z > 0))
        def _():
            remote(there, there, left_send.at[origin], line_recv.at[0, 0], left).wait_send()

        remote(there, there, pair_send.at[origin], line_recv.at[0, 0], partner).wait_send()


def whole_layer(*arrays):
    (query, _, _, _, _, residual, head_gain, out_weight, norm_gain, ids, _, expert_gate) = arrays[:12]
    shared_gate = arrays[14]
    places_count, size = lax.axis_size("sp"), lax.axis_size("tp")
    rows_all, width = query.shape
    tokens, depth = residual.shape
    blocks = rows_all // tokens
    chosen = ids.shape[1]
    capacity = 3 * tokens * chosen // (2 * places_count)
    ff = expert_gate.shape[1]
    shared = shared_gate.shape[1]
    chips = size // 2
    pieces = len(piece_widths(depth))
    units = 4 + pieces
    heads = width // HEAD
    dma = pltpu.SemaphoreType.DMA
    arrays = list(arrays)
    arrays[6] = head_gain[None, :]
    arrays[8] = norm_gain[None, :]
    arrays[9], arrays[10] = arrays[9].T, arrays[10].T
    vmem, anywhere = pl.BlockSpec(memory_space=pltpu.VMEM), pl.BlockSpec(memory_space=pl.ANY)
    block = lambda *shape: pltpu.VMEM(shape, BF16)
    wide = lambda *shape: pltpu.VMEM(shape, F32)
    return pl.pallas_call(
        layer_kernel,
        in_specs=[anywhere] * len(arrays),
        out_specs=vmem,
        out_shape=pltpu.VMEM((tokens, depth), BF16),
        scratch_shapes=[
            wide(*arrays[4].shape), wide(1, width), wide(1, depth),
            pltpu.VMEM(arrays[9].shape, jnp.int32), wide(*arrays[10].shape),
            block(rows_all, width), block(rows_all, width), block(rows_all, width), block(rows_all, width),
            block(tokens, depth), block(depth, shared), block(depth, shared), block(depth, shared),
            block(size, 3, depth, ff),
            block(size, out_weight.shape[0], out_weight.shape[1]),
            wide(blocks, tokens, width),
            wide(heads * blocks, tokens),
            wide(blocks, width, width),
            wide(places_count, width + EXTRA, width),
            wide(width + EXTRA, width),
            wide(blocks, tokens, width),
            block(blocks, tokens, width),
            block(size, tokens, width),
            block(tokens, depth), block(tokens, depth),
            wide(tokens, 128),
            wide(3, 16, tokens),
            block(places_count - 1, capacity, depth),
            block(places_count, capacity, depth),
            block(places_count * capacity, size * ff),
            block(depth // 128, places_count, capacity, 128),
            block(depth // 128, capacity, 128), block(depth // 128, capacity, 128),
            block(depth // 128, tokens, 128), block(depth // 128, tokens, 128),
            block(places_count - 1, capacity, 128),
            wide(tokens, depth),
            block(tokens, shared),
            block(5, 2, tokens, capacity), wide(5, 2, tokens, 128),
            dma((17,)),
            dma, dma((places_count,)),
            dma, dma((size,)),
            dma, dma((chips - 1,)), dma((chips,)), dma((chips,)),
            dma, dma,
            dma((chips,)), dma((chips,)), dma((chips,)), dma((chips, units)), dma((chips,)), dma((pieces,)),
            dma, dma((places_count,)),
            dma, dma((2,)),
            dma, dma((pieces,)), dma, dma((pieces,)), dma, dma((pieces,)), dma, dma,
        ],
        compiler_params=pltpu.CompilerParams(
            collective_id=0, has_side_effects=True, vmem_limit_bytes=58 * 1000 * 1000
        ),
        cost_estimate=pl.CostEstimate(
            flops=20 * 10**9, bytes_accessed=40 * 10**6, transcendentals=4 * 10**6
        ),
    )(*arrays)


def kernel_fits(mesh, shapes):
    places_count, size = mesh.shape["sp"], mesh.shape["tp"]
    if places_count != 4 or size != 8:
        return False
    width = shapes[0][1] // size
    tokens = shapes[5][0] // (places_count * size)
    rows_all = shapes[0][0] // places_count
    ff = shapes[11][1] // (places_count * size)
    return width == 128 and ff % 128 == 0 and tokens % 128 == 0 and rows_all == tokens * size


def solution(mesh):
    placed = (
        P("sp", "tp"),
        P("sp", "tp"),
        P("sp", "tp"),
        P("sp", "tp"),
        P("tp", "sp"),
        P(("sp", "tp"), None),
        P("tp"),
        P(None, "tp"),
        P(),
        P(("sp", "tp"), None),
        P(("sp", "tp"), None),
        P(None, ("sp", "tp")),
        P(None, ("sp", "tp")),
        P(None, ("sp", "tp")),
        P(),
        P(),
        P(),
    )

    placement = dict(mesh=mesh, in_specs=placed, out_specs=P(("sp", "tp"), None), check_vma=False)
    step = jax.shard_map(on_device, **placement)
    fused = jax.shard_map(whole_layer, **placement)

    def run(*arrays):
        fits = kernel_fits(mesh, [array.shape for array in arrays])
        return fused(*arrays) if fits else step(*arrays)

    return run
```

```python
import functools

import jax
import jax.numpy as jnp
from jax import lax
from jax.experimental import pallas as pl
from jax.experimental.pallas import tpu as pltpu
from jax.sharding import PartitionSpec as P


HEAD = 64
BLOCK = 256
EXTRA = 8


eps = 1e-05
F32 = jnp.float32
BF16 = jnp.bfloat16


def split(value):
    high = value.astype(BF16)
    return high, (value - high.astype(F32)).astype(BF16)


def per_head(columns, lanes):
    heads = columns.shape[1]
    out = jnp.broadcast_to(columns[:, 0:1], lanes.shape)
    for head in range(1, heads):
        out = jnp.where(lanes // HEAD == head, columns[:, head : head + 1], out)
    return out


def gathered_update(keys, values, column, lanes, end):
    scale = HEAD ** (-0.5)
    weighted = keys.astype(F32) * (jnp.exp(per_head(end - column, lanes)) * scale)
    high, low = split(weighted)
    dims = (((0,), (0,)), ((), ()))
    return lax.dot_general(high, values, dims, preferred_element_type=F32) + lax.dot_general(
        low, values, dims, preferred_element_type=F32
    )


def state_kernel(key_ref, value_ref, column_ref, out_ref):
    width = key_ref.shape[1]
    step = pl.program_id(0)

    @pl.when(step == 0)
    def _():
        out_ref[0:width, :] = jnp.zeros((width, width), F32)
        out_ref[width:, :] = jnp.zeros((EXTRA, width), F32)

    lanes = lax.broadcasted_iota(jnp.int32, key_ref.shape, 1)
    column = column_ref[...]
    end = column[BLOCK - 1 : BLOCK, :]
    end_lanes = per_head(end, lanes[0:1, :])
    fresh = gathered_update(key_ref[...], value_ref[...], column, lanes, end)
    out_ref[0:width, :] = out_ref[0:width, :] * jnp.exp(end_lanes) + fresh
    out_ref[width:, :] = out_ref[width:, :] + end_lanes


def retention_kernel(
    mine_ref, query_ref, key_ref, value_ref, gate_ref, column_ref, row_ref, gain_ref, states_ref,
    out_ref, state
):
    rows, width = query_ref.shape
    heads = width // HEAD
    step = pl.program_id(0)
    count = states_ref.shape[0]
    row_ids = lax.broadcasted_iota(jnp.int32, (width, width), 0) // HEAD
    column_ids = lax.broadcasted_iota(jnp.int32, (width, width), 1) // HEAD

    @pl.when(step == 0)
    def _():
        total = jnp.zeros((width, width), F32)
        for position in range(count - 1):
            decay = jnp.exp(states_ref[position, width : width + 1, :])
            longer = total * decay + states_ref[position, 0:width, :]
            total = jnp.where(position < mine_ref[0], longer, total)
        state[...] = jnp.where(row_ids == column_ids, total, 0.0)

    lanes = lax.broadcasted_iota(jnp.int32, (rows, width), 1)
    queries, keys, values = query_ref[...], key_ref[...], value_ref[...]
    column = column_ref[...]
    end = column[rows - 1 : rows, :]
    causal = lax.broadcasted_iota(jnp.int32, (rows, rows), 0) >= lax.broadcasted_iota(
        jnp.int32, (rows, rows), 1
    )
    scale = HEAD ** (-0.5)
    high, low = split(state[...])
    carried = jnp.dot(queries, high, preferred_element_type=F32) + jnp.dot(
        queries, low, preferred_element_type=F32
    )
    retained = carried * jnp.exp(per_head(column, lanes))
    inner = None
    for head in range(heads):
        own = jnp.where(lanes // HEAD == head, queries.astype(F32), 0.0).astype(BF16)
        scores = lax.dot_general(
            own, keys, (((1,), (1,)), ((), ())), preferred_element_type=F32
        )
        spread = column[:, head : head + 1] - row_ref[0, head : head + 1, :]
        damping = jnp.exp(jnp.where(causal, spread, -jnp.inf))
        factor = (scores * scale * damping).astype(BF16)
        term = jnp.dot(factor, values, preferred_element_type=F32)
        inner = term if inner is None else jnp.where(lanes // HEAD == head, term, inner)
    retained = retained + inner
    fresh = gathered_update(keys, values, column, lanes, end)
    end_lanes = per_head(end, lanes[0:1, :])
    state[...] = state[...] * jnp.exp(end_lanes) + jnp.where(row_ids == column_ids, fresh, 0.0)

    def head_mean(array):
        out = None
        for head in range(heads):
            inside = lanes // HEAD == head
            mean = jnp.sum(jnp.where(inside, array, 0.0), axis=1, keepdims=True) * (1.0 / HEAD)
            out = jnp.broadcast_to(mean, array.shape) if out is None else jnp.where(inside, mean, out)
        return out

    centered = retained - head_mean(retained)
    normed = centered * lax.rsqrt(head_mean(centered * centered) + eps)
    gates = gate_ref[...].astype(F32)
    out_ref[...] = (normed * gain_ref[...] * (gates * jax.nn.sigmoid(gates))).astype(BF16)


def retention(query_rows, key_rows, value_rows, gate_rows, log_decay, head_gain):
    rows, width = query_rows.shape
    heads = width // HEAD
    count = rows // BLOCK
    running = jnp.cumsum(log_decay.reshape(heads, count, BLOCK), axis=2)
    row = running.transpose(1, 0, 2)
    column = running.reshape(heads, rows).T
    block = pl.BlockSpec((BLOCK, width), lambda i: (i, 0))
    column_block = pl.BlockSpec((BLOCK, heads), lambda i: (i, 0))
    state_call = pl.pallas_call(
        state_kernel,
        grid=(count,),
        in_specs=[block, block, column_block],
        out_specs=pl.BlockSpec((width + EXTRA, width), lambda i: (0, 0)),
        out_shape=jax.ShapeDtypeStruct((width + EXTRA, width), F32),
        compiler_params=pltpu.CompilerParams(dimension_semantics=("arbitrary",)),
        cost_estimate=pl.CostEstimate(
            flops=4 * rows * width * width, bytes_accessed=4 * rows * width, transcendentals=rows * width
        ),
    )
    own = state_call(key_rows, value_rows, column)
    states = lax.all_gather(own, "sp")
    mine = lax.axis_index("sp").astype(jnp.int32).reshape(1)
    return pl.pallas_call(
        retention_kernel,
        grid=(count,),
        in_specs=[
            pl.BlockSpec(memory_space=pltpu.SMEM),
            block,
            block,
            block,
            block,
            column_block,
            pl.BlockSpec((1, heads, BLOCK), lambda i: (i, 0, 0)),
            pl.BlockSpec((1, width), lambda i: (0, 0)),
            pl.BlockSpec(states.shape, lambda i: (0, 0, 0)),
        ],
        out_specs=block,
        out_shape=jax.ShapeDtypeStruct((rows, width), BF16),
        scratch_shapes=[pltpu.VMEM((width, width), F32)],
        compiler_params=pltpu.CompilerParams(dimension_semantics=("arbitrary",)),
        cost_estimate=pl.CostEstimate(
            flops=8 * rows * width * BLOCK,
            bytes_accessed=10 * rows * width,
            transcendentals=rows * BLOCK * heads,
        ),
    )(mine, query_rows, key_rows, value_rows, gate_rows, column, row, head_gain[None, :], states)


def send(piece, pairs):
    return lax.ppermute(piece, "tp", pairs)


def ring_start(own):
    size = lax.axis_size("tp")
    right = [(i, (i + 2) % size) for i in range(size)]
    left = [(i, (i - 2) % size) for i in range(size)]
    swap = [(i, i ^ 1) for i in range(size)]
    return send(own, right), send(own, left), send(own, swap)


def ring_finish(own, from_left, from_right, other):
    size = lax.axis_size("tp")
    chips = size // 2
    right = [(i, (i + 2) % size) for i in range(size)]
    left = [(i, (i - 2) % size) for i in range(size)]
    swap = [(i, i ^ 1) for i in range(size)]
    half = own.shape[1] // 2
    last = chips // 2
    pieces = [[own], [other]]
    for hop in range(1, (chips - 1) // 2 + 1):
        if hop > 1:
            from_left = send(from_left, right)
            from_right = send(from_right, left)
        for piece in (from_left, from_right):
            pieces += [[piece], [send(piece, swap)]]
    if chips % 2 == 0 and last > 1:
        first = send(from_left[:, :half], right)
        second = send(from_right[:, half:], left)
        pieces += [[first, second], [send(first, swap), send(second, swap)]]
    elif chips == 2:
        pieces += [[from_left], [send(from_left, swap)]]
    return pieces


def expert_kernel(layout, row_ref, *refs):
    count = len(layout)
    piece_refs, out_ref = refs[:count], refs[count]
    weights, middle, sems = refs[count + 1 :]
    slots, _, width, ff = weights.shape
    rows = row_ref.shape[0]
    copies = []
    for index, (slot, start, length) in enumerate(layout):
        copy = pltpu.make_async_copy(
            piece_refs[index], weights.at[slot, :, pl.ds(start, length), :], sems.at[index]
        )
        copy.start()
        copies.append(copy)
    tile = rows // 2
    for pair in range(slots // 2):
        for index, (slot, _, _) in enumerate(layout):
            if slot // 2 == pair:
                copies[index].wait()

        @pl.loop(0, 2)
        def _(step):
            span = pl.ds(pl.multiple_of(step * tile, tile), tile)
            block = row_ref[span, :]
            gate = jnp.concatenate([weights[2 * pair, 0], weights[2 * pair + 1, 0]], axis=1)
            up = jnp.concatenate([weights[2 * pair, 1], weights[2 * pair + 1, 1]], axis=1)
            gated = jnp.dot(block, gate, preferred_element_type=F32)
            raised = jnp.dot(block, up, preferred_element_type=F32)
            value = gated * jax.nn.sigmoid(gated) * raised
            middle[span, 2 * pair * ff : 2 * (pair + 1) * ff] = value.astype(BF16)

    part = 512

    @pl.loop(0, width // part)
    def _(step):
        span = pl.ds(pl.multiple_of(step * part, part), part)
        down = jnp.concatenate([weights[slot, 2, span, :] for slot in range(slots)], axis=1)
        out_ref[:, span] = lax.dot_general(
            middle[...], down, (((1,), (1,)), ((), ())), preferred_element_type=F32
        ).astype(BF16)


def experts(rows, shards):
    _, width, ff = shards[0][0].shape
    count = len(shards)
    if ff % 128 or count % 2:
        whole = jnp.concatenate([jnp.concatenate(shard, axis=1) for shard in shards], axis=2)
        middle = (
            jax.nn.silu(jnp.dot(rows, whole[0], preferred_element_type=F32))
            * jnp.dot(rows, whole[1], preferred_element_type=F32)
        ).astype(BF16)
        return lax.dot_general(
            middle, whole[2], (((1,), (1,)), ((), ())), preferred_element_type=F32
        ).astype(BF16)
    layout, pieces = [], []
    for slot, shard in enumerate(shards):
        start = 0
        for piece in shard:
            layout.append((slot, start, piece.shape[1]))
            pieces.append(piece)
            start += piece.shape[1]
    return pl.pallas_call(
        functools.partial(expert_kernel, layout),
        in_specs=[pl.BlockSpec(memory_space=pltpu.VMEM)]
        + [pl.BlockSpec(memory_space=pl.ANY)] * len(pieces),
        out_specs=pl.BlockSpec(memory_space=pltpu.VMEM),
        out_shape=jax.ShapeDtypeStruct(rows.shape, BF16),
        scratch_shapes=[
            pltpu.VMEM((count, 3, width, ff), BF16),
            pltpu.VMEM((rows.shape[0], count * ff), BF16),
            pltpu.SemaphoreType.DMA((len(pieces),)),
        ],
        compiler_params=pltpu.CompilerParams(vmem_limit_bytes=60 * 1024 * 1024),
        cost_estimate=pl.CostEstimate(
            flops=6 * rows.shape[0] * width * count * ff,
            bytes_accessed=6 * width * count * ff + 4 * rows.size,
            transcendentals=rows.shape[0] * count * ff,
        ),
    )(rows, *pieces)


def on_device(
    query_rows,
    key_rows,
    value_rows,
    gate_rows,
    log_decay,
    residual,
    head_gain,
    out_weight,
    norm_gain,
    expert_ids,
    route_weights,
    expert_gate,
    expert_up,
    expert_down,
    shared_gate,
    shared_up,
    shared_down,
):
    part = out_weight.shape[0] // lax.axis_size("sp")
    own_part = lax.dynamic_slice_in_dim(out_weight, lax.axis_index("sp") * part, part, 0)
    out_part = lax.all_gather(own_part, "tp", axis=1, tiled=True)
    out_full = lax.all_gather(out_part, "sp", axis=0, tiled=True)
    shard = jnp.stack([expert_gate, expert_up, expert_down])
    shard, log_decay = lax.optimization_barrier((shard, log_decay))
    from_left, from_right, other = ring_start(shard)

    specialists = lax.axis_size("sp")
    tokens, chosen = expert_ids.shape
    width = residual.shape[1]
    capacity = 3 * tokens * chosen // (2 * specialists)
    names = jnp.arange(specialists, dtype=jnp.int32)[:, None]
    named = [expert_ids[:, j][None, :] == names for j in range(chosen)]
    match = functools.reduce(jnp.logical_or, named)
    weight = sum(jnp.where(named[j], route_weights[:, j][None, :], 0.0) for j in range(chosen))
    earlier = jnp.arange(tokens)[:, None] < jnp.arange(tokens)[None, :]
    position = jnp.dot(match.astype(BF16), earlier.astype(BF16), preferred_element_type=F32)
    place = jnp.where(match, position.astype(jnp.int32), -1)
    sits = place[:, None, :] == jnp.arange(capacity, dtype=jnp.int32)[None, :, None]
    pick = sits.astype(BF16).reshape(specialists * capacity, tokens)
    weight_high = lax.reduce_precision(weight, 8, 7)
    weight_low = weight - weight_high
    back_high = jnp.where(sits, weight_high[:, None, :], 0.0).astype(BF16)
    back_low = jnp.where(sits, weight_low[:, None, :], 0.0).astype(BF16)

    ret_rows = retention(query_rows, key_rows, value_rows, gate_rows, log_decay, head_gain)
    token_rows = lax.all_to_all(ret_rows, "tp", split_axis=0, concat_axis=1, tiled=True)
    token_rows, from_left, from_right = lax.optimization_barrier((token_rows, from_left, from_right))
    shards = ring_finish(shard, from_left, from_right, other)
    mixer = jnp.dot(token_rows, out_full, preferred_element_type=F32)
    hidden = (residual.astype(F32) + mixer).astype(BF16)
    hidden_wide = hidden.astype(F32)
    normed_rows = (
        hidden_wide
        * lax.rsqrt(jnp.mean(hidden_wide * hidden_wide, axis=1, keepdims=True) + eps)
        * norm_gain
    ).astype(BF16)
    outgoing = jnp.dot(pick, normed_rows, preferred_element_type=F32).astype(BF16)
    outgoing = outgoing.reshape(specialists, capacity, width)
    arrived = lax.all_to_all(outgoing, "sp", split_axis=0, concat_axis=0, tiled=True)
    shared_mid = (
        jax.nn.silu(jnp.dot(normed_rows, shared_gate, preferred_element_type=F32))
        * jnp.dot(normed_rows, shared_up, preferred_element_type=F32)
    ).astype(BF16)
    shared_out = lax.dot_general(
        shared_mid, shared_down, (((1,), (1,)), ((), ())), preferred_element_type=F32
    )
    flat_rows = arrived.reshape(-1, width)
    processed = experts(flat_rows, shards).reshape(arrived.shape)
    returned = lax.all_to_all(processed, "sp", split_axis=0, concat_axis=0, tiled=True)
    dims = (((0, 1), (0, 1)), ((), ()))
    routed = lax.dot_general(back_high, returned, dims, preferred_element_type=F32)
    routed += lax.dot_general(back_low, returned, dims, preferred_element_type=F32)
    return (hidden_wide + routed + shared_out).astype(BF16)


MESH = pl.DeviceIdType.MESH
NT = (((1,), (1,)), ((), ()))
TN = (((0,), (0,)), ((), ()))


def thirds(value):
    first = value.astype(BF16)
    rest = value - first.astype(F32)
    second = rest.astype(BF16)
    return first, second, (rest - second.astype(F32)).astype(BF16)


def piece_widths(depth):
    return [128] + [256] * ((depth - 256) // 256) + [128]


def layer_kernel(
    query_hbm, key_hbm, value_hbm, gate_hbm, decay_hbm, residual_hbm, head_gain_hbm, out_weight_hbm,
    norm_gain_hbm, ids_hbm, route_hbm, expert_gate_hbm, expert_up_hbm, expert_down_hbm,
    shared_gate_hbm, shared_up_hbm, shared_down_hbm,
    result_ref,
    decay_ref, head_gain_ref, norm_gain_ref, ids_ref, route_ref,
    query, key, value, gates, residual, shared_gate, shared_up, shared_down,
    weights, out_full, running, row_running, updates, states, state, inner, ret_rows, token_rows,
    hidden, normed, squares, tables, outgoing, arrived, middle, processed, direct, passing, merged,
    combined, final, base, shared_middle, back, shares,
    local_sem, state_send, state_recv, mix_send, mix_recv, out_z_send, out_xy_send, out_z_recv, out_xy_recv,
    out_pair_send, out_pair_recv, right_send, left_send, pair_send, line_recv, pair_recv, pair_down_recv,
    go_send, go_recv, table_send, table_recv, direct_send, direct_recv, passing_send, passing_recv,
    merged_send, merged_recv, final_send, final_recv, hello,
):
    places_count = states.shape[0]
    size = token_rows.shape[0]
    chips = size // 2
    sp = lax.axis_index("sp")
    tp = lax.axis_index("tp")
    z, core = tp // 2, tp % 2
    blocks, rows, width = ret_rows.shape
    heads = width // HEAD
    depth = residual.shape[1]
    capacity = arrived.shape[1]
    specialists = arrived.shape[0]
    ff = weights.shape[3]
    quarter = out_full.shape[1] // places_count
    out_columns = out_full.shape[2]
    widths = piece_widths(depth)
    pieces = len(widths)
    starts = [sum(widths[:index]) for index in range(pieces)]
    half = depth // 2
    tile = processed.shape[3]
    scale = HEAD ** (-0.5)
    inputs = (expert_gate_hbm, expert_up_hbm, expert_down_hbm)
    units = [(which, start, half) for which in (0, 1) for start in (0, half)]
    first_down = len(units)
    units += [(2, start, length) for start, length in zip(starts, widths)]

    def remote(src, dst, send, recv, device):
        return pltpu.make_async_remote_copy(
            src_ref=src, dst_ref=dst, send_sem=send, recv_sem=recv, device_id=device, device_id_type=MESH
        )

    partner = (sp, z * 2 + 1 - core)
    right = (sp, tp + 2)
    left = (sp, tp - 2)

    local = [
        pltpu.make_async_copy(src, dst, local_sem.at[index])
        for index, (src, dst) in enumerate(
            [
                (decay_hbm, decay_ref),
                (ids_hbm, ids_ref),
                (route_hbm, route_ref),
                (key_hbm, key),
                (value_hbm, value),
                (query_hbm, query),
                (gate_hbm, gates),
                (head_gain_hbm, head_gain_ref),
                (norm_gain_hbm, norm_gain_ref),
                (out_weight_hbm, out_full.at[tp]),
                (residual_hbm, residual),
                (shared_gate_hbm, shared_gate),
                (shared_up_hbm, shared_up),
                (shared_down_hbm, shared_down),
                (expert_gate_hbm, weights.at[tp, 0]),
                (expert_up_hbm, weights.at[tp, 1]),
                (expert_down_hbm, weights.at[tp, 2]),
            ]
        )
    ]
    barrier = pltpu.get_barrier_semaphore()

    def greet(flag):
        for step in (1, 2):
            pl.semaphore_signal(flag, inc=1, device_id=(sp ^ step, tp), device_id_type=MESH)
        pl.semaphore_signal(flag, inc=1, device_id=partner, device_id_type=MESH)

        @pl.when(z < chips - 1)
        def _():
            pl.semaphore_signal(flag, inc=1, device_id=right, device_id_type=MESH)

        @pl.when(z > 0)
        def _():
            pl.semaphore_signal(flag, inc=1, device_id=left, device_id_type=MESH)

    def greeted(flag):
        pl.semaphore_wait(flag, jnp.where(jnp.logical_or(z == 0, z == chips - 1), 4, 5))

    greet(barrier)
    for copy in local[:9]:
        copy.start()
    greeted(barrier)
    greet(hello.at[0])

    def weight_copy(origin, unit, send, device, own=False, pair=False):
        which, start, length = units[unit]
        span = pl.ds(start, length)
        there = weights.at[origin * 2 + core, which, span, :]
        here = inputs[which].at[span, :] if own else there
        if not pair:
            received = line_recv.at[origin, unit]
        elif unit < first_down:
            received = pair_recv.at[origin]
        else:
            received = pair_down_recv.at[unit - first_down]
        return remote(here, there, send, received, device)

    def to_partner(origin, unit, own=False):
        return weight_copy(origin, unit, pair_send.at[origin], partner, own, True)

    def own_send(unit):
        @pl.when(z < chips - 1)
        def _():
            weight_copy(z, unit, right_send.at[z], right, True).start()

        @pl.when(z > 0)
        def _():
            weight_copy(z, unit, left_send.at[z], left, True).start()

        to_partner(z, unit, True).start()

    def relay(unit, distance):
        @pl.when(z - distance >= 0)
        def _():
            origin = z - distance
            copy = weight_copy(origin, unit, right_send.at[origin], right)
            copy.wait_recv()

            @pl.when(z < chips - 1)
            def _():
                copy.start()

            to_partner(origin, unit).start()

        @pl.when(z + distance < chips)
        def _():
            origin = z + distance
            copy = weight_copy(origin, unit, left_send.at[origin], left)
            copy.wait_recv()

            @pl.when(z > 0)
            def _():
                copy.start()

            to_partner(origin, unit).start()

    def from_partner(origin):
        there = weights.at[0, 0:2]
        remote(there, there, pair_send.at[origin], pair_recv.at[origin], partner).wait_recv()

    def downs_from_partner(index):
        there = weights.at[0, 2, pl.ds(0, chips * widths[index]), :]
        remote(there, there, pair_send.at[0], pair_down_recv.at[index], partner).wait_recv()

    def out_z(step):
        target = (z + step) % chips
        span = pl.ds(pl.multiple_of(sp * quarter, quarter), quarter)
        return remote(
            out_weight_hbm.at[span, :], out_full.at[tp, span, :], out_z_send, out_z_recv.at[z],
            (sp, target * 2 + core),
        )

    def out_z_arrival(step):
        origin = (z + step) % chips
        there = out_full.at[0, pl.ds(0, quarter), :]
        return remote(there, there, out_z_send, out_z_recv.at[origin], partner)

    def out_piece(step, device):
        origin = (z + step) % chips
        span = pl.ds(pl.multiple_of(sp * quarter, quarter), quarter)
        there = out_full.at[origin * 2 + core, span, :]
        return remote(there, there, out_xy_send.at[step - 1], out_xy_recv.at[origin], device)

    def out_pieces(step):
        origin = (z + step) % chips
        there = out_full.at[0, pl.ds(0, (places_count - 1) * quarter), :]
        return remote(there, there, out_xy_send.at[step - 1], out_xy_recv.at[origin], partner)

    def out_pair(slot, own=False):
        return remote(
            out_weight_hbm if own else out_full.at[slot], out_full.at[slot], out_pair_send,
            out_pair_recv, partner,
        )

    def out_pairs():
        there = out_full.at[0:chips]
        return remote(there, there, out_pair_send, out_pair_recv, partner)

    @pl.when(z < chips - 1)
    def _():
        out_z(1).start()

    @pl.when(z > 0)
    def _():
        out_z(chips - 1).start()

    own_send(0)
    out_pair(tp, True).start()
    for copy in local[9:]:
        copy.start()

    for copy in local[:3]:
        copy.wait()

    row_ids = lax.broadcasted_iota(jnp.int32, (width, width), 0) // HEAD
    column_ids = lax.broadcasted_iota(jnp.int32, (width, width), 1) // HEAD
    same_head = row_ids == column_ids
    lanes = lax.broadcasted_iota(jnp.int32, (rows, width), 1)
    later = lax.broadcasted_iota(jnp.int32, (rows, rows), 0)
    sooner = lax.broadcasted_iota(jnp.int32, (rows, rows), 1)
    lower = jnp.where(later >= sooner, 1.0, 0.0).astype(BF16)
    upper = jnp.where(later <= sooner, 1.0, 0.0).astype(BF16)

    chosen, tokens = ids_ref.shape
    names = lax.broadcasted_iota(jnp.int32, (8, tokens), 0)
    match = names < 0
    weight = jnp.zeros((8, tokens), F32)
    for j in range(chosen):
        named = ids_ref[j : j + 1, :] == names
        match = jnp.logical_or(match, named)
        weight = weight + jnp.where(named, route_ref[j : j + 1, :], 0.0)
    strict = jnp.where(later < sooner, 1.0, 0.0).astype(BF16)
    position = jnp.dot(jnp.where(match, 1.0, 0.0).astype(BF16), strict, preferred_element_type=F32)
    tables[0, 0:8, :] = jnp.where(match, position, -1.0)
    tables[0, 8:16, :] = weight

    def table_copy(step):
        return remote(
            tables.at[0], tables.at[step], table_send, table_recv.at[step - 1], (sp ^ step, tp)
        )

    greeted(hello.at[0])
    greet(hello.at[1])
    listed = jnp.concatenate(
        [
            decay_ref[head : head + 1, block * rows : (block + 1) * rows]
            for head in range(heads)
            for block in range(blocks)
        ],
        axis=0,
    )
    row_running[...] = functools.reduce(
        jnp.add, [jnp.dot(part, upper, preferred_element_type=F32) for part in thirds(listed)]
    )
    head_rows = lax.broadcasted_iota(jnp.int32, (width, rows), 0) // HEAD
    for block in range(blocks):
        spread = jnp.broadcast_to(listed[block : block + 1, :], (width, rows))
        for head in range(1, heads):
            spread = jnp.where(
                head_rows == head, listed[head * blocks + block : head * blocks + block + 1, :], spread
            )
        running[block] = functools.reduce(
            jnp.add,
            [
                lax.dot_general(lower, part, NT, preferred_element_type=F32)
                for part in thirds(spread)
            ],
        )

    greeted(hello.at[1])
    greet(hello.at[2])

    @pl.when(z == chips - 1)
    def _():
        out_z(1).start()

    for step in range(2, chips - 1):
        out_z(step).start()

    @pl.when(z == 0)
    def _():
        out_z(chips - 1).start()

    own_send(1)
    for copy in local[3:5]:
        copy.wait()
    state[...] = jnp.zeros((width + EXTRA, width), F32)

    @pl.loop(0, blocks)
    def _(block):
        span = pl.ds(pl.multiple_of(block * rows, rows), rows)
        column = running[block]
        end = column[rows - 1 : rows, :]
        weighted = key[span, :].astype(F32) * (jnp.exp(end - column) * scale)
        high, low = split(weighted)
        fresh = lax.dot_general(high, value[span, :], TN, preferred_element_type=F32)
        fresh += lax.dot_general(low, value[span, :], TN, preferred_element_type=F32)
        fresh = jnp.where(same_head, fresh, 0.0)
        updates[block] = fresh
        state[0:width, :] = state[0:width, :] * jnp.exp(end) + fresh
        state[width:, :] = state[width:, :] + end

    greeted(hello.at[2])
    states[sp] = state[...]

    def state_copy(step):
        return remote(
            state, states.at[sp], state_send, state_recv.at[sp], (sp ^ step, tp)
        )

    def state_arrival(step):
        return remote(
            state, states.at[sp ^ step], state_send, state_recv.at[sp ^ step], (sp ^ step, tp)
        )

    local[5].wait()
    for step in range(1, places_count):
        state_copy(step).start()
    for step in (1, 2):
        table_copy(step).start()

    @pl.loop(0, blocks)
    def _(block):
        span = pl.ds(pl.multiple_of(block * rows, rows), rows)
        queries, keys, values = query[span, :], key[span, :], value[span, :]
        column = running[block]
        causal = later >= sooner
        total = None
        for head in range(heads):
            own = jnp.where(lanes // HEAD == head, queries.astype(F32), 0.0).astype(BF16)
            scores = lax.dot_general(own, keys, NT, preferred_element_type=F32)
            spread = column[:, head * HEAD : head * HEAD + 1] - row_running[pl.ds(head * blocks + block, 1), :]
            damping = jnp.exp(jnp.where(causal, spread, -jnp.inf))
            factor = (scores * scale * damping).astype(BF16)
            term = jnp.dot(factor, values, preferred_element_type=F32)
            total = term if total is None else jnp.where(lanes // HEAD == head, term, total)
        inner[block] = total

    for step in range(1, places_count):
        state_arrival(step).wait_recv()
    there = states.at[pl.ds(0, places_count - 1)]
    remote(there, there, state_send, state_recv.at[0], partner).wait_send()
    total = jnp.zeros((width, width), F32)
    for position in range(places_count - 1):
        longer = total * jnp.exp(states[position, width : width + 1, :]) + states[position, 0:width, :]
        total = jnp.where(position < sp, longer, total)
    state[0:width, :] = total
    local[6].wait()
    local[7].wait()

    def head_mean(array):
        out = None
        for head in range(heads):
            inside = lanes // HEAD == head
            mean = jnp.sum(jnp.where(inside, array, 0.0), axis=1, keepdims=True) * (1.0 / HEAD)
            out = jnp.broadcast_to(mean, array.shape) if out is None else jnp.where(inside, mean, out)
        return out

    def mix_copy(block):
        return remote(
            ret_rows.at[block], token_rows.at[tp], mix_send, mix_recv.at[tp], (sp, block)
        )

    def mix_start(block):
        @pl.when(block != tp)
        def _():
            mix_copy(block).start()

    @pl.loop(0, blocks)
    def _(block):
        span = pl.ds(pl.multiple_of(block * rows, rows), rows)
        column = running[block]
        end = column[rows - 1 : rows, :]
        before = state[0:width, :]
        high, low = split(before)
        queries = query[span, :]
        carried = jnp.dot(queries, high, preferred_element_type=F32) + jnp.dot(
            queries, low, preferred_element_type=F32
        )
        state[0:width, :] = before * jnp.exp(end) + updates[block]
        retained = carried * jnp.exp(column) + inner[block]
        centered = retained - head_mean(retained)
        norm = centered * lax.rsqrt(head_mean(centered * centered) + eps)
        gate = gates[span, :].astype(F32)
        mixed = (norm * head_gain_ref[...] * (gate * jax.nn.sigmoid(gate))).astype(BF16)
        ret_rows[block] = mixed

        @pl.when(block == tp)
        def _():
            token_rows[tp] = mixed

        @pl.when(block > 0)
        def _():
            mix_start(block - 1)

    mix_start(blocks - 1)

    between = jnp.logical_and(z > 0, z < chips - 1)

    @pl.when(jnp.logical_not(between))
    def _():
        for unit in range(2, len(units)):
            own_send(unit)

    for step in range(1, chips):
        out_z_arrival(step).wait_recv()
        for other in range(1, places_count):
            out_piece(step, (sp ^ other, tp)).start()

    @pl.when(jnp.logical_not(between))
    def _():
        relay(0, 1)
        relay(1, 1)

    @pl.when(between)
    def _():
        relay(0, 1)
        own_send(2)
        relay(1, 1)
        own_send(3)

    def pass_on(unit, distance, rightward):
        origin = z - distance if rightward else z + distance
        sent, device = (right_send, right) if rightward else (left_send, left)
        copy = weight_copy(origin, unit, sent.at[origin], device)
        copy.wait_recv()
        copy.start()
        to_partner(origin, unit).start()

    def inward(unit):
        for chip, rightward in ((1, True), (chips - 2, False)):

            @pl.when(z == chip)
            def _():
                sent, device = (right_send, right) if rightward else (left_send, left)
                weight_copy(z, unit, sent.at[z], device, True).start()
                to_partner(z, unit, True).start()
                pass_on(unit, 1, rightward)

    def outward(unit):
        for chip, rightward in ((1, False), (chips - 2, True)):

            @pl.when(z == chip)
            def _():
                sent, device = (right_send, right) if rightward else (left_send, left)
                weight_copy(z, unit, sent.at[z], device, True).start()
                for distance in (1, 2):
                    pass_on(unit, distance, rightward)


    slot_rows = lax.broadcasted_iota(jnp.int32, (capacity, tokens), 0).astype(F32)
    for step in (1, 2):
        table_copy(step).wait_recv()
    for turn, (table, pair) in enumerate(
        ((0, (0, 2)), (0, (0, 1)), (1, (0, 2)), (2, (0, 1)), (0, (2, 3)))
    ):
        for side, other in enumerate(pair):
            name = sp ^ other
            place = tables[table, pl.ds(name, 1), :]
            back[turn, side] = jnp.where(place == slot_rows, 1.0, 0.0).T.astype(BF16)
            share = tables[table, pl.ds(8 + name, 1), :]
            shares[turn, side] = jnp.broadcast_to(share, (tile, tokens)).T

    for copy in local[8:11]:
        copy.wait()
    for step in range(1, chips):
        out_pieces(step).wait_recv()
        out_pair(((z + step) % chips) * 2 + core).start()
    out_pairs().wait_recv()
    for step in range(1, size):
        source = (tp + step) % size
        remote(
            ret_rows.at[0], token_rows.at[source], mix_send, mix_recv.at[source], (sp, source)
        ).wait_recv()

    squares[...] = jnp.zeros(squares.shape, F32)

    @pl.loop(0, size)
    def _(slot):
        span = pl.ds(pl.multiple_of(slot * out_columns, out_columns), out_columns)
        token = jnp.concatenate([token_rows[index] for index in range(size)], axis=1)
        mixer = jnp.dot(token, out_full[slot], preferred_element_type=F32)
        total = (residual[:, span].astype(F32) + mixer).astype(BF16)
        hidden[:, span] = total
        wide = total.astype(F32)
        wide = wide * wide
        squares[...] += functools.reduce(
            jnp.add, [wide[:, start : start + 128] for start in range(0, out_columns, 128)]
        )

    factor = lax.rsqrt(jnp.sum(squares[...], axis=1, keepdims=True) * (1.0 / depth) + eps)

    @pl.loop(0, depth // 256)
    def _(index):
        span = pl.ds(pl.multiple_of(index * 256, 256), 256)
        normed[:, span] = (hidden[:, span].astype(F32) * factor * norm_gain_ref[:, span]).astype(BF16)

    relay(0, 2)

    def go(step):
        return remote(
            outgoing.at[step - 1], arrived.at[sp], go_send, go_recv.at[sp], (sp ^ step, tp)
        )

    for step in list(range(places_count - 1, -1, -1)):
        sits = jnp.where(tables[0, pl.ds(sp ^ step, 1), :] == slot_rows, 1.0, 0.0).astype(BF16)

        @pl.loop(0, depth // 512)
        def _(index):
            span = pl.ds(pl.multiple_of(index * 512, 512), 512)
            picked = jnp.dot(sits, normed[:, span], preferred_element_type=F32).astype(BF16)
            if step:
                outgoing[step - 1, :, span] = picked
            else:
                arrived[sp, :, span] = picked

        if step:
            go(step).start()

    relay(1, 2)
    relay(2, 1)

    for copy in local[11:14]:
        copy.wait()
    shared = shared_gate.shape[1]

    @pl.loop(0, shared // 256)
    def _(index):
        span = pl.ds(pl.multiple_of(index * 256, 256), 256)
        gated = jnp.dot(normed[...], shared_gate[:, span], preferred_element_type=F32)
        raised = jnp.dot(normed[...], shared_up[:, span], preferred_element_type=F32)
        shared_middle[:, span] = (gated * jax.nn.sigmoid(gated) * raised).astype(BF16)

    @pl.loop(0, depth // 512)
    def _(index):
        span = pl.ds(pl.multiple_of(index * 512, 512), 512)
        base[:, span] = hidden[:, span].astype(F32) + lax.dot_general(
            shared_middle[...], shared_down[span, :], NT, preferred_element_type=F32
        )

    relay(0, 3)
    relay(3, 1)
    relay(2, 2)
    relay(1, 3)
    relay(3, 2)
    inward(first_down)
    inward(first_down + 1)

    for copy in local[14:]:
        copy.wait()
    for step in range(1, places_count):
        remote(
            outgoing.at[0], arrived.at[sp ^ step], go_send, go_recv.at[sp ^ step], (sp ^ step, tp)
        ).wait_recv()

    outward(first_down)
    inward(first_down + 2)

    def pair_middle(chip):
        @pl.loop(0, specialists // 2)
        def _(index):
            rows_here = jnp.concatenate([arrived[2 * index], arrived[2 * index + 1]], axis=0)
            gate_pair = jnp.concatenate([weights[2 * chip, 0], weights[2 * chip + 1, 0]], axis=1)
            up_pair = jnp.concatenate([weights[2 * chip, 1], weights[2 * chip + 1, 1]], axis=1)
            gated = jnp.dot(rows_here, gate_pair, preferred_element_type=F32)
            raised = jnp.dot(rows_here, up_pair, preferred_element_type=F32)
            found = (gated * jax.nn.sigmoid(gated) * raised).astype(BF16)
            span = pl.ds(pl.multiple_of(index * 2 * capacity, 2 * capacity), 2 * capacity)
            middle[span, pl.ds(pl.multiple_of(chip * 2 * ff, 2 * ff), 2 * ff)] = found

    last_chip = jnp.where(z * 2 < chips, chips - 1, 0)

    def chip_at(index):
        if index == 0:
            return z
        if index == chips - 1:
            return last_chip
        toward = jnp.where(last_chip == 0, chips - 1 - index, index)
        shifted = jnp.where(last_chip == 0, chips - index, index - 1)
        passed = jnp.where(last_chip == 0, z <= chips - 1 - index, z >= index)
        return jnp.where(passed, shifted, toward)

    for index in range(chips):
        chip = chip_at(index)
        if index == chips - 1:
            relay(2, 3)
            relay(3, 3)
        from_partner(chip)
        pair_middle(chip)

    def tiles(index):
        return range(starts[index] // tile, (starts[index] + widths[index]) // tile)

    def piece_of(number):
        return next(index for index in range(pieces) if number in tiles(index))

    def arrivals(buffer, send, received, index):
        there = buffer.at[pl.ds(starts[index] // tile, widths[index] // tile)]
        remote(there, there, send, received.at[index], partner).wait_recv()

    def near(number):
        return sp ^ (2, 1)[number % 2]

    def far(number):
        return sp ^ (1, 2)[number % 2]

    def direct_copy(number):
        return remote(
            processed.at[number, near(number)], direct.at[number], direct_send,
            direct_recv.at[piece_of(number)], (near(number), tp),
        )

    def passing_copy(number):
        return remote(
            processed.at[number, sp ^ 3], passing.at[number], passing_send,
            passing_recv.at[piece_of(number)], (near(number), tp),
        )

    def merged_copy(number):
        return remote(
            merged.at[number], combined.at[number], merged_send,
            merged_recv.at[piece_of(number)], (far(number), tp),
        )

    def weighted(turn, first, second):
        first = jnp.dot(back[turn, 0], first, preferred_element_type=F32) * shares[turn, 0]
        return first + jnp.dot(back[turn, 1], second, preferred_element_type=F32) * shares[turn, 1]

    def merge(index):
        arrivals(passing, passing_send, passing_recv, index)
        for number in tiles(index):
            found = weighted(2 + number % 2, processed[number, far(number)], passing[number])
            merged[number] = found.astype(BF16)
        for number in tiles(index):
            merged_copy(number).start()

    last_tile = depth // tile - 1

    def final_copy(step):
        return remote(
            processed.at[last_tile, sp ^ step], final.at[step - 1], final_send, final_recv, (sp ^ step, tp)
        )

    def store(number, routed):
        span = slice(number * tile, (number + 1) * tile)
        result_ref[:, span] = (base[:, span] + routed).astype(BF16)

    def combine(index):
        arrivals(direct, direct_send, direct_recv, index)
        arrivals(merged, merged_send, merged_recv, index)
        for number in tiles(index):
            routed = weighted(number % 2, processed[number, sp], direct[number])
            store(number, routed + combined[number].astype(F32))

    lag = 3

    outward(first_down + 1)
    inward(first_down + 3)
    for index in range(pieces):
        unit = first_down + index

        if index + 2 < pieces:
            outward(unit + 2)
        if index + 4 < pieces:
            inward(unit + 4)

        @pl.when(jnp.logical_not(between))
        def _():
            for distance in range(1, chips):
                relay(unit, distance)

        downs_from_partner(index)
        down = jnp.concatenate(
            [weights[slot, 2, starts[index] : starts[index] + widths[index], :] for slot in range(size)], axis=1
        )

        if index == pieces - 1:
            for step in range(places_count - 1, -1, -1):
                span = pl.ds(pl.multiple_of((sp ^ step) * capacity, capacity), capacity)
                found = lax.dot_general(middle[span, :], down, NT, preferred_element_type=F32)
                processed[last_tile, sp ^ step] = found.astype(BF16)
                if step:
                    final_copy(step).start()
            merge(index - 1)
            continue
        found = lax.dot_general(middle[...], down, NT, preferred_element_type=F32).astype(BF16)
        for part, number in enumerate(tiles(index)):
            for source in range(specialists):
                processed[number, source] = found[
                    source * capacity : (source + 1) * capacity, part * tile : (part + 1) * tile
                ]

        for number in tiles(index):
            passing_copy(number).start()
        for number in tiles(index):
            direct_copy(number).start()
        if index:
            merge(index - 1)
        if index >= lag:
            combine(index - lag)

    for index in range(pieces - 1 - lag, pieces - 1):
        combine(index)
    remote(final, final, final_send, final_recv, partner).wait_recv()
    routed = weighted(1, processed[last_tile, sp], final[0]) + weighted(4, final[1], final[2])
    store(last_tile, routed)

    there = out_full.at[0, pl.ds(0, (chips - 1) * quarter), :]
    remote(there, there, out_z_send, out_z_recv.at[0], partner).wait_send()
    for step in range(1, chips):
        out_pieces(step).wait_send()
    out_pairs().wait_send()
    there = ret_rows.at[pl.ds(0, blocks - 1)]
    remote(there, there, mix_send, mix_recv.at[0], partner).wait_send()
    remote(outgoing, outgoing, go_send, go_recv.at[0], partner).wait_send()
    for buffer, sent, received in (
        (direct, direct_send, direct_recv), (passing, passing_send, passing_recv),
        (merged, merged_send, merged_recv),
    ):
        there = buffer.at[pl.ds(0, last_tile)]
        remote(there, there, sent, received.at[0], partner).wait_send()
    remote(final, final, final_send, final_recv, partner).wait_send()
    there = tables.at[0:2]
    remote(there, there, table_send, table_recv.at[0], partner).wait_send()
    for origin in range(chips):
        there = weights.at[origin]

        @pl.when(jnp.logical_and(origin <= z, z < chips - 1))
        def _():
            remote(there, there, right_send.at[origin], line_recv.at[0, 0], right).wait_send()

        @pl.when(jnp.logical_and(origin >= z, z > 0))
        def _():
            remote(there, there, left_send.at[origin], line_recv.at[0, 0], left).wait_send()

        remote(there, there, pair_send.at[origin], line_recv.at[0, 0], partner).wait_send()


def whole_layer(*arrays):
    (query, _, _, _, _, residual, head_gain, out_weight, norm_gain, ids, _, expert_gate) = arrays[:12]
    shared_gate = arrays[14]
    places_count, size = lax.axis_size("sp"), lax.axis_size("tp")
    rows_all, width = query.shape
    tokens, depth = residual.shape
    blocks = rows_all // tokens
    chosen = ids.shape[1]
    capacity = 3 * tokens * chosen // (2 * places_count)
    ff = expert_gate.shape[1]
    shared = shared_gate.shape[1]
    chips = size // 2
    pieces = len(piece_widths(depth))
    units = 4 + pieces
    heads = width // HEAD
    dma = pltpu.SemaphoreType.DMA
    arrays = list(arrays)
    arrays[6] = head_gain[None, :]
    arrays[8] = norm_gain[None, :]
    arrays[9], arrays[10] = arrays[9].T, arrays[10].T
    vmem, anywhere = pl.BlockSpec(memory_space=pltpu.VMEM), pl.BlockSpec(memory_space=pl.ANY)
    block = lambda *shape: pltpu.VMEM(shape, BF16)
    wide = lambda *shape: pltpu.VMEM(shape, F32)
    return pl.pallas_call(
        layer_kernel,
        in_specs=[anywhere] * len(arrays),
        out_specs=vmem,
        out_shape=pltpu.VMEM((tokens, depth), BF16),
        scratch_shapes=[
            wide(*arrays[4].shape), wide(1, width), wide(1, depth),
            pltpu.VMEM(arrays[9].shape, jnp.int32), wide(*arrays[10].shape),
            block(rows_all, width), block(rows_all, width), block(rows_all, width), block(rows_all, width),
            block(tokens, depth), block(depth, shared), block(depth, shared), block(depth, shared),
            block(size, 3, depth, ff),
            block(size, out_weight.shape[0], out_weight.shape[1]),
            wide(blocks, tokens, width),
            wide(heads * blocks, tokens),
            wide(blocks, width, width),
            wide(places_count, width + EXTRA, width),
            wide(width + EXTRA, width),
            wide(blocks, tokens, width),
            block(blocks, tokens, width),
            block(size, tokens, width),
            block(tokens, depth), block(tokens, depth),
            wide(tokens, 128),
            wide(3, 16, tokens),
            block(places_count - 1, capacity, depth),
            block(places_count, capacity, depth),
            block(places_count * capacity, size * ff),
            block(depth // 128, places_count, capacity, 128),
            block(depth // 128, capacity, 128), block(depth // 128, capacity, 128),
            block(depth // 128, tokens, 128), block(depth // 128, tokens, 128),
            block(places_count - 1, capacity, 128),
            wide(tokens, depth),
            block(tokens, shared),
            block(5, 2, tokens, capacity), wide(5, 2, tokens, 128),
            dma((17,)),
            dma, dma((places_count,)),
            dma, dma((size,)),
            dma, dma((chips - 1,)), dma((chips,)), dma((chips,)),
            dma, dma,
            dma((chips,)), dma((chips,)), dma((chips,)), dma((chips, units)), dma((chips,)), dma((pieces,)),
            dma, dma((places_count,)),
            dma, dma((2,)),
            dma, dma((pieces,)), dma, dma((pieces,)), dma, dma((pieces,)), dma, dma,
            pltpu.SemaphoreType.REGULAR((3,)),
        ],
        compiler_params=pltpu.CompilerParams(
            collective_id=0, has_side_effects=True, vmem_limit_bytes=58 * 1000 * 1000
        ),
        cost_estimate=pl.CostEstimate(
            flops=20 * 10**9, bytes_accessed=40 * 10**6, transcendentals=4 * 10**6
        ),
    )(*arrays)


def kernel_fits(mesh, shapes):
    places_count, size = mesh.shape["sp"], mesh.shape["tp"]
    if places_count != 4 or size != 8:
        return False
    width = shapes[0][1] // size
    tokens = shapes[5][0] // (places_count * size)
    rows_all = shapes[0][0] // places_count
    ff = shapes[11][1] // (places_count * size)
    return width == 128 and ff % 128 == 0 and tokens % 128 == 0 and rows_all == tokens * size


def solution(mesh):
    placed = (
        P("sp", "tp"),
        P("sp", "tp"),
        P("sp", "tp"),
        P("sp", "tp"),
        P("tp", "sp"),
        P(("sp", "tp"), None),
        P("tp"),
        P(None, "tp"),
        P(),
        P(("sp", "tp"), None),
        P(("sp", "tp"), None),
        P(None, ("sp", "tp")),
        P(None, ("sp", "tp")),
        P(None, ("sp", "tp")),
        P(),
        P(),
        P(),
    )

    placement = dict(mesh=mesh, in_specs=placed, out_specs=P(("sp", "tp"), None), check_vma=False)
    step = jax.shard_map(on_device, **placement)
    fused = jax.shard_map(whole_layer, **placement)

    def run(*arrays):
        fits = kernel_fits(mesh, [array.shape for array in arrays])
        return fused(*arrays) if fits else step(*arrays)

    return run
```

```python
import functools

import jax
import jax.numpy as jnp
from jax import lax
from jax.experimental import pallas as pl
from jax.experimental.pallas import tpu as pltpu
from jax.sharding import PartitionSpec as P


HEAD = 64
BLOCK = 256
EXTRA = 8


eps = 1e-05
F32 = jnp.float32
BF16 = jnp.bfloat16


def split(value):
    high = value.astype(BF16)
    return high, (value - high.astype(F32)).astype(BF16)


def per_head(columns, lanes):
    heads = columns.shape[1]
    out = jnp.broadcast_to(columns[:, 0:1], lanes.shape)
    for head in range(1, heads):
        out = jnp.where(lanes // HEAD == head, columns[:, head : head + 1], out)
    return out


def gathered_update(keys, values, column, lanes, end):
    scale = HEAD ** (-0.5)
    weighted = keys.astype(F32) * (jnp.exp(per_head(end - column, lanes)) * scale)
    high, low = split(weighted)
    dims = (((0,), (0,)), ((), ()))
    return lax.dot_general(high, values, dims, preferred_element_type=F32) + lax.dot_general(
        low, values, dims, preferred_element_type=F32
    )


def state_kernel(key_ref, value_ref, column_ref, out_ref):
    width = key_ref.shape[1]
    step = pl.program_id(0)

    @pl.when(step == 0)
    def _():
        out_ref[0:width, :] = jnp.zeros((width, width), F32)
        out_ref[width:, :] = jnp.zeros((EXTRA, width), F32)

    lanes = lax.broadcasted_iota(jnp.int32, key_ref.shape, 1)
    column = column_ref[...]
    end = column[BLOCK - 1 : BLOCK, :]
    end_lanes = per_head(end, lanes[0:1, :])
    fresh = gathered_update(key_ref[...], value_ref[...], column, lanes, end)
    out_ref[0:width, :] = out_ref[0:width, :] * jnp.exp(end_lanes) + fresh
    out_ref[width:, :] = out_ref[width:, :] + end_lanes


def retention_kernel(
    mine_ref, query_ref, key_ref, value_ref, gate_ref, column_ref, row_ref, gain_ref, states_ref,
    out_ref, state
):
    rows, width = query_ref.shape
    heads = width // HEAD
    step = pl.program_id(0)
    count = states_ref.shape[0]
    row_ids = lax.broadcasted_iota(jnp.int32, (width, width), 0) // HEAD
    column_ids = lax.broadcasted_iota(jnp.int32, (width, width), 1) // HEAD

    @pl.when(step == 0)
    def _():
        total = jnp.zeros((width, width), F32)
        for position in range(count - 1):
            decay = jnp.exp(states_ref[position, width : width + 1, :])
            longer = total * decay + states_ref[position, 0:width, :]
            total = jnp.where(position < mine_ref[0], longer, total)
        state[...] = jnp.where(row_ids == column_ids, total, 0.0)

    lanes = lax.broadcasted_iota(jnp.int32, (rows, width), 1)
    queries, keys, values = query_ref[...], key_ref[...], value_ref[...]
    column = column_ref[...]
    end = column[rows - 1 : rows, :]
    causal = lax.broadcasted_iota(jnp.int32, (rows, rows), 0) >= lax.broadcasted_iota(
        jnp.int32, (rows, rows), 1
    )
    scale = HEAD ** (-0.5)
    high, low = split(state[...])
    carried = jnp.dot(queries, high, preferred_element_type=F32) + jnp.dot(
        queries, low, preferred_element_type=F32
    )
    retained = carried * jnp.exp(per_head(column, lanes))
    inner = None
    for head in range(heads):
        own = jnp.where(lanes // HEAD == head, queries.astype(F32), 0.0).astype(BF16)
        scores = lax.dot_general(
            own, keys, (((1,), (1,)), ((), ())), preferred_element_type=F32
        )
        spread = column[:, head : head + 1] - row_ref[0, head : head + 1, :]
        damping = jnp.exp(jnp.where(causal, spread, -jnp.inf))
        factor = (scores * scale * damping).astype(BF16)
        term = jnp.dot(factor, values, preferred_element_type=F32)
        inner = term if inner is None else jnp.where(lanes // HEAD == head, term, inner)
    retained = retained + inner
    fresh = gathered_update(keys, values, column, lanes, end)
    end_lanes = per_head(end, lanes[0:1, :])
    state[...] = state[...] * jnp.exp(end_lanes) + jnp.where(row_ids == column_ids, fresh, 0.0)

    def head_mean(array):
        out = None
        for head in range(heads):
            inside = lanes // HEAD == head
            mean = jnp.sum(jnp.where(inside, array, 0.0), axis=1, keepdims=True) * (1.0 / HEAD)
            out = jnp.broadcast_to(mean, array.shape) if out is None else jnp.where(inside, mean, out)
        return out

    centered = retained - head_mean(retained)
    normed = centered * lax.rsqrt(head_mean(centered * centered) + eps)
    gates = gate_ref[...].astype(F32)
    out_ref[...] = (normed * gain_ref[...] * (gates * jax.nn.sigmoid(gates))).astype(BF16)


def retention(query_rows, key_rows, value_rows, gate_rows, log_decay, head_gain):
    rows, width = query_rows.shape
    heads = width // HEAD
    count = rows // BLOCK
    running = jnp.cumsum(log_decay.reshape(heads, count, BLOCK), axis=2)
    row = running.transpose(1, 0, 2)
    column = running.reshape(heads, rows).T
    block = pl.BlockSpec((BLOCK, width), lambda i: (i, 0))
    column_block = pl.BlockSpec((BLOCK, heads), lambda i: (i, 0))
    state_call = pl.pallas_call(
        state_kernel,
        grid=(count,),
        in_specs=[block, block, column_block],
        out_specs=pl.BlockSpec((width + EXTRA, width), lambda i: (0, 0)),
        out_shape=jax.ShapeDtypeStruct((width + EXTRA, width), F32),
        compiler_params=pltpu.CompilerParams(dimension_semantics=("arbitrary",)),
        cost_estimate=pl.CostEstimate(
            flops=4 * rows * width * width, bytes_accessed=4 * rows * width, transcendentals=rows * width
        ),
    )
    own = state_call(key_rows, value_rows, column)
    states = lax.all_gather(own, "sp")
    mine = lax.axis_index("sp").astype(jnp.int32).reshape(1)
    return pl.pallas_call(
        retention_kernel,
        grid=(count,),
        in_specs=[
            pl.BlockSpec(memory_space=pltpu.SMEM),
            block,
            block,
            block,
            block,
            column_block,
            pl.BlockSpec((1, heads, BLOCK), lambda i: (i, 0, 0)),
            pl.BlockSpec((1, width), lambda i: (0, 0)),
            pl.BlockSpec(states.shape, lambda i: (0, 0, 0)),
        ],
        out_specs=block,
        out_shape=jax.ShapeDtypeStruct((rows, width), BF16),
        scratch_shapes=[pltpu.VMEM((width, width), F32)],
        compiler_params=pltpu.CompilerParams(dimension_semantics=("arbitrary",)),
        cost_estimate=pl.CostEstimate(
            flops=8 * rows * width * BLOCK,
            bytes_accessed=10 * rows * width,
            transcendentals=rows * BLOCK * heads,
        ),
    )(mine, query_rows, key_rows, value_rows, gate_rows, column, row, head_gain[None, :], states)


def send(piece, pairs):
    return lax.ppermute(piece, "tp", pairs)


def ring_start(own):
    size = lax.axis_size("tp")
    right = [(i, (i + 2) % size) for i in range(size)]
    left = [(i, (i - 2) % size) for i in range(size)]
    swap = [(i, i ^ 1) for i in range(size)]
    return send(own, right), send(own, left), send(own, swap)


def ring_finish(own, from_left, from_right, other):
    size = lax.axis_size("tp")
    chips = size // 2
    right = [(i, (i + 2) % size) for i in range(size)]
    left = [(i, (i - 2) % size) for i in range(size)]
    swap = [(i, i ^ 1) for i in range(size)]
    half = own.shape[1] // 2
    last = chips // 2
    pieces = [[own], [other]]
    for hop in range(1, (chips - 1) // 2 + 1):
        if hop > 1:
            from_left = send(from_left, right)
            from_right = send(from_right, left)
        for piece in (from_left, from_right):
            pieces += [[piece], [send(piece, swap)]]
    if chips % 2 == 0 and last > 1:
        first = send(from_left[:, :half], right)
        second = send(from_right[:, half:], left)
        pieces += [[first, second], [send(first, swap), send(second, swap)]]
    elif chips == 2:
        pieces += [[from_left], [send(from_left, swap)]]
    return pieces


def expert_kernel(layout, row_ref, *refs):
    count = len(layout)
    piece_refs, out_ref = refs[:count], refs[count]
    weights, middle, sems = refs[count + 1 :]
    slots, _, width, ff = weights.shape
    rows = row_ref.shape[0]
    copies = []
    for index, (slot, start, length) in enumerate(layout):
        copy = pltpu.make_async_copy(
            piece_refs[index], weights.at[slot, :, pl.ds(start, length), :], sems.at[index]
        )
        copy.start()
        copies.append(copy)
    tile = rows // 2
    for pair in range(slots // 2):
        for index, (slot, _, _) in enumerate(layout):
            if slot // 2 == pair:
                copies[index].wait()

        @pl.loop(0, 2)
        def _(step):
            span = pl.ds(pl.multiple_of(step * tile, tile), tile)
            block = row_ref[span, :]
            gate = jnp.concatenate([weights[2 * pair, 0], weights[2 * pair + 1, 0]], axis=1)
            up = jnp.concatenate([weights[2 * pair, 1], weights[2 * pair + 1, 1]], axis=1)
            gated = jnp.dot(block, gate, preferred_element_type=F32)
            raised = jnp.dot(block, up, preferred_element_type=F32)
            value = gated * jax.nn.sigmoid(gated) * raised
            middle[span, 2 * pair * ff : 2 * (pair + 1) * ff] = value.astype(BF16)

    part = 512

    @pl.loop(0, width // part)
    def _(step):
        span = pl.ds(pl.multiple_of(step * part, part), part)
        down = jnp.concatenate([weights[slot, 2, span, :] for slot in range(slots)], axis=1)
        out_ref[:, span] = lax.dot_general(
            middle[...], down, (((1,), (1,)), ((), ())), preferred_element_type=F32
        ).astype(BF16)


def experts(rows, shards):
    _, width, ff = shards[0][0].shape
    count = len(shards)
    if ff % 128 or count % 2:
        whole = jnp.concatenate([jnp.concatenate(shard, axis=1) for shard in shards], axis=2)
        middle = (
            jax.nn.silu(jnp.dot(rows, whole[0], preferred_element_type=F32))
            * jnp.dot(rows, whole[1], preferred_element_type=F32)
        ).astype(BF16)
        return lax.dot_general(
            middle, whole[2], (((1,), (1,)), ((), ())), preferred_element_type=F32
        ).astype(BF16)
    layout, pieces = [], []
    for slot, shard in enumerate(shards):
        start = 0
        for piece in shard:
            layout.append((slot, start, piece.shape[1]))
            pieces.append(piece)
            start += piece.shape[1]
    return pl.pallas_call(
        functools.partial(expert_kernel, layout),
        in_specs=[pl.BlockSpec(memory_space=pltpu.VMEM)]
        + [pl.BlockSpec(memory_space=pl.ANY)] * len(pieces),
        out_specs=pl.BlockSpec(memory_space=pltpu.VMEM),
        out_shape=jax.ShapeDtypeStruct(rows.shape, BF16),
        scratch_shapes=[
            pltpu.VMEM((count, 3, width, ff), BF16),
            pltpu.VMEM((rows.shape[0], count * ff), BF16),
            pltpu.SemaphoreType.DMA((len(pieces),)),
        ],
        compiler_params=pltpu.CompilerParams(vmem_limit_bytes=60 * 1024 * 1024),
        cost_estimate=pl.CostEstimate(
            flops=6 * rows.shape[0] * width * count * ff,
            bytes_accessed=6 * width * count * ff + 4 * rows.size,
            transcendentals=rows.shape[0] * count * ff,
        ),
    )(rows, *pieces)


def on_device(
    query_rows,
    key_rows,
    value_rows,
    gate_rows,
    log_decay,
    residual,
    head_gain,
    out_weight,
    norm_gain,
    expert_ids,
    route_weights,
    expert_gate,
    expert_up,
    expert_down,
    shared_gate,
    shared_up,
    shared_down,
):
    part = out_weight.shape[0] // lax.axis_size("sp")
    own_part = lax.dynamic_slice_in_dim(out_weight, lax.axis_index("sp") * part, part, 0)
    out_part = lax.all_gather(own_part, "tp", axis=1, tiled=True)
    out_full = lax.all_gather(out_part, "sp", axis=0, tiled=True)
    shard = jnp.stack([expert_gate, expert_up, expert_down])
    shard, log_decay = lax.optimization_barrier((shard, log_decay))
    from_left, from_right, other = ring_start(shard)

    specialists = lax.axis_size("sp")
    tokens, chosen = expert_ids.shape
    width = residual.shape[1]
    capacity = 3 * tokens * chosen // (2 * specialists)
    names = jnp.arange(specialists, dtype=jnp.int32)[:, None]
    named = [expert_ids[:, j][None, :] == names for j in range(chosen)]
    match = functools.reduce(jnp.logical_or, named)
    weight = sum(jnp.where(named[j], route_weights[:, j][None, :], 0.0) for j in range(chosen))
    earlier = jnp.arange(tokens)[:, None] < jnp.arange(tokens)[None, :]
    position = jnp.dot(match.astype(BF16), earlier.astype(BF16), preferred_element_type=F32)
    place = jnp.where(match, position.astype(jnp.int32), -1)
    sits = place[:, None, :] == jnp.arange(capacity, dtype=jnp.int32)[None, :, None]
    pick = sits.astype(BF16).reshape(specialists * capacity, tokens)
    weight_high = lax.reduce_precision(weight, 8, 7)
    weight_low = weight - weight_high
    back_high = jnp.where(sits, weight_high[:, None, :], 0.0).astype(BF16)
    back_low = jnp.where(sits, weight_low[:, None, :], 0.0).astype(BF16)

    ret_rows = retention(query_rows, key_rows, value_rows, gate_rows, log_decay, head_gain)
    token_rows = lax.all_to_all(ret_rows, "tp", split_axis=0, concat_axis=1, tiled=True)
    token_rows, from_left, from_right = lax.optimization_barrier((token_rows, from_left, from_right))
    shards = ring_finish(shard, from_left, from_right, other)
    mixer = jnp.dot(token_rows, out_full, preferred_element_type=F32)
    hidden = (residual.astype(F32) + mixer).astype(BF16)
    hidden_wide = hidden.astype(F32)
    normed_rows = (
        hidden_wide
        * lax.rsqrt(jnp.mean(hidden_wide * hidden_wide, axis=1, keepdims=True) + eps)
        * norm_gain
    ).astype(BF16)
    outgoing = jnp.dot(pick, normed_rows, preferred_element_type=F32).astype(BF16)
    outgoing = outgoing.reshape(specialists, capacity, width)
    arrived = lax.all_to_all(outgoing, "sp", split_axis=0, concat_axis=0, tiled=True)
    shared_mid = (
        jax.nn.silu(jnp.dot(normed_rows, shared_gate, preferred_element_type=F32))
        * jnp.dot(normed_rows, shared_up, preferred_element_type=F32)
    ).astype(BF16)
    shared_out = lax.dot_general(
        shared_mid, shared_down, (((1,), (1,)), ((), ())), preferred_element_type=F32
    )
    flat_rows = arrived.reshape(-1, width)
    processed = experts(flat_rows, shards).reshape(arrived.shape)
    returned = lax.all_to_all(processed, "sp", split_axis=0, concat_axis=0, tiled=True)
    dims = (((0, 1), (0, 1)), ((), ()))
    routed = lax.dot_general(back_high, returned, dims, preferred_element_type=F32)
    routed += lax.dot_general(back_low, returned, dims, preferred_element_type=F32)
    return (hidden_wide + routed + shared_out).astype(BF16)


MESH = pl.DeviceIdType.MESH
NT = (((1,), (1,)), ((), ()))
TN = (((0,), (0,)), ((), ()))


def thirds(value):
    first = value.astype(BF16)
    rest = value - first.astype(F32)
    second = rest.astype(BF16)
    return first, second, (rest - second.astype(F32)).astype(BF16)


def piece_widths(depth):
    return [128] + [256] * ((depth - 256) // 256) + [128]


STRAIGHT = 1


def layer_kernel(
    query_hbm, key_hbm, value_hbm, gate_hbm, decay_hbm, residual_hbm, head_gain_hbm, out_weight_hbm,
    norm_gain_hbm, ids_hbm, route_hbm, expert_gate_hbm, expert_up_hbm, expert_down_hbm,
    shared_gate_hbm, shared_up_hbm, shared_down_hbm,
    result_ref,
    decay_ref, head_gain_ref, norm_gain_ref, ids_ref, route_ref,
    query, key, value, gates, residual, shared_gate, shared_up, shared_down,
    weights, out_full, running, row_running, updates, states, state, inner, ret_rows, token_rows,
    hidden, normed, squares, tables, outgoing, arrived, middle, processed, direct, passing, merged,
    combined, final, base, shared_middle, back, shares,
    local_sem, state_send, state_recv, mix_send, mix_recv, out_z_send, out_xy_send, out_z_recv, out_xy_recv,
    out_pair_send, out_pair_recv, right_send, left_send, pair_send, line_recv, pair_recv, pair_down_recv,
    go_send, go_recv, table_send, table_recv, direct_send, home_recv, passing_send, passing_recv,
    merged_send, final_send, final_recv, hello,
):
    places_count = states.shape[0]
    size = token_rows.shape[0]
    chips = size // 2
    sp = lax.axis_index("sp")
    tp = lax.axis_index("tp")
    z, core = tp // 2, tp % 2
    blocks, rows, width = ret_rows.shape
    heads = width // HEAD
    depth = residual.shape[1]
    capacity = arrived.shape[1]
    specialists = arrived.shape[0]
    ff = weights.shape[3]
    quarter = out_full.shape[1] // places_count
    out_columns = out_full.shape[2]
    widths = piece_widths(depth)
    pieces = len(widths)
    starts = [sum(widths[:index]) for index in range(pieces)]
    half = depth // 2
    tile = processed.shape[3]
    scale = HEAD ** (-0.5)
    inputs = (expert_gate_hbm, expert_up_hbm, expert_down_hbm)
    units = [(which, start, half) for which in (0, 1) for start in (0, half)]
    first_down = len(units)
    units += [(2, start, length) for start, length in zip(starts, widths)]

    def remote(src, dst, send, recv, device):
        return pltpu.make_async_remote_copy(
            src_ref=src, dst_ref=dst, send_sem=send, recv_sem=recv, device_id=device, device_id_type=MESH
        )

    partner = (sp, z * 2 + 1 - core)
    right = (sp, tp + 2)
    left = (sp, tp - 2)

    local = [
        pltpu.make_async_copy(src, dst, local_sem.at[index])
        for index, (src, dst) in enumerate(
            [
                (decay_hbm, decay_ref),
                (ids_hbm, ids_ref),
                (route_hbm, route_ref),
                (key_hbm, key),
                (value_hbm, value),
                (query_hbm, query),
                (gate_hbm, gates),
                (head_gain_hbm, head_gain_ref),
                (norm_gain_hbm, norm_gain_ref),
                (out_weight_hbm, out_full.at[tp]),
                (residual_hbm, residual),
                (shared_gate_hbm, shared_gate),
                (shared_up_hbm, shared_up),
                (shared_down_hbm, shared_down),
                (expert_gate_hbm, weights.at[tp, 0]),
                (expert_up_hbm, weights.at[tp, 1]),
                (expert_down_hbm, weights.at[tp, 2]),
            ]
        )
    ]
    barrier = pltpu.get_barrier_semaphore()

    def greet(flag):
        for step in (1, 2):
            pl.semaphore_signal(flag, inc=1, device_id=(sp ^ step, tp), device_id_type=MESH)
        pl.semaphore_signal(flag, inc=1, device_id=partner, device_id_type=MESH)

        @pl.when(z < chips - 1)
        def _():
            pl.semaphore_signal(flag, inc=1, device_id=right, device_id_type=MESH)

        @pl.when(z > 0)
        def _():
            pl.semaphore_signal(flag, inc=1, device_id=left, device_id_type=MESH)

    def greeted(flag):
        pl.semaphore_wait(flag, jnp.where(jnp.logical_or(z == 0, z == chips - 1), 4, 5))

    greet(barrier)
    for copy in local[:9]:
        copy.start()
    greeted(barrier)
    greet(hello.at[0])

    def weight_copy(origin, unit, send, device, own=False, pair=False):
        rightward = device is right
        which, start, length = units[unit]
        span = pl.ds(start, length)
        there = weights.at[origin * 2 + core, which, span, :]
        here = inputs[which].at[span, :] if own else there
        if not pair:
            received = line_recv.at[origin if rightward else origin - 1, unit]
        elif unit < first_down:
            received = pair_recv.at[origin]
        else:
            received = pair_down_recv.at[unit - first_down]
        return remote(here, there, send, received, device)

    def to_partner(origin, unit, own=False):
        return weight_copy(origin, unit, pair_send, partner, own, True)

    def own_send(unit):
        @pl.when(z < chips - 1)
        def _():
            weight_copy(z, unit, right_send, right, True).start()

        @pl.when(z > 0)
        def _():
            weight_copy(z, unit, left_send, left, True).start()

        to_partner(z, unit, True).start()

    def relay(unit, distance):
        @pl.when(z - distance >= 0)
        def _():
            origin = z - distance
            copy = weight_copy(origin, unit, right_send, right)
            copy.wait_recv()

            @pl.when(z < chips - 1)
            def _():
                copy.start()

            to_partner(origin, unit).start()

        @pl.when(z + distance < chips)
        def _():
            origin = z + distance
            copy = weight_copy(origin, unit, left_send, left)
            copy.wait_recv()

            @pl.when(z > 0)
            def _():
                copy.start()

            to_partner(origin, unit).start()

    def from_partner(origin):
        there = weights.at[0, 0:2]
        remote(there, there, pair_send, pair_recv.at[origin], partner).wait_recv()

    def downs_from_partner(index):
        there = weights.at[0, 2, pl.ds(0, chips * widths[index]), :]
        remote(there, there, pair_send, pair_down_recv.at[index], partner).wait_recv()

    def out_z(step):
        target = (z + step) % chips
        span = pl.ds(pl.multiple_of(sp * quarter, quarter), quarter)
        return remote(
            out_weight_hbm.at[span, :], out_full.at[tp, span, :], out_z_send, out_z_recv.at[z],
            (sp, target * 2 + core),
        )

    def out_z_arrival(step):
        origin = (z + step) % chips
        there = out_full.at[0, pl.ds(0, quarter), :]
        return remote(there, there, out_z_send, out_z_recv.at[origin], partner)

    def out_piece(step, device):
        origin = (z + step) % chips
        span = pl.ds(pl.multiple_of(sp * quarter, quarter), quarter)
        there = out_full.at[origin * 2 + core, span, :]
        return remote(there, there, out_xy_send.at[step - 1], out_xy_recv.at[origin], device)

    def out_pieces(step):
        origin = (z + step) % chips
        there = out_full.at[0, pl.ds(0, (places_count - 1) * quarter), :]
        return remote(there, there, out_xy_send.at[step - 1], out_xy_recv.at[origin], partner)

    def out_pair(slot, own=False):
        return remote(
            out_weight_hbm if own else out_full.at[slot], out_full.at[slot], out_pair_send,
            out_pair_recv, partner,
        )

    def out_pairs():
        there = out_full.at[0:chips]
        return remote(there, there, out_pair_send, out_pair_recv, partner)

    @pl.when(z < chips - 1)
    def _():
        out_z(1).start()

    @pl.when(z > 0)
    def _():
        out_z(chips - 1).start()

    own_send(0)
    out_pair(tp, True).start()
    for copy in local[9:]:
        copy.start()

    for copy in local[:3]:
        copy.wait()

    row_ids = lax.broadcasted_iota(jnp.int32, (width, width), 0) // HEAD
    column_ids = lax.broadcasted_iota(jnp.int32, (width, width), 1) // HEAD
    same_head = row_ids == column_ids
    lanes = lax.broadcasted_iota(jnp.int32, (rows, width), 1)
    later = lax.broadcasted_iota(jnp.int32, (rows, rows), 0)
    sooner = lax.broadcasted_iota(jnp.int32, (rows, rows), 1)
    lower = jnp.where(later >= sooner, 1.0, 0.0).astype(BF16)
    upper = jnp.where(later <= sooner, 1.0, 0.0).astype(BF16)

    chosen, tokens = ids_ref.shape
    names = lax.broadcasted_iota(jnp.int32, (8, tokens), 0)
    match = names < 0
    weight = jnp.zeros((8, tokens), F32)
    for j in range(chosen):
        named = ids_ref[j : j + 1, :] == names
        match = jnp.logical_or(match, named)
        weight = weight + jnp.where(named, route_ref[j : j + 1, :], 0.0)
    strict = jnp.where(later < sooner, 1.0, 0.0).astype(BF16)
    position = jnp.dot(jnp.where(match, 1.0, 0.0).astype(BF16), strict, preferred_element_type=F32)
    tables[0, 0:8, :] = jnp.where(match, position, -1.0)
    tables[0, 8:16, :] = weight

    def table_copy(step):
        return remote(
            tables.at[0], tables.at[step], table_send, table_recv.at[step - 1], (sp ^ step, tp)
        )

    greeted(hello.at[0])
    greet(hello.at[1])
    listed = jnp.concatenate(
        [
            decay_ref[head : head + 1, block * rows : (block + 1) * rows]
            for head in range(heads)
            for block in range(blocks)
        ],
        axis=0,
    )
    row_running[...] = functools.reduce(
        jnp.add, [jnp.dot(part, upper, preferred_element_type=F32) for part in thirds(listed)]
    )
    head_rows = lax.broadcasted_iota(jnp.int32, (width, rows), 0) // HEAD
    for block in range(blocks):
        spread = jnp.broadcast_to(listed[block : block + 1, :], (width, rows))
        for head in range(1, heads):
            spread = jnp.where(
                head_rows == head, listed[head * blocks + block : head * blocks + block + 1, :], spread
            )
        running[block] = functools.reduce(
            jnp.add,
            [
                lax.dot_general(lower, part, NT, preferred_element_type=F32)
                for part in thirds(spread)
            ],
        )

    greeted(hello.at[1])
    greet(hello.at[2])

    @pl.when(z == chips - 1)
    def _():
        out_z(1).start()

    for step in range(2, chips - 1):
        out_z(step).start()

    @pl.when(z == 0)
    def _():
        out_z(chips - 1).start()

    own_send(1)
    for copy in local[3:5]:
        copy.wait()
    state[...] = jnp.zeros((width + EXTRA, width), F32)

    @pl.loop(0, blocks)
    def _(block):
        span = pl.ds(pl.multiple_of(block * rows, rows), rows)
        column = running[block]
        end = column[rows - 1 : rows, :]
        weighted = key[span, :].astype(F32) * (jnp.exp(end - column) * scale)
        high, low = split(weighted)
        fresh = lax.dot_general(high, value[span, :], TN, preferred_element_type=F32)
        fresh += lax.dot_general(low, value[span, :], TN, preferred_element_type=F32)
        fresh = jnp.where(same_head, fresh, 0.0)
        updates[block] = fresh
        state[0:width, :] = state[0:width, :] * jnp.exp(end) + fresh
        state[width:, :] = state[width:, :] + end

    greeted(hello.at[2])
    states[sp] = state[...]

    def state_copy(step):
        return remote(
            state, states.at[sp], state_send, state_recv.at[sp], (sp ^ step, tp)
        )

    def state_arrival(step):
        return remote(
            state, states.at[sp ^ step], state_send, state_recv.at[sp ^ step], (sp ^ step, tp)
        )

    local[5].wait()
    for step in range(1, places_count):
        state_copy(step).start()
    for step in (1, 2):
        table_copy(step).start()

    @pl.loop(0, blocks)
    def _(block):
        span = pl.ds(pl.multiple_of(block * rows, rows), rows)
        queries, keys, values = query[span, :], key[span, :], value[span, :]
        column = running[block]
        causal = later >= sooner
        total = None
        for head in range(heads):
            own = jnp.where(lanes // HEAD == head, queries.astype(F32), 0.0).astype(BF16)
            scores = lax.dot_general(own, keys, NT, preferred_element_type=F32)
            spread = column[:, head * HEAD : head * HEAD + 1] - row_running[pl.ds(head * blocks + block, 1), :]
            damping = jnp.exp(jnp.where(causal, spread, -jnp.inf))
            factor = (scores * scale * damping).astype(BF16)
            term = jnp.dot(factor, values, preferred_element_type=F32)
            total = term if total is None else jnp.where(lanes // HEAD == head, term, total)
        inner[block] = total

    for step in range(1, places_count):
        state_arrival(step).wait_recv()
    there = states.at[pl.ds(0, places_count - 1)]
    remote(there, there, state_send, state_recv.at[0], partner).wait_send()
    total = jnp.zeros((width, width), F32)
    for position in range(places_count - 1):
        longer = total * jnp.exp(states[position, width : width + 1, :]) + states[position, 0:width, :]
        total = jnp.where(position < sp, longer, total)
    state[0:width, :] = total
    local[6].wait()
    local[7].wait()

    def head_mean(array):
        out = None
        for head in range(heads):
            inside = lanes // HEAD == head
            mean = jnp.sum(jnp.where(inside, array, 0.0), axis=1, keepdims=True) * (1.0 / HEAD)
            out = jnp.broadcast_to(mean, array.shape) if out is None else jnp.where(inside, mean, out)
        return out

    def mix_copy(block):
        return remote(
            ret_rows.at[block], token_rows.at[tp], mix_send, mix_recv, (sp, block)
        )

    def mix_start(block):
        @pl.when(block != tp)
        def _():
            mix_copy(block).start()

    @pl.loop(0, blocks)
    def _(block):
        span = pl.ds(pl.multiple_of(block * rows, rows), rows)
        column = running[block]
        end = column[rows - 1 : rows, :]
        before = state[0:width, :]
        high, low = split(before)
        queries = query[span, :]
        carried = jnp.dot(queries, high, preferred_element_type=F32) + jnp.dot(
            queries, low, preferred_element_type=F32
        )
        state[0:width, :] = before * jnp.exp(end) + updates[block]
        retained = carried * jnp.exp(column) + inner[block]
        centered = retained - head_mean(retained)
        norm = centered * lax.rsqrt(head_mean(centered * centered) + eps)
        gate = gates[span, :].astype(F32)
        mixed = (norm * head_gain_ref[...] * (gate * jax.nn.sigmoid(gate))).astype(BF16)
        ret_rows[block] = mixed

        @pl.when(block == tp)
        def _():
            token_rows[tp] = mixed

        @pl.when(block > 0)
        def _():
            mix_start(block - 1)

    mix_start(blocks - 1)

    between = jnp.logical_and(z > 0, z < chips - 1)

    @pl.when(jnp.logical_not(between))
    def _():
        for unit in range(2, len(units)):
            own_send(unit)

    for step in range(1, chips):
        out_z_arrival(step).wait_recv()
        for other in range(1, places_count):
            out_piece(step, (sp ^ other, tp)).start()

    @pl.when(jnp.logical_not(between))
    def _():
        relay(0, 1)
        relay(1, 1)

    @pl.when(between)
    def _():
        relay(0, 1)
        own_send(2)
        relay(1, 1)
        own_send(3)

    def pass_on(unit, distance, rightward):
        origin = z - distance if rightward else z + distance
        sent, device = (right_send, right) if rightward else (left_send, left)
        copy = weight_copy(origin, unit, sent, device)
        copy.wait_recv()
        copy.start()
        to_partner(origin, unit).start()

    def inward(unit):
        for chip, rightward in ((1, True), (chips - 2, False)):

            @pl.when(z == chip)
            def _():
                sent, device = (right_send, right) if rightward else (left_send, left)
                weight_copy(z, unit, sent, device, True).start()
                to_partner(z, unit, True).start()
                pass_on(unit, 1, rightward)

    def outward(unit):
        for chip, rightward in ((1, False), (chips - 2, True)):

            @pl.when(z == chip)
            def _():
                sent, device = (right_send, right) if rightward else (left_send, left)
                weight_copy(z, unit, sent, device, True).start()
                for distance in (1, 2):
                    pass_on(unit, distance, rightward)


    slot_rows = lax.broadcasted_iota(jnp.int32, (capacity, tokens), 0).astype(F32)
    for step in (1, 2):
        table_copy(step).wait_recv()
    for turn, (table, pair) in enumerate(
        ((0, (0, 2)), (0, (0, 1)), (1, (0, 2)), (2, (0, 1)), (0, (2, 3)))
    ):
        for side, other in enumerate(pair):
            name = sp ^ other
            place = tables[table, pl.ds(name, 1), :]
            back[turn, side] = jnp.where(place == slot_rows, 1.0, 0.0).T.astype(BF16)
            share = tables[table, pl.ds(8 + name, 1), :]
            shares[turn, side] = jnp.broadcast_to(share, (tile, tokens)).T

    for copy in local[8:11]:
        copy.wait()
    for step in range(1, chips):
        out_pieces(step).wait_recv()
        out_pair(((z + step) % chips) * 2 + core).start()
    out_pairs().wait_recv()
    there = token_rows.at[pl.ds(0, size - 1)]
    remote(there, there, mix_send, mix_recv, partner).wait_recv()

    squares[...] = jnp.zeros(squares.shape, F32)

    @pl.loop(0, size)
    def _(slot):
        span = pl.ds(pl.multiple_of(slot * out_columns, out_columns), out_columns)
        token = jnp.concatenate([token_rows[index] for index in range(size)], axis=1)
        mixer = jnp.dot(token, out_full[slot], preferred_element_type=F32)
        total = (residual[:, span].astype(F32) + mixer).astype(BF16)
        hidden[:, span] = total
        wide = total.astype(F32)
        wide = wide * wide
        squares[...] += functools.reduce(
            jnp.add, [wide[:, start : start + 128] for start in range(0, out_columns, 128)]
        )

    factor = lax.rsqrt(jnp.sum(squares[...], axis=1, keepdims=True) * (1.0 / depth) + eps)

    @pl.loop(0, depth // 256)
    def _(index):
        span = pl.ds(pl.multiple_of(index * 256, 256), 256)
        normed[:, span] = (hidden[:, span].astype(F32) * factor * norm_gain_ref[:, span]).astype(BF16)

    relay(0, 2)

    def go(step):
        return remote(
            outgoing.at[step - 1], arrived.at[sp], go_send, go_recv.at[sp], (sp ^ step, tp)
        )

    for step in list(range(places_count - 1, -1, -1)):
        sits = jnp.where(tables[0, pl.ds(sp ^ step, 1), :] == slot_rows, 1.0, 0.0).astype(BF16)

        @pl.loop(0, depth // 512)
        def _(index):
            span = pl.ds(pl.multiple_of(index * 512, 512), 512)
            picked = jnp.dot(sits, normed[:, span], preferred_element_type=F32).astype(BF16)
            if step:
                outgoing[step - 1, :, span] = picked
            else:
                arrived[sp, :, span] = picked

        if step:
            go(step).start()

    relay(1, 2)
    relay(2, 1)

    for copy in local[11:14]:
        copy.wait()
    shared = shared_gate.shape[1]

    @pl.loop(0, shared // 256)
    def _(index):
        span = pl.ds(pl.multiple_of(index * 256, 256), 256)
        gated = jnp.dot(normed[...], shared_gate[:, span], preferred_element_type=F32)
        raised = jnp.dot(normed[...], shared_up[:, span], preferred_element_type=F32)
        shared_middle[:, span] = (gated * jax.nn.sigmoid(gated) * raised).astype(BF16)

    @pl.loop(0, depth // 512)
    def _(index):
        span = pl.ds(pl.multiple_of(index * 512, 512), 512)
        base[:, span] = hidden[:, span].astype(F32) + lax.dot_general(
            shared_middle[...], shared_down[span, :], NT, preferred_element_type=F32
        )

    relay(0, 3)
    relay(3, 1)
    relay(2, 2)
    relay(1, 3)
    relay(3, 2)
    inward(first_down)
    inward(first_down + 1)

    for copy in local[14:]:
        copy.wait()
    for step in range(1, places_count):
        remote(
            outgoing.at[0], arrived.at[sp ^ step], go_send, go_recv.at[sp ^ step], (sp ^ step, tp)
        ).wait_recv()

    outward(first_down)
    inward(first_down + 2)

    def pair_middle(chip):
        @pl.loop(0, specialists // 2)
        def _(index):
            rows_here = jnp.concatenate([arrived[2 * index], arrived[2 * index + 1]], axis=0)
            gate_pair = jnp.concatenate([weights[2 * chip, 0], weights[2 * chip + 1, 0]], axis=1)
            up_pair = jnp.concatenate([weights[2 * chip, 1], weights[2 * chip + 1, 1]], axis=1)
            gated = jnp.dot(rows_here, gate_pair, preferred_element_type=F32)
            raised = jnp.dot(rows_here, up_pair, preferred_element_type=F32)
            found = (gated * jax.nn.sigmoid(gated) * raised).astype(BF16)
            span = pl.ds(pl.multiple_of(index * 2 * capacity, 2 * capacity), 2 * capacity)
            middle[span, pl.ds(pl.multiple_of(chip * 2 * ff, 2 * ff), 2 * ff)] = found

    last_chip = jnp.where(z * 2 < chips, chips - 1, 0)

    def chip_at(index):
        if index == 0:
            return z
        if index == chips - 1:
            return last_chip
        toward = jnp.where(last_chip == 0, chips - 1 - index, index)
        shifted = jnp.where(last_chip == 0, chips - index, index - 1)
        passed = jnp.where(last_chip == 0, z <= chips - 1 - index, z >= index)
        return jnp.where(passed, shifted, toward)

    for index in range(chips):
        chip = chip_at(index)
        if index == chips - 1:
            relay(2, 3)
            relay(3, 3)
        from_partner(chip)
        pair_middle(chip)

    def tiles(index):
        return range(starts[index] // tile, (starts[index] + widths[index]) // tile)

    bent_tiles = depth // tile - STRAIGHT

    def bent(index):
        return [number for number in tiles(index) if number < bent_tiles]

    def straight(index):
        return [number for number in tiles(index) if number >= bent_tiles]

    def piece_of(number):
        return next(index for index in range(pieces) if number in tiles(index))

    def arrivals(buffer, send, received, index):
        there = buffer.at[pl.ds(starts[index] // tile, len(bent(index)))]
        remote(there, there, send, received.at[index], partner).wait_recv()

    def near(number):
        return sp ^ (2, 1)[number % 2]

    def far(number):
        return sp ^ (1, 2)[number % 2]

    def direct_copy(number):
        return remote(
            processed.at[number, near(number)], direct.at[number], direct_send,
            home_recv.at[piece_of(number)], (near(number), tp),
        )

    def passing_copy(number):
        return remote(
            processed.at[number, sp ^ 3], passing.at[number], passing_send,
            passing_recv.at[piece_of(number)], (near(number), tp),
        )

    def merged_copy(number):
        return remote(
            merged.at[number], combined.at[number], merged_send,
            home_recv.at[piece_of(number)], (far(number), tp),
        )

    def weighted(turn, first, second):
        first = jnp.dot(back[turn, 0], first, preferred_element_type=F32) * shares[turn, 0]
        return first + jnp.dot(back[turn, 1], second, preferred_element_type=F32) * shares[turn, 1]

    def merge(index):
        arrivals(passing, passing_send, passing_recv, index)
        for number in bent(index):
            found = weighted(2 + number % 2, processed[number, far(number)], passing[number])
            merged[number] = found.astype(BF16)
        for number in bent(index):
            merged_copy(number).start()

    last_tile = depth // tile - 1

    def final_copy(number, step):
        turn = number - bent_tiles
        return remote(
            processed.at[number, sp ^ step], final.at[turn, step - 1], final_send, final_recv.at[turn],
            (sp ^ step, tp),
        )

    def final_combine(number):
        turn = number - bent_tiles
        there = final.at[turn]
        remote(there, there, final_send, final_recv.at[turn], partner).wait_recv()
        routed = weighted(1, processed[number, sp], final[turn, 0])
        store(number, routed + weighted(4, final[turn, 1], final[turn, 2]))

    def store(number, routed):
        span = slice(number * tile, (number + 1) * tile)
        result_ref[:, span] = (base[:, span] + routed).astype(BF16)

    def combine(index):
        count = len(bent(index))
        there = weights.at[0, 0, pl.ds(0, count * (capacity + tokens)), :]
        remote(there, there, direct_send, home_recv.at[index], partner).wait_recv()
        for number in bent(index):
            routed = weighted(number % 2, processed[number, sp], direct[number])
            store(number, routed + combined[number].astype(F32))

    lag = 3

    outward(first_down + 1)
    inward(first_down + 3)
    for index in range(pieces):
        unit = first_down + index

        if index + 2 < pieces:
            outward(unit + 2)
        if index + 4 < pieces:
            inward(unit + 4)

        @pl.when(jnp.logical_not(between))
        def _():
            for distance in range(1, chips):
                relay(unit, distance)

        downs_from_partner(index)
        down = jnp.concatenate(
            [weights[slot, 2, starts[index] : starts[index] + widths[index], :] for slot in range(size)], axis=1
        )

        if index == pieces - 1:
            for step in range(places_count - 1, -1, -1):
                span = pl.ds(pl.multiple_of((sp ^ step) * capacity, capacity), capacity)
                found = lax.dot_general(middle[span, :], down, NT, preferred_element_type=F32)
                processed[last_tile, sp ^ step] = found.astype(BF16)
                if step:
                    final_copy(last_tile, step).start()
            merge(index - 1)
            continue
        found = lax.dot_general(middle[...], down, NT, preferred_element_type=F32).astype(BF16)
        for part, number in enumerate(tiles(index)):
            for source in range(specialists):
                processed[number, source] = found[
                    source * capacity : (source + 1) * capacity, part * tile : (part + 1) * tile
                ]

        for number in straight(index):
            final_copy(number, 3).start()
        for number in bent(index):
            passing_copy(number).start()
        for number in bent(index):
            direct_copy(number).start()
        for number in straight(index):
            final_copy(number, 2).start()
            final_copy(number, 1).start()
        if index:
            merge(index - 1)
        if index >= lag:
            combine(index - lag)

    for index in range(pieces - 1 - lag, pieces - 2):
        combine(index)
    for number in range(bent_tiles, last_tile):
        final_combine(number)
    combine(pieces - 2)
    final_combine(last_tile)

    there = out_full.at[0, pl.ds(0, (chips - 1) * quarter), :]
    remote(there, there, out_z_send, out_z_recv.at[0], partner).wait_send()
    for step in range(1, chips):
        out_pieces(step).wait_send()
    out_pairs().wait_send()
    there = ret_rows.at[pl.ds(0, blocks - 1)]
    remote(there, there, mix_send, mix_recv, partner).wait_send()
    remote(outgoing, outgoing, go_send, go_recv.at[0], partner).wait_send()
    for buffer, sent in ((direct, direct_send), (passing, passing_send), (merged, merged_send)):
        there = buffer.at[pl.ds(0, bent_tiles)]
        remote(there, there, sent, passing_recv.at[0], partner).wait_send()
    remote(final, final, final_send, final_recv.at[0], partner).wait_send()
    there = tables.at[0:2]
    remote(there, there, table_send, table_recv.at[0], partner).wait_send()
    for chip in range(chips):

        @pl.when(z == chip)
        def _():
            if chip < chips - 1:
                there = weights.at[0 : chip + 1]
                remote(there, there, right_send, line_recv.at[0, 0], right).wait_send()
            if chip > 0:
                there = weights.at[0 : chips - chip]
                remote(there, there, left_send, line_recv.at[0, 0], left).wait_send()

    there = weights.at[0:chips]
    remote(there, there, pair_send, line_recv.at[0, 0], partner).wait_send()


def whole_layer(*arrays):
    (query, _, _, _, _, residual, head_gain, out_weight, norm_gain, ids, _, expert_gate) = arrays[:12]
    shared_gate = arrays[14]
    places_count, size = lax.axis_size("sp"), lax.axis_size("tp")
    rows_all, width = query.shape
    tokens, depth = residual.shape
    blocks = rows_all // tokens
    chosen = ids.shape[1]
    capacity = 3 * tokens * chosen // (2 * places_count)
    ff = expert_gate.shape[1]
    shared = shared_gate.shape[1]
    chips = size // 2
    pieces = len(piece_widths(depth))
    units = 4 + pieces
    heads = width // HEAD
    dma = pltpu.SemaphoreType.DMA
    arrays = list(arrays)
    arrays[6] = head_gain[None, :]
    arrays[8] = norm_gain[None, :]
    arrays[9], arrays[10] = arrays[9].T, arrays[10].T
    vmem, anywhere = pl.BlockSpec(memory_space=pltpu.VMEM), pl.BlockSpec(memory_space=pl.ANY)
    block = lambda *shape: pltpu.VMEM(shape, BF16)
    wide = lambda *shape: pltpu.VMEM(shape, F32)
    return pl.pallas_call(
        layer_kernel,
        in_specs=[anywhere] * len(arrays),
        out_specs=vmem,
        out_shape=pltpu.VMEM((tokens, depth), BF16),
        scratch_shapes=[
            wide(*arrays[4].shape), wide(1, width), wide(1, depth),
            pltpu.VMEM(arrays[9].shape, jnp.int32), wide(*arrays[10].shape),
            block(rows_all, width), block(rows_all, width), block(rows_all, width), block(rows_all, width),
            block(tokens, depth), block(depth, shared), block(depth, shared), block(depth, shared),
            block(size, 3, depth, ff),
            block(size, out_weight.shape[0], out_weight.shape[1]),
            wide(blocks, tokens, width),
            wide(heads * blocks, tokens),
            wide(blocks, width, width),
            wide(places_count, width + EXTRA, width),
            wide(width + EXTRA, width),
            wide(blocks, tokens, width),
            block(blocks, tokens, width),
            block(size, tokens, width),
            block(tokens, depth), block(tokens, depth),
            wide(tokens, 128),
            wide(3, 16, tokens),
            block(places_count - 1, capacity, depth),
            block(places_count, capacity, depth),
            block(places_count * capacity, size * ff),
            block(depth // 128, places_count, capacity, 128),
            block(depth // 128, capacity, 128), block(depth // 128, capacity, 128),
            block(depth // 128, tokens, 128), block(depth // 128, tokens, 128),
            block(STRAIGHT, places_count - 1, capacity, 128),
            wide(tokens, depth),
            block(tokens, shared),
            block(5, 2, tokens, capacity), wide(5, 2, tokens, 128),
            dma((17,)),
            dma, dma((places_count,)),
            dma, dma,
            dma, dma((chips - 1,)), dma((chips,)), dma((chips,)),
            dma, dma,
            dma, dma, dma, dma((chips - 1, units)), dma((chips,)), dma((pieces,)),
            dma, dma((places_count,)),
            dma, dma((2,)),
            dma, dma((pieces,)), dma, dma((pieces,)), dma, dma, dma((STRAIGHT,)),
            pltpu.SemaphoreType.REGULAR((3,)),
        ],
        compiler_params=pltpu.CompilerParams(
            collective_id=0, has_side_effects=True, vmem_limit_bytes=58 * 1000 * 1000
        ),
        cost_estimate=pl.CostEstimate(
            flops=20 * 10**9, bytes_accessed=40 * 10**6, transcendentals=4 * 10**6
        ),
    )(*arrays)


def kernel_fits(mesh, shapes):
    places_count, size = mesh.shape["sp"], mesh.shape["tp"]
    if places_count != 4 or size != 8:
        return False
    width = shapes[0][1] // size
    tokens = shapes[5][0] // (places_count * size)
    rows_all = shapes[0][0] // places_count
    ff = shapes[11][1] // (places_count * size)
    return width == 128 and ff % 128 == 0 and tokens % 128 == 0 and rows_all == tokens * size


def solution(mesh):
    placed = (
        P("sp", "tp"),
        P("sp", "tp"),
        P("sp", "tp"),
        P("sp", "tp"),
        P("tp", "sp"),
        P(("sp", "tp"), None),
        P("tp"),
        P(None, "tp"),
        P(),
        P(("sp", "tp"), None),
        P(("sp", "tp"), None),
        P(None, ("sp", "tp")),
        P(None, ("sp", "tp")),
        P(None, ("sp", "tp")),
        P(),
        P(),
        P(),
    )

    placement = dict(mesh=mesh, in_specs=placed, out_specs=P(("sp", "tp"), None), check_vma=False)
    step = jax.shard_map(on_device, **placement)
    fused = jax.shard_map(whole_layer, **placement)

    def run(*arrays):
        fits = kernel_fits(mesh, [array.shape for array in arrays])
        return fused(*arrays) if fits else step(*arrays)

    return run
```

```python
import functools

import jax
import jax.numpy as jnp
from jax import lax
from jax.experimental import pallas as pl
from jax.experimental.pallas import tpu as pltpu
from jax.sharding import PartitionSpec as P


HEAD = 64
BLOCK = 256
EXTRA = 8


eps = 1e-05
F32 = jnp.float32
BF16 = jnp.bfloat16


def split(value):
    high = value.astype(BF16)
    return high, (value - high.astype(F32)).astype(BF16)


def per_head(columns, lanes):
    heads = columns.shape[1]
    out = jnp.broadcast_to(columns[:, 0:1], lanes.shape)
    for head in range(1, heads):
        out = jnp.where(lanes // HEAD == head, columns[:, head : head + 1], out)
    return out


def gathered_update(keys, values, column, lanes, end):
    scale = HEAD ** (-0.5)
    weighted = keys.astype(F32) * (jnp.exp(per_head(end - column, lanes)) * scale)
    high, low = split(weighted)
    dims = (((0,), (0,)), ((), ()))
    return lax.dot_general(high, values, dims, preferred_element_type=F32) + lax.dot_general(
        low, values, dims, preferred_element_type=F32
    )


def state_kernel(key_ref, value_ref, column_ref, out_ref):
    width = key_ref.shape[1]
    step = pl.program_id(0)

    @pl.when(step == 0)
    def _():
        out_ref[0:width, :] = jnp.zeros((width, width), F32)
        out_ref[width:, :] = jnp.zeros((EXTRA, width), F32)

    lanes = lax.broadcasted_iota(jnp.int32, key_ref.shape, 1)
    column = column_ref[...]
    end = column[BLOCK - 1 : BLOCK, :]
    end_lanes = per_head(end, lanes[0:1, :])
    fresh = gathered_update(key_ref[...], value_ref[...], column, lanes, end)
    out_ref[0:width, :] = out_ref[0:width, :] * jnp.exp(end_lanes) + fresh
    out_ref[width:, :] = out_ref[width:, :] + end_lanes


def retention_kernel(
    mine_ref, query_ref, key_ref, value_ref, gate_ref, column_ref, row_ref, gain_ref, states_ref,
    out_ref, state
):
    rows, width = query_ref.shape
    heads = width // HEAD
    step = pl.program_id(0)
    count = states_ref.shape[0]
    row_ids = lax.broadcasted_iota(jnp.int32, (width, width), 0) // HEAD
    column_ids = lax.broadcasted_iota(jnp.int32, (width, width), 1) // HEAD

    @pl.when(step == 0)
    def _():
        total = jnp.zeros((width, width), F32)
        for position in range(count - 1):
            decay = jnp.exp(states_ref[position, width : width + 1, :])
            longer = total * decay + states_ref[position, 0:width, :]
            total = jnp.where(position < mine_ref[0], longer, total)
        state[...] = jnp.where(row_ids == column_ids, total, 0.0)

    lanes = lax.broadcasted_iota(jnp.int32, (rows, width), 1)
    queries, keys, values = query_ref[...], key_ref[...], value_ref[...]
    column = column_ref[...]
    end = column[rows - 1 : rows, :]
    causal = lax.broadcasted_iota(jnp.int32, (rows, rows), 0) >= lax.broadcasted_iota(
        jnp.int32, (rows, rows), 1
    )
    scale = HEAD ** (-0.5)
    high, low = split(state[...])
    carried = jnp.dot(queries, high, preferred_element_type=F32) + jnp.dot(
        queries, low, preferred_element_type=F32
    )
    retained = carried * jnp.exp(per_head(column, lanes))
    inner = None
    for head in range(heads):
        own = jnp.where(lanes // HEAD == head, queries.astype(F32), 0.0).astype(BF16)
        scores = lax.dot_general(
            own, keys, (((1,), (1,)), ((), ())), preferred_element_type=F32
        )
        spread = column[:, head : head + 1] - row_ref[0, head : head + 1, :]
        damping = jnp.exp(jnp.where(causal, spread, -jnp.inf))
        factor = (scores * scale * damping).astype(BF16)
        term = jnp.dot(factor, values, preferred_element_type=F32)
        inner = term if inner is None else jnp.where(lanes // HEAD == head, term, inner)
    retained = retained + inner
    fresh = gathered_update(keys, values, column, lanes, end)
    end_lanes = per_head(end, lanes[0:1, :])
    state[...] = state[...] * jnp.exp(end_lanes) + jnp.where(row_ids == column_ids, fresh, 0.0)

    def head_mean(array):
        out = None
        for head in range(heads):
            inside = lanes // HEAD == head
            mean = jnp.sum(jnp.where(inside, array, 0.0), axis=1, keepdims=True) * (1.0 / HEAD)
            out = jnp.broadcast_to(mean, array.shape) if out is None else jnp.where(inside, mean, out)
        return out

    centered = retained - head_mean(retained)
    normed = centered * lax.rsqrt(head_mean(centered * centered) + eps)
    gates = gate_ref[...].astype(F32)
    out_ref[...] = (normed * gain_ref[...] * (gates * jax.nn.sigmoid(gates))).astype(BF16)


def retention(query_rows, key_rows, value_rows, gate_rows, log_decay, head_gain):
    rows, width = query_rows.shape
    heads = width // HEAD
    count = rows // BLOCK
    running = jnp.cumsum(log_decay.reshape(heads, count, BLOCK), axis=2)
    row = running.transpose(1, 0, 2)
    column = running.reshape(heads, rows).T
    block = pl.BlockSpec((BLOCK, width), lambda i: (i, 0))
    column_block = pl.BlockSpec((BLOCK, heads), lambda i: (i, 0))
    state_call = pl.pallas_call(
        state_kernel,
        grid=(count,),
        in_specs=[block, block, column_block],
        out_specs=pl.BlockSpec((width + EXTRA, width), lambda i: (0, 0)),
        out_shape=jax.ShapeDtypeStruct((width + EXTRA, width), F32),
        compiler_params=pltpu.CompilerParams(dimension_semantics=("arbitrary",)),
        cost_estimate=pl.CostEstimate(
            flops=4 * rows * width * width, bytes_accessed=4 * rows * width, transcendentals=rows * width
        ),
    )
    own = state_call(key_rows, value_rows, column)
    states = lax.all_gather(own, "sp")
    mine = lax.axis_index("sp").astype(jnp.int32).reshape(1)
    return pl.pallas_call(
        retention_kernel,
        grid=(count,),
        in_specs=[
            pl.BlockSpec(memory_space=pltpu.SMEM),
            block,
            block,
            block,
            block,
            column_block,
            pl.BlockSpec((1, heads, BLOCK), lambda i: (i, 0, 0)),
            pl.BlockSpec((1, width), lambda i: (0, 0)),
            pl.BlockSpec(states.shape, lambda i: (0, 0, 0)),
        ],
        out_specs=block,
        out_shape=jax.ShapeDtypeStruct((rows, width), BF16),
        scratch_shapes=[pltpu.VMEM((width, width), F32)],
        compiler_params=pltpu.CompilerParams(dimension_semantics=("arbitrary",)),
        cost_estimate=pl.CostEstimate(
            flops=8 * rows * width * BLOCK,
            bytes_accessed=10 * rows * width,
            transcendentals=rows * BLOCK * heads,
        ),
    )(mine, query_rows, key_rows, value_rows, gate_rows, column, row, head_gain[None, :], states)


def send(piece, pairs):
    return lax.ppermute(piece, "tp", pairs)


def ring_start(own):
    size = lax.axis_size("tp")
    right = [(i, (i + 2) % size) for i in range(size)]
    left = [(i, (i - 2) % size) for i in range(size)]
    swap = [(i, i ^ 1) for i in range(size)]
    return send(own, right), send(own, left), send(own, swap)


def ring_finish(own, from_left, from_right, other):
    size = lax.axis_size("tp")
    chips = size // 2
    right = [(i, (i + 2) % size) for i in range(size)]
    left = [(i, (i - 2) % size) for i in range(size)]
    swap = [(i, i ^ 1) for i in range(size)]
    half = own.shape[1] // 2
    last = chips // 2
    pieces = [[own], [other]]
    for hop in range(1, (chips - 1) // 2 + 1):
        if hop > 1:
            from_left = send(from_left, right)
            from_right = send(from_right, left)
        for piece in (from_left, from_right):
            pieces += [[piece], [send(piece, swap)]]
    if chips % 2 == 0 and last > 1:
        first = send(from_left[:, :half], right)
        second = send(from_right[:, half:], left)
        pieces += [[first, second], [send(first, swap), send(second, swap)]]
    elif chips == 2:
        pieces += [[from_left], [send(from_left, swap)]]
    return pieces


def expert_kernel(layout, row_ref, *refs):
    count = len(layout)
    piece_refs, out_ref = refs[:count], refs[count]
    weights, middle, sems = refs[count + 1 :]
    slots, _, width, ff = weights.shape
    rows = row_ref.shape[0]
    copies = []
    for index, (slot, start, length) in enumerate(layout):
        copy = pltpu.make_async_copy(
            piece_refs[index], weights.at[slot, :, pl.ds(start, length), :], sems.at[index]
        )
        copy.start()
        copies.append(copy)
    tile = rows // 2
    for pair in range(slots // 2):
        for index, (slot, _, _) in enumerate(layout):
            if slot // 2 == pair:
                copies[index].wait()

        @pl.loop(0, 2)
        def _(step):
            span = pl.ds(pl.multiple_of(step * tile, tile), tile)
            block = row_ref[span, :]
            gate = jnp.concatenate([weights[2 * pair, 0], weights[2 * pair + 1, 0]], axis=1)
            up = jnp.concatenate([weights[2 * pair, 1], weights[2 * pair + 1, 1]], axis=1)
            gated = jnp.dot(block, gate, preferred_element_type=F32)
            raised = jnp.dot(block, up, preferred_element_type=F32)
            value = gated * jax.nn.sigmoid(gated) * raised
            middle[span, 2 * pair * ff : 2 * (pair + 1) * ff] = value.astype(BF16)

    part = 512

    @pl.loop(0, width // part)
    def _(step):
        span = pl.ds(pl.multiple_of(step * part, part), part)
        down = jnp.concatenate([weights[slot, 2, span, :] for slot in range(slots)], axis=1)
        out_ref[:, span] = lax.dot_general(
            middle[...], down, (((1,), (1,)), ((), ())), preferred_element_type=F32
        ).astype(BF16)


def experts(rows, shards):
    _, width, ff = shards[0][0].shape
    count = len(shards)
    if ff % 128 or count % 2:
        whole = jnp.concatenate([jnp.concatenate(shard, axis=1) for shard in shards], axis=2)
        middle = (
            jax.nn.silu(jnp.dot(rows, whole[0], preferred_element_type=F32))
            * jnp.dot(rows, whole[1], preferred_element_type=F32)
        ).astype(BF16)
        return lax.dot_general(
            middle, whole[2], (((1,), (1,)), ((), ())), preferred_element_type=F32
        ).astype(BF16)
    layout, pieces = [], []
    for slot, shard in enumerate(shards):
        start = 0
        for piece in shard:
            layout.append((slot, start, piece.shape[1]))
            pieces.append(piece)
            start += piece.shape[1]
    return pl.pallas_call(
        functools.partial(expert_kernel, layout),
        in_specs=[pl.BlockSpec(memory_space=pltpu.VMEM)]
        + [pl.BlockSpec(memory_space=pl.ANY)] * len(pieces),
        out_specs=pl.BlockSpec(memory_space=pltpu.VMEM),
        out_shape=jax.ShapeDtypeStruct(rows.shape, BF16),
        scratch_shapes=[
            pltpu.VMEM((count, 3, width, ff), BF16),
            pltpu.VMEM((rows.shape[0], count * ff), BF16),
            pltpu.SemaphoreType.DMA((len(pieces),)),
        ],
        compiler_params=pltpu.CompilerParams(vmem_limit_bytes=60 * 1024 * 1024),
        cost_estimate=pl.CostEstimate(
            flops=6 * rows.shape[0] * width * count * ff,
            bytes_accessed=6 * width * count * ff + 4 * rows.size,
            transcendentals=rows.shape[0] * count * ff,
        ),
    )(rows, *pieces)


def on_device(
    query_rows,
    key_rows,
    value_rows,
    gate_rows,
    log_decay,
    residual,
    head_gain,
    out_weight,
    norm_gain,
    expert_ids,
    route_weights,
    expert_gate,
    expert_up,
    expert_down,
    shared_gate,
    shared_up,
    shared_down,
):
    part = out_weight.shape[0] // lax.axis_size("sp")
    own_part = lax.dynamic_slice_in_dim(out_weight, lax.axis_index("sp") * part, part, 0)
    out_part = lax.all_gather(own_part, "tp", axis=1, tiled=True)
    out_full = lax.all_gather(out_part, "sp", axis=0, tiled=True)
    shard = jnp.stack([expert_gate, expert_up, expert_down])
    shard, log_decay = lax.optimization_barrier((shard, log_decay))
    from_left, from_right, other = ring_start(shard)

    specialists = lax.axis_size("sp")
    tokens, chosen = expert_ids.shape
    width = residual.shape[1]
    capacity = 3 * tokens * chosen // (2 * specialists)
    names = jnp.arange(specialists, dtype=jnp.int32)[:, None]
    named = [expert_ids[:, j][None, :] == names for j in range(chosen)]
    match = functools.reduce(jnp.logical_or, named)
    weight = sum(jnp.where(named[j], route_weights[:, j][None, :], 0.0) for j in range(chosen))
    earlier = jnp.arange(tokens)[:, None] < jnp.arange(tokens)[None, :]
    position = jnp.dot(match.astype(BF16), earlier.astype(BF16), preferred_element_type=F32)
    place = jnp.where(match, position.astype(jnp.int32), -1)
    sits = place[:, None, :] == jnp.arange(capacity, dtype=jnp.int32)[None, :, None]
    pick = sits.astype(BF16).reshape(specialists * capacity, tokens)
    weight_high = lax.reduce_precision(weight, 8, 7)
    weight_low = weight - weight_high
    back_high = jnp.where(sits, weight_high[:, None, :], 0.0).astype(BF16)
    back_low = jnp.where(sits, weight_low[:, None, :], 0.0).astype(BF16)

    ret_rows = retention(query_rows, key_rows, value_rows, gate_rows, log_decay, head_gain)
    token_rows = lax.all_to_all(ret_rows, "tp", split_axis=0, concat_axis=1, tiled=True)
    token_rows, from_left, from_right = lax.optimization_barrier((token_rows, from_left, from_right))
    shards = ring_finish(shard, from_left, from_right, other)
    mixer = jnp.dot(token_rows, out_full, preferred_element_type=F32)
    hidden = (residual.astype(F32) + mixer).astype(BF16)
    hidden_wide = hidden.astype(F32)
    normed_rows = (
        hidden_wide
        * lax.rsqrt(jnp.mean(hidden_wide * hidden_wide, axis=1, keepdims=True) + eps)
        * norm_gain
    ).astype(BF16)
    outgoing = jnp.dot(pick, normed_rows, preferred_element_type=F32).astype(BF16)
    outgoing = outgoing.reshape(specialists, capacity, width)
    arrived = lax.all_to_all(outgoing, "sp", split_axis=0, concat_axis=0, tiled=True)
    shared_mid = (
        jax.nn.silu(jnp.dot(normed_rows, shared_gate, preferred_element_type=F32))
        * jnp.dot(normed_rows, shared_up, preferred_element_type=F32)
    ).astype(BF16)
    shared_out = lax.dot_general(
        shared_mid, shared_down, (((1,), (1,)), ((), ())), preferred_element_type=F32
    )
    flat_rows = arrived.reshape(-1, width)
    processed = experts(flat_rows, shards).reshape(arrived.shape)
    returned = lax.all_to_all(processed, "sp", split_axis=0, concat_axis=0, tiled=True)
    dims = (((0, 1), (0, 1)), ((), ()))
    routed = lax.dot_general(back_high, returned, dims, preferred_element_type=F32)
    routed += lax.dot_general(back_low, returned, dims, preferred_element_type=F32)
    return (hidden_wide + routed + shared_out).astype(BF16)


MESH = pl.DeviceIdType.MESH
NT = (((1,), (1,)), ((), ()))
TN = (((0,), (0,)), ((), ()))


def thirds(value):
    first = value.astype(BF16)
    rest = value - first.astype(F32)
    second = rest.astype(BF16)
    return first, second, (rest - second.astype(F32)).astype(BF16)


def piece_widths(depth):
    return [128] + [256] * ((depth - 256) // 256) + [128]


STRAIGHT = 1


def layer_kernel(
    query_hbm, key_hbm, value_hbm, gate_hbm, decay_hbm, residual_hbm, head_gain_hbm, out_weight_hbm,
    norm_gain_hbm, ids_hbm, route_hbm, expert_gate_hbm, expert_up_hbm, expert_down_hbm,
    shared_gate_hbm, shared_up_hbm, shared_down_hbm,
    result_ref,
    decay_ref, head_gain_ref, norm_gain_ref, ids_ref, route_ref,
    query, key, value, gates, residual, shared_gate, shared_up, shared_down,
    weights, out_full, running, row_running, updates, states, state, inner, ret_rows, token_rows,
    hidden, normed, squares, tables, outgoing, arrived, middle, processed, direct, passing, merged,
    combined, final, base, shared_middle, back, shares,
    local_sem, state_send, state_recv, mix_send, mix_recv, out_z_send, out_xy_send, out_z_recv, out_xy_recv,
    out_pair_send, out_pair_recv, right_send, left_send, pair_send, line_recv, pair_recv, pair_down_recv,
    go_send, go_recv, table_send, table_recv, direct_send, home_recv, passing_send, passing_recv,
    merged_send, final_send, final_recv, hello,
):
    places_count = states.shape[0]
    size = token_rows.shape[0]
    chips = size // 2
    sp = lax.axis_index("sp")
    tp = lax.axis_index("tp")
    z, core = tp // 2, tp % 2
    blocks, rows, width = ret_rows.shape
    heads = width // HEAD
    depth = residual.shape[1]
    capacity = arrived.shape[1]
    specialists = arrived.shape[0]
    ff = weights.shape[3]
    quarter = out_full.shape[1] // places_count
    out_columns = out_full.shape[2]
    widths = piece_widths(depth)
    pieces = len(widths)
    starts = [sum(widths[:index]) for index in range(pieces)]
    half = depth // 2
    tile = processed.shape[3]
    scale = HEAD ** (-0.5)
    inputs = (expert_gate_hbm, expert_up_hbm, expert_down_hbm)
    units = [(which, start, half) for which in (0, 1) for start in (0, half)]
    first_down = len(units)
    units += [(2, start, length) for start, length in zip(starts, widths)]

    def remote(src, dst, send, recv, device):
        return pltpu.make_async_remote_copy(
            src_ref=src, dst_ref=dst, send_sem=send, recv_sem=recv, device_id=device, device_id_type=MESH
        )

    partner = (sp, z * 2 + 1 - core)
    right = (sp, tp + 2)
    left = (sp, tp - 2)

    local = [
        pltpu.make_async_copy(src, dst, local_sem.at[index])
        for index, (src, dst) in enumerate(
            [
                (decay_hbm, decay_ref),
                (ids_hbm, ids_ref),
                (route_hbm, route_ref),
                (key_hbm, key),
                (value_hbm, value),
                (query_hbm, query),
                (gate_hbm, gates),
                (head_gain_hbm, head_gain_ref),
                (norm_gain_hbm, norm_gain_ref),
                (out_weight_hbm, out_full.at[tp]),
                (residual_hbm, residual),
                (shared_gate_hbm, shared_gate),
                (shared_up_hbm, shared_up),
                (shared_down_hbm, shared_down),
                (expert_gate_hbm, weights.at[tp, 0]),
                (expert_up_hbm, weights.at[tp, 1]),
                (expert_down_hbm, weights.at[tp, 2]),
            ]
        )
    ]
    barrier = pltpu.get_barrier_semaphore()

    def greet(flag):
        for step in (1, 2):
            pl.semaphore_signal(flag, inc=1, device_id=(sp ^ step, tp), device_id_type=MESH)
        pl.semaphore_signal(flag, inc=1, device_id=partner, device_id_type=MESH)

        @pl.when(z < chips - 1)
        def _():
            pl.semaphore_signal(flag, inc=1, device_id=right, device_id_type=MESH)

        @pl.when(z > 0)
        def _():
            pl.semaphore_signal(flag, inc=1, device_id=left, device_id_type=MESH)

    def greeted(flag):
        pl.semaphore_wait(flag, jnp.where(jnp.logical_or(z == 0, z == chips - 1), 4, 5))

    greet(barrier)
    for copy in local[:9]:
        copy.start()
    greeted(barrier)
    greet(hello.at[0])

    def weight_copy(origin, unit, send, device, own=False, pair=False):
        rightward = device is right
        which, start, length = units[unit]
        span = pl.ds(start, length)
        there = weights.at[origin * 2 + core, which, span, :]
        here = inputs[which].at[span, :] if own else there
        if not pair:
            received = line_recv.at[origin if rightward else origin - 1, unit]
        elif unit < first_down:
            received = pair_recv.at[origin]
        else:
            received = pair_down_recv.at[unit - first_down]
        return remote(here, there, send, received, device)

    def to_partner(origin, unit, own=False):
        return weight_copy(origin, unit, pair_send, partner, own, True)

    def own_send(unit):
        @pl.when(z < chips - 1)
        def _():
            weight_copy(z, unit, right_send, right, True).start()

        @pl.when(z > 0)
        def _():
            weight_copy(z, unit, left_send, left, True).start()

        to_partner(z, unit, True).start()

    def relay(unit, distance):
        @pl.when(z - distance >= 0)
        def _():
            origin = z - distance
            copy = weight_copy(origin, unit, right_send, right)
            copy.wait_recv()

            @pl.when(z < chips - 1)
            def _():
                copy.start()

            to_partner(origin, unit).start()

        @pl.when(z + distance < chips)
        def _():
            origin = z + distance
            copy = weight_copy(origin, unit, left_send, left)
            copy.wait_recv()

            @pl.when(z > 0)
            def _():
                copy.start()

            to_partner(origin, unit).start()

    def from_partner(origin):
        there = weights.at[0, 0:2]
        remote(there, there, pair_send, pair_recv.at[origin], partner).wait_recv()

    def downs_from_partner(index):
        there = weights.at[0, 2, pl.ds(0, chips * widths[index]), :]
        remote(there, there, pair_send, pair_down_recv.at[index], partner).wait_recv()

    def out_z(step):
        target = (z + step) % chips
        span = pl.ds(pl.multiple_of(sp * quarter, quarter), quarter)
        return remote(
            out_weight_hbm.at[span, :], out_full.at[tp, span, :], out_z_send, out_z_recv.at[z],
            (sp, target * 2 + core),
        )

    def out_z_arrival(step):
        origin = (z + step) % chips
        there = out_full.at[0, pl.ds(0, quarter), :]
        return remote(there, there, out_z_send, out_z_recv.at[origin], partner)

    def out_piece(step, device):
        origin = (z + step) % chips
        span = pl.ds(pl.multiple_of(sp * quarter, quarter), quarter)
        there = out_full.at[origin * 2 + core, span, :]
        return remote(there, there, out_xy_send.at[step - 1], out_xy_recv.at[origin], device)

    def out_pieces(step):
        origin = (z + step) % chips
        there = out_full.at[0, pl.ds(0, (places_count - 1) * quarter), :]
        return remote(there, there, out_xy_send.at[step - 1], out_xy_recv.at[origin], partner)

    def out_pair(slot, own=False):
        return remote(
            out_weight_hbm if own else out_full.at[slot], out_full.at[slot], out_pair_send,
            out_pair_recv, partner,
        )

    def out_pairs():
        there = out_full.at[0:chips]
        return remote(there, there, out_pair_send, out_pair_recv, partner)

    @pl.when(z < chips - 1)
    def _():
        out_z(1).start()

    @pl.when(z > 0)
    def _():
        out_z(chips - 1).start()

    own_send(0)
    out_pair(tp, True).start()
    for copy in local[9:]:
        copy.start()

    for copy in local[:3]:
        copy.wait()

    row_ids = lax.broadcasted_iota(jnp.int32, (width, width), 0) // HEAD
    column_ids = lax.broadcasted_iota(jnp.int32, (width, width), 1) // HEAD
    same_head = row_ids == column_ids
    lanes = lax.broadcasted_iota(jnp.int32, (rows, width), 1)
    later = lax.broadcasted_iota(jnp.int32, (rows, rows), 0)
    sooner = lax.broadcasted_iota(jnp.int32, (rows, rows), 1)
    lower = jnp.where(later >= sooner, 1.0, 0.0).astype(BF16)
    upper = jnp.where(later <= sooner, 1.0, 0.0).astype(BF16)

    chosen, tokens = ids_ref.shape
    names = lax.broadcasted_iota(jnp.int32, (8, tokens), 0)
    match = names < 0
    weight = jnp.zeros((8, tokens), F32)
    for j in range(chosen):
        named = ids_ref[j : j + 1, :] == names
        match = jnp.logical_or(match, named)
        weight = weight + jnp.where(named, route_ref[j : j + 1, :], 0.0)
    strict = jnp.where(later < sooner, 1.0, 0.0).astype(BF16)
    position = jnp.dot(jnp.where(match, 1.0, 0.0).astype(BF16), strict, preferred_element_type=F32)
    tables[0, 0:8, :] = jnp.where(match, position, -1.0)
    tables[0, 8:16, :] = weight

    def table_copy(step):
        return remote(
            tables.at[0], tables.at[step], table_send, table_recv, (sp ^ step, tp)
        )

    greeted(hello.at[0])
    greet(hello.at[1])
    listed = jnp.concatenate(
        [
            decay_ref[head : head + 1, block * rows : (block + 1) * rows]
            for head in range(heads)
            for block in range(blocks)
        ],
        axis=0,
    )
    row_running[...] = functools.reduce(
        jnp.add, [jnp.dot(part, upper, preferred_element_type=F32) for part in thirds(listed)]
    )
    head_rows = lax.broadcasted_iota(jnp.int32, (width, rows), 0) // HEAD
    for block in range(blocks):
        spread = jnp.broadcast_to(listed[block : block + 1, :], (width, rows))
        for head in range(1, heads):
            spread = jnp.where(
                head_rows == head, listed[head * blocks + block : head * blocks + block + 1, :], spread
            )
        running[block] = functools.reduce(
            jnp.add,
            [
                lax.dot_general(lower, part, NT, preferred_element_type=F32)
                for part in thirds(spread)
            ],
        )

    greeted(hello.at[1])
    greet(hello.at[2])

    @pl.when(z == chips - 1)
    def _():
        out_z(1).start()

    for step in range(2, chips - 1):
        out_z(step).start()

    @pl.when(z == 0)
    def _():
        out_z(chips - 1).start()

    own_send(1)
    for copy in local[3:5]:
        copy.wait()
    state[...] = jnp.zeros((width + EXTRA, width), F32)

    @pl.loop(0, blocks)
    def _(block):
        span = pl.ds(pl.multiple_of(block * rows, rows), rows)
        column = running[block]
        end = column[rows - 1 : rows, :]
        weighted = key[span, :].astype(F32) * (jnp.exp(end - column) * scale)
        high, low = split(weighted)
        fresh = lax.dot_general(high, value[span, :], TN, preferred_element_type=F32)
        fresh += lax.dot_general(low, value[span, :], TN, preferred_element_type=F32)
        fresh = jnp.where(same_head, fresh, 0.0)
        updates[block] = fresh
        state[0:width, :] = state[0:width, :] * jnp.exp(end) + fresh
        state[width:, :] = state[width:, :] + end

    greeted(hello.at[2])
    states[sp] = state[...]

    def state_copy(step):
        return remote(
            state, states.at[sp], state_send, state_recv, (sp ^ step, tp)
        )

    local[5].wait()
    for step in range(1, places_count):
        state_copy(step).start()
    for step in (1, 2):
        table_copy(step).start()

    @pl.loop(0, blocks)
    def _(block):
        span = pl.ds(pl.multiple_of(block * rows, rows), rows)
        queries, keys, values = query[span, :], key[span, :], value[span, :]
        column = running[block]
        causal = later >= sooner
        total = None
        for head in range(heads):
            own = jnp.where(lanes // HEAD == head, queries.astype(F32), 0.0).astype(BF16)
            scores = lax.dot_general(own, keys, NT, preferred_element_type=F32)
            spread = column[:, head * HEAD : head * HEAD + 1] - row_running[pl.ds(head * blocks + block, 1), :]
            damping = jnp.exp(jnp.where(causal, spread, -jnp.inf))
            factor = (scores * scale * damping).astype(BF16)
            term = jnp.dot(factor, values, preferred_element_type=F32)
            total = term if total is None else jnp.where(lanes // HEAD == head, term, total)
        inner[block] = total

    there = states.at[pl.ds(0, places_count - 1)]
    remote(there, there, state_send, state_recv, partner).wait()
    total = jnp.zeros((width, width), F32)
    for position in range(places_count - 1):
        longer = total * jnp.exp(states[position, width : width + 1, :]) + states[position, 0:width, :]
        total = jnp.where(position < sp, longer, total)
    state[0:width, :] = total
    local[6].wait()
    local[7].wait()

    def head_mean(array):
        out = None
        for head in range(heads):
            inside = lanes // HEAD == head
            mean = jnp.sum(jnp.where(inside, array, 0.0), axis=1, keepdims=True) * (1.0 / HEAD)
            out = jnp.broadcast_to(mean, array.shape) if out is None else jnp.where(inside, mean, out)
        return out

    def mix_copy(block):
        return remote(
            ret_rows.at[block], token_rows.at[tp], mix_send, mix_recv, (sp, block)
        )

    def mix_start(block):
        @pl.when(block != tp)
        def _():
            mix_copy(block).start()

    @pl.loop(0, blocks)
    def _(block):
        span = pl.ds(pl.multiple_of(block * rows, rows), rows)
        column = running[block]
        end = column[rows - 1 : rows, :]
        before = state[0:width, :]
        high, low = split(before)
        queries = query[span, :]
        carried = jnp.dot(queries, high, preferred_element_type=F32) + jnp.dot(
            queries, low, preferred_element_type=F32
        )
        state[0:width, :] = before * jnp.exp(end) + updates[block]
        retained = carried * jnp.exp(column) + inner[block]
        centered = retained - head_mean(retained)
        norm = centered * lax.rsqrt(head_mean(centered * centered) + eps)
        gate = gates[span, :].astype(F32)
        mixed = (norm * head_gain_ref[...] * (gate * jax.nn.sigmoid(gate))).astype(BF16)
        ret_rows[block] = mixed

        @pl.when(block == tp)
        def _():
            token_rows[tp] = mixed

        @pl.when(block > 0)
        def _():
            mix_start(block - 1)

    mix_start(blocks - 1)

    between = jnp.logical_and(z > 0, z < chips - 1)

    @pl.when(jnp.logical_not(between))
    def _():
        for unit in range(2, len(units)):
            own_send(unit)

    for step in range(1, chips):
        out_z_arrival(step).wait_recv()
        for other in range(1, places_count):
            out_piece(step, (sp ^ other, tp)).start()

    @pl.when(jnp.logical_not(between))
    def _():
        relay(0, 1)
        relay(1, 1)

    @pl.when(between)
    def _():
        relay(0, 1)
        own_send(2)
        relay(1, 1)
        own_send(3)

    def pass_on(unit, distance, rightward):
        origin = z - distance if rightward else z + distance
        sent, device = (right_send, right) if rightward else (left_send, left)
        copy = weight_copy(origin, unit, sent, device)
        copy.wait_recv()
        copy.start()
        to_partner(origin, unit).start()

    def inward(unit):
        for chip, rightward in ((1, True), (chips - 2, False)):

            @pl.when(z == chip)
            def _():
                sent, device = (right_send, right) if rightward else (left_send, left)
                weight_copy(z, unit, sent, device, True).start()
                to_partner(z, unit, True).start()
                pass_on(unit, 1, rightward)

    def outward(unit):
        for chip, rightward in ((1, False), (chips - 2, True)):

            @pl.when(z == chip)
            def _():
                sent, device = (right_send, right) if rightward else (left_send, left)
                weight_copy(z, unit, sent, device, True).start()
                for distance in (1, 2):
                    pass_on(unit, distance, rightward)


    slot_rows = lax.broadcasted_iota(jnp.int32, (capacity, tokens), 0).astype(F32)
    there = tables.at[0:2]
    remote(there, there, table_send, table_recv, partner).wait_recv()
    for turn, (table, pair) in enumerate(
        ((0, (0, 2)), (0, (0, 1)), (1, (0, 2)), (2, (0, 1)), (0, (2, 3)))
    ):
        for side, other in enumerate(pair):
            name = sp ^ other
            place = tables[table, pl.ds(name, 1), :]
            back[turn, side] = jnp.where(place == slot_rows, 1.0, 0.0).T.astype(BF16)
            share = tables[table, pl.ds(8 + name, 1), :]
            shares[turn, side] = jnp.broadcast_to(share, (tile, tokens)).T

    for copy in local[8:11]:
        copy.wait()
    for step in range(1, chips):
        out_pieces(step).wait_recv()
        out_pair(((z + step) % chips) * 2 + core).start()
    out_pairs().wait_recv()
    there = token_rows.at[pl.ds(0, size - 1)]
    remote(there, there, mix_send, mix_recv, partner).wait_recv()

    squares[...] = jnp.zeros(squares.shape, F32)

    @pl.loop(0, size)
    def _(slot):
        span = pl.ds(pl.multiple_of(slot * out_columns, out_columns), out_columns)
        token = jnp.concatenate([token_rows[index] for index in range(size)], axis=1)
        mixer = jnp.dot(token, out_full[slot], preferred_element_type=F32)
        total = (residual[:, span].astype(F32) + mixer).astype(BF16)
        hidden[:, span] = total
        wide = total.astype(F32)
        wide = wide * wide
        squares[...] += functools.reduce(
            jnp.add, [wide[:, start : start + 128] for start in range(0, out_columns, 128)]
        )

    factor = lax.rsqrt(jnp.sum(squares[...], axis=1, keepdims=True) * (1.0 / depth) + eps)

    @pl.loop(0, depth // 256)
    def _(index):
        span = pl.ds(pl.multiple_of(index * 256, 256), 256)
        normed[:, span] = (hidden[:, span].astype(F32) * factor * norm_gain_ref[:, span]).astype(BF16)

    relay(0, 2)

    def go(step):
        return remote(
            outgoing.at[step - 1], arrived.at[sp], go_send, go_recv, (sp ^ step, tp)
        )

    for step in list(range(places_count - 1, -1, -1)):
        sits = jnp.where(tables[0, pl.ds(sp ^ step, 1), :] == slot_rows, 1.0, 0.0).astype(BF16)

        @pl.loop(0, depth // 512)
        def _(index):
            span = pl.ds(pl.multiple_of(index * 512, 512), 512)
            picked = jnp.dot(sits, normed[:, span], preferred_element_type=F32).astype(BF16)
            if step:
                outgoing[step - 1, :, span] = picked
            else:
                arrived[sp, :, span] = picked

        if step:
            go(step).start()

    relay(1, 2)
    relay(2, 1)

    for copy in local[11:14]:
        copy.wait()
    shared = shared_gate.shape[1]

    @pl.loop(0, shared // 256)
    def _(index):
        span = pl.ds(pl.multiple_of(index * 256, 256), 256)
        gated = jnp.dot(normed[...], shared_gate[:, span], preferred_element_type=F32)
        raised = jnp.dot(normed[...], shared_up[:, span], preferred_element_type=F32)
        shared_middle[:, span] = (gated * jax.nn.sigmoid(gated) * raised).astype(BF16)

    @pl.loop(0, depth // 512)
    def _(index):
        span = pl.ds(pl.multiple_of(index * 512, 512), 512)
        base[:, span] = hidden[:, span].astype(F32) + lax.dot_general(
            shared_middle[...], shared_down[span, :], NT, preferred_element_type=F32
        )

    relay(0, 3)
    relay(3, 1)
    relay(2, 2)
    relay(1, 3)
    relay(3, 2)
    inward(first_down)
    inward(first_down + 1)

    for copy in local[14:]:
        copy.wait()
    there = arrived.at[pl.ds(0, places_count - 1)]
    remote(there, there, go_send, go_recv, partner).wait_recv()

    outward(first_down)
    inward(first_down + 2)

    def pair_middle(chip):
        @pl.loop(0, specialists // 2)
        def _(index):
            rows_here = jnp.concatenate([arrived[2 * index], arrived[2 * index + 1]], axis=0)
            gate_pair = jnp.concatenate([weights[2 * chip, 0], weights[2 * chip + 1, 0]], axis=1)
            up_pair = jnp.concatenate([weights[2 * chip, 1], weights[2 * chip + 1, 1]], axis=1)
            gated = jnp.dot(rows_here, gate_pair, preferred_element_type=F32)
            raised = jnp.dot(rows_here, up_pair, preferred_element_type=F32)
            found = (gated * jax.nn.sigmoid(gated) * raised).astype(BF16)
            span = pl.ds(pl.multiple_of(index * 2 * capacity, 2 * capacity), 2 * capacity)
            middle[span, pl.ds(pl.multiple_of(chip * 2 * ff, 2 * ff), 2 * ff)] = found

    last_chip = jnp.where(z * 2 < chips, chips - 1, 0)

    def chip_at(index):
        if index == 0:
            return z
        if index == chips - 1:
            return last_chip
        toward = jnp.where(last_chip == 0, chips - 1 - index, index)
        shifted = jnp.where(last_chip == 0, chips - index, index - 1)
        passed = jnp.where(last_chip == 0, z <= chips - 1 - index, z >= index)
        return jnp.where(passed, shifted, toward)

    for index in range(chips):
        chip = chip_at(index)
        if index == chips - 1:
            relay(2, 3)
            relay(3, 3)
        from_partner(chip)
        pair_middle(chip)

    def tiles(index):
        return range(starts[index] // tile, (starts[index] + widths[index]) // tile)

    bent_tiles = depth // tile - STRAIGHT

    def bent(index):
        return [number for number in tiles(index) if number < bent_tiles]

    def straight(index):
        return [number for number in tiles(index) if number >= bent_tiles]

    def piece_of(number):
        return next(index for index in range(pieces) if number in tiles(index))

    def arrivals(buffer, send, received, index):
        there = buffer.at[pl.ds(starts[index] // tile, len(bent(index)))]
        remote(there, there, send, received.at[index], partner).wait_recv()

    def near(number):
        return sp ^ (2, 1)[number % 2]

    def far(number):
        return sp ^ (1, 2)[number % 2]

    def direct_copy(number):
        return remote(
            processed.at[number, near(number)], direct.at[number], direct_send,
            home_recv.at[piece_of(number)], (near(number), tp),
        )

    def passing_copy(number):
        return remote(
            processed.at[number, sp ^ 3], passing.at[number], passing_send,
            passing_recv.at[piece_of(number)], (near(number), tp),
        )

    def merged_copy(number):
        return remote(
            merged.at[number], combined.at[number], merged_send,
            home_recv.at[piece_of(number)], (far(number), tp),
        )

    def weighted(turn, first, second):
        first = jnp.dot(back[turn, 0], first, preferred_element_type=F32) * shares[turn, 0]
        return first + jnp.dot(back[turn, 1], second, preferred_element_type=F32) * shares[turn, 1]

    def merge(index):
        arrivals(passing, passing_send, passing_recv, index)
        for number in bent(index):
            found = weighted(2 + number % 2, processed[number, far(number)], passing[number])
            merged[number] = found.astype(BF16)
        for number in bent(index):
            merged_copy(number).start()

    last_tile = depth // tile - 1

    def final_copy(number, step):
        turn = number - bent_tiles
        return remote(
            processed.at[number, sp ^ step], final.at[turn, step - 1], final_send, final_recv.at[turn],
            (sp ^ step, tp),
        )

    def final_combine(number):
        turn = number - bent_tiles
        there = final.at[turn]
        remote(there, there, final_send, final_recv.at[turn], partner).wait_recv()
        routed = weighted(1, processed[number, sp], final[turn, 0])
        store(number, routed + weighted(4, final[turn, 1], final[turn, 2]))

    def store(number, routed):
        span = slice(number * tile, (number + 1) * tile)
        result_ref[:, span] = (base[:, span] + routed).astype(BF16)

    def combine(index):
        count = len(bent(index))
        there = weights.at[0, 0, pl.ds(0, count * (capacity + tokens)), :]
        remote(there, there, direct_send, home_recv.at[index], partner).wait_recv()
        for number in bent(index):
            routed = weighted(number % 2, processed[number, sp], direct[number])
            store(number, routed + combined[number].astype(F32))

    lag = 4

    outward(first_down + 1)
    inward(first_down + 3)
    for index in range(pieces):
        unit = first_down + index

        if index + 2 < pieces:
            outward(unit + 2)
        if index + 4 < pieces:
            inward(unit + 4)

        @pl.when(jnp.logical_not(between))
        def _():
            for distance in range(1, chips):
                relay(unit, distance)

        downs_from_partner(index)
        down = jnp.concatenate(
            [weights[slot, 2, starts[index] : starts[index] + widths[index], :] for slot in range(size)], axis=1
        )

        if index == pieces - 1:
            for step in range(places_count - 1, -1, -1):
                span = pl.ds(pl.multiple_of((sp ^ step) * capacity, capacity), capacity)
                found = lax.dot_general(middle[span, :], down, NT, preferred_element_type=F32)
                processed[last_tile, sp ^ step] = found.astype(BF16)
                if step:
                    final_copy(last_tile, step).start()
            merge(index - 1)
            continue
        found = lax.dot_general(middle[...], down, NT, preferred_element_type=F32).astype(BF16)
        for part, number in enumerate(tiles(index)):
            for source in range(specialists):
                processed[number, source] = found[
                    source * capacity : (source + 1) * capacity, part * tile : (part + 1) * tile
                ]

        for number in straight(index):
            final_copy(number, 3).start()
        for number in bent(index):
            passing_copy(number).start()
        for number in bent(index):
            direct_copy(number).start()
        for number in straight(index):
            final_copy(number, 2).start()
            final_copy(number, 1).start()
        if index:
            merge(index - 1)
        if index >= lag:
            combine(index - lag)

    for index in range(pieces - 1 - lag, pieces - 2):
        combine(index)
    for number in range(bent_tiles, last_tile):
        final_combine(number)
    combine(pieces - 2)
    final_combine(last_tile)

    there = out_full.at[0, pl.ds(0, (chips - 1) * quarter), :]
    remote(there, there, out_z_send, out_z_recv.at[0], partner).wait_send()
    for step in range(1, chips):
        out_pieces(step).wait_send()
    out_pairs().wait_send()
    there = ret_rows.at[pl.ds(0, blocks - 1)]
    remote(there, there, mix_send, mix_recv, partner).wait_send()
    remote(outgoing, outgoing, go_send, go_recv, partner).wait_send()
    for buffer, sent in ((direct, direct_send), (passing, passing_send), (merged, merged_send)):
        there = buffer.at[pl.ds(0, bent_tiles)]
        remote(there, there, sent, passing_recv.at[0], partner).wait_send()
    remote(final, final, final_send, final_recv.at[0], partner).wait_send()
    there = tables.at[0:2]
    remote(there, there, table_send, table_recv, partner).wait_send()
    for chip in range(chips):

        @pl.when(z == chip)
        def _():
            if chip < chips - 1:
                there = weights.at[0 : chip + 1]
                remote(there, there, right_send, line_recv.at[0, 0], right).wait_send()
            if chip > 0:
                there = weights.at[0 : chips - chip]
                remote(there, there, left_send, line_recv.at[0, 0], left).wait_send()

    there = weights.at[0:chips]
    remote(there, there, pair_send, line_recv.at[0, 0], partner).wait_send()


def whole_layer(*arrays):
    (query, _, _, _, _, residual, head_gain, out_weight, norm_gain, ids, _, expert_gate) = arrays[:12]
    shared_gate = arrays[14]
    places_count, size = lax.axis_size("sp"), lax.axis_size("tp")
    rows_all, width = query.shape
    tokens, depth = residual.shape
    blocks = rows_all // tokens
    chosen = ids.shape[1]
    capacity = 3 * tokens * chosen // (2 * places_count)
    ff = expert_gate.shape[1]
    shared = shared_gate.shape[1]
    chips = size // 2
    pieces = len(piece_widths(depth))
    units = 4 + pieces
    heads = width // HEAD
    dma = pltpu.SemaphoreType.DMA
    arrays = list(arrays)
    arrays[6] = head_gain[None, :]
    arrays[8] = norm_gain[None, :]
    arrays[9], arrays[10] = arrays[9].T, arrays[10].T
    vmem, anywhere = pl.BlockSpec(memory_space=pltpu.VMEM), pl.BlockSpec(memory_space=pl.ANY)
    block = lambda *shape: pltpu.VMEM(shape, BF16)
    wide = lambda *shape: pltpu.VMEM(shape, F32)
    return pl.pallas_call(
        layer_kernel,
        in_specs=[anywhere] * len(arrays),
        out_specs=vmem,
        out_shape=pltpu.VMEM((tokens, depth), BF16),
        scratch_shapes=[
            wide(*arrays[4].shape), wide(1, width), wide(1, depth),
            pltpu.VMEM(arrays[9].shape, jnp.int32), wide(*arrays[10].shape),
            block(rows_all, width), block(rows_all, width), block(rows_all, width), block(rows_all, width),
            block(tokens, depth), block(depth, shared), block(depth, shared), block(depth, shared),
            block(size, 3, depth, ff),
            block(size, out_weight.shape[0], out_weight.shape[1]),
            wide(blocks, tokens, width),
            wide(heads * blocks, tokens),
            wide(blocks, width, width),
            wide(places_count, width + EXTRA, width),
            wide(width + EXTRA, width),
            wide(blocks, tokens, width),
            block(blocks, tokens, width),
            block(size, tokens, width),
            block(tokens, depth), block(tokens, depth),
            wide(tokens, 128),
            wide(3, 16, tokens),
            block(places_count - 1, capacity, depth),
            block(places_count, capacity, depth),
            block(places_count * capacity, size * ff),
            block(depth // 128, places_count, capacity, 128),
            block(depth // 128, capacity, 128), block(depth // 128, capacity, 128),
            block(depth // 128, tokens, 128), block(depth // 128, tokens, 128),
            block(STRAIGHT, places_count - 1, capacity, 128),
            wide(tokens, depth),
            block(tokens, shared),
            block(5, 2, tokens, capacity), wide(5, 2, tokens, 128),
            dma((17,)),
            dma, dma,
            dma, dma,
            dma, dma((chips - 1,)), dma((chips,)), dma((chips,)),
            dma, dma,
            dma, dma, dma, dma((chips - 1, units)), dma((chips,)), dma((pieces,)),
            dma, dma,
            dma, dma,
            dma, dma((pieces,)), dma, dma((pieces,)), dma, dma, dma((STRAIGHT,)),
            pltpu.SemaphoreType.REGULAR((3,)),
        ],
        compiler_params=pltpu.CompilerParams(
            collective_id=0, has_side_effects=True, vmem_limit_bytes=58 * 1000 * 1000
        ),
        cost_estimate=pl.CostEstimate(
            flops=20 * 10**9, bytes_accessed=40 * 10**6, transcendentals=4 * 10**6
        ),
    )(*arrays)


def kernel_fits(mesh, shapes):
    places_count, size = mesh.shape["sp"], mesh.shape["tp"]
    if places_count != 4 or size != 8:
        return False
    width = shapes[0][1] // size
    tokens = shapes[5][0] // (places_count * size)
    rows_all = shapes[0][0] // places_count
    ff = shapes[11][1] // (places_count * size)
    return width == 128 and ff % 128 == 0 and tokens % 128 == 0 and rows_all == tokens * size


def solution(mesh):
    placed = (
        P("sp", "tp"),
        P("sp", "tp"),
        P("sp", "tp"),
        P("sp", "tp"),
        P("tp", "sp"),
        P(("sp", "tp"), None),
        P("tp"),
        P(None, "tp"),
        P(),
        P(("sp", "tp"), None),
        P(("sp", "tp"), None),
        P(None, ("sp", "tp")),
        P(None, ("sp", "tp")),
        P(None, ("sp", "tp")),
        P(),
        P(),
        P(),
    )

    placement = dict(mesh=mesh, in_specs=placed, out_specs=P(("sp", "tp"), None), check_vma=False)
    step = jax.shard_map(on_device, **placement)
    fused = jax.shard_map(whole_layer, **placement)

    def run(*arrays):
        fits = kernel_fits(mesh, [array.shape for array in arrays])
        return fused(*arrays) if fits else step(*arrays)

    return run
```
